256 devices in a mesh: ep: 16 (over y, x), tp: 16 (over z, core).
Axes of the slice: x: 4, y: 4, z: 8, core: 2. Of those that a mesh axis runs over, the one named last changes fastest.
Arguments:
- tokens: bfloat16 [1024, 2048], P('ep', 'tp'), may hold values from -6 to 6
- conv_state: bfloat16 [1024, 3, 2048], P('ep', None, 'tp'), may hold values from -6 to 6
- recur_state: float32 [1024, 2048], P('ep', 'tp'), may hold values from -6 to 6
- norm1_gain: bfloat16 [2048], P('tp'), may hold values from 0.099609375 to 1.8984375
- branch_weight: bfloat16 [2048, 2048], P(None, 'tp'), may hold values from -0.125 to 0.125
- gating_weight: bfloat16 [2048, 2048], P(None, 'tp'), may hold values from -0.125 to 0.125
- conv_taps: bfloat16 [4, 2048], P(None, 'tp'), may hold values from -3 to 3
- conv_bias: bfloat16 [2048], P('tp'), may hold values from -3 to 3
- recur_weight: bfloat16 [16, 128, 128], P('tp'), may hold values from -0.5 to 0.5
- recur_bias: float32 [2048], P('tp'), may hold values from -4 to 4
- input_weight: bfloat16 [16, 128, 128], P('tp'), may hold values from -0.5 to 0.5
- input_bias: float32 [2048], P('tp'), may hold values from -4 to 4
- decay_logit: float32 [2048], P('tp'), may hold values from 1.5 to 7.5
- out_weight: bfloat16 [2048, 2048], P(None, 'tp'), may hold values from -0.125 to 0.125
- norm2_gain: bfloat16 [2048], P('tp'), may hold values from 0.099609375 to 1.8984375
- group_router: bfloat16 [2048, 4], replicated, may hold values from -0.125 to 0.125
- expert_router: bfloat16 [2048, 16], replicated, may hold values from -0.125 to 0.125
- routes: int32 [1024, 2], P('ep'), may hold values from 0 to 15, as said below
- gate_experts: bfloat16 [16, 2048, 1024], P('ep', None, 'tp'), may hold values from -0.125 to 0.125
- up_experts: bfloat16 [16, 2048, 1024], P('ep', None, 'tp'), may hold values from -0.125 to 0.125
- down_experts: bfloat16 [16, 1024, 2048], P('ep', 'tp'), may hold values from -0.75 to 0.75
Outputs:
- mixed: bfloat16 [1024, 2048], P('ep', 'tp')
- new_state: float32 [1024, 2048], P('ep', 'tp')
- new_conv: bfloat16 [1024, 3, 2048], P('ep', None, 'tp')
The draws below stay inside these ranges and needn't reach their ends.
Inputs may be any that keep to these rules, and one draw needn't show every extreme that they name: `routes`: each row names 2 different experts. In each aligned block of 64 rows (the rows of one index of ep) exactly half of the 16 experts are named, each by exactly 16 rows, and some expert is named by 16 rows in every block.
All inputs are finite; a program needn't handle non-finite values.
Results may differ from the reference program's by a relative error of at most 0.018.
Values may be sent and summed in bfloat16 or wider, within the bound.
A program may use at most 64 MiB of HBM per device.

```python
import jax
import jax.numpy as jnp
from jax import lax

D = 2048
FF = 1024
RNN_BLOCKS = 16
TAPS = 4
GROUPS = 4
TOPK = 2
SEQS_DEV = 64
EXPERTS = 16
GROUP_SIZE = 4
CAP = 16
BATCH = 1024
N_EP = 16


def draw_routes(key, part):
    half_count = EXPERTS // 2
    rest_count = EXPERTS - 1
    base_order = jax.random.permutation(jax.random.fold_in(key, 7), EXPERTS).astype(jnp.int32)
    positions = jnp.arange(SEQS_DEV)[:, None] + SEQS_DEV * jnp.arange(TOPK)[None, :]
    column_ids = positions // CAP

    def one_block(block_index):
        block_key = jax.random.fold_in(key, 1000 + block_index)
        others = 1 + (block_index * (half_count - 1) + jnp.arange(half_count - 1)) % rest_count
        chosen = jnp.concatenate([base_order[:1], base_order[others]])
        chosen = chosen[jax.random.permutation(jax.random.fold_in(block_key, 1), half_count)]
        picked = chosen[column_ids]
        row_order = jax.random.permutation(jax.random.fold_in(block_key, 2), SEQS_DEV)
        return picked[row_order]
    blocks = BATCH // SEQS_DEV
    return jax.vmap(one_block)(jnp.arange(blocks)).reshape(BATCH, TOPK).astype(jnp.int32)


def steps_of(stream_key, dims, shards, smallest, largest):
    factor_of = 1.0
    for axis_at, parts in shards:
        draws = jax.random.uniform(jax.random.fold_in(jax.random.fold_in(stream_key, 6), axis_at), (parts,), jnp.float32, smallest / len(shards), largest / len(shards))
        factor_of = factor_of * jnp.repeat(jnp.exp(draws), dims[axis_at] // parts).reshape((-1,) + (1,) * (len(dims) - 1 - axis_at))
    return factor_of


def normal_values(stream_key, dims, width, reach, pieces=(), held_as=jnp.bfloat16):
    array = jax.random.normal(stream_key, dims, jnp.float32) * width
    if len(pieces) > 0:
        array = steps_of(stream_key, dims, pieces, -0.22, 0.18) * array
    return jnp.clip(array, min=-reach, max=reach).astype(held_as)


def setup_inputs(seed: int = 0) -> dict:
    arg_keys = jax.random.split(jax.random.key(seed), 22)
    return {
        "tokens": normal_values(arg_keys[0], (BATCH, D), 1.0, 6.0, ((0, 16), (1, 16))),
        "conv_state": normal_values(arg_keys[1], (BATCH, TAPS - 1, D), 1.0, 6.0, ((0, 16), (2, 16))),
        "recur_state": normal_values(arg_keys[2], (BATCH, D), 1.0, 6.0, ((0, 16), (1, 16)), jnp.float32),
        "norm1_gain": jnp.clip(1.0 + 0.18 * jax.random.normal(arg_keys[3], (D,), jnp.float32), 0.099609375, 1.8984375).astype(jnp.bfloat16),
        "branch_weight": normal_values(arg_keys[4], (D, D), D ** -0.5, 0.125, ((1, 16),)),
        "gating_weight": normal_values(arg_keys[5], (D, D), D ** -0.5, 0.125, ((1, 16),)),
        "conv_taps": normal_values(arg_keys[6], (TAPS, D), 0.5, 3.0, ((1, 16),)),
        "conv_bias": normal_values(arg_keys[7], (D,), 0.5, 3.0, ((0, 16),)),
        "recur_weight": normal_values(arg_keys[8], (RNN_BLOCKS, D // RNN_BLOCKS, D // RNN_BLOCKS), (D // RNN_BLOCKS) ** -0.5, 0.5, ((0, 16),)),
        "recur_bias": normal_values(arg_keys[9], (D,), 1.0, 4.0, ((0, 16),), jnp.float32),
        "input_weight": normal_values(arg_keys[10], (RNN_BLOCKS, D // RNN_BLOCKS, D // RNN_BLOCKS), (D // RNN_BLOCKS) ** -0.5, 0.5, ((0, 16),)),
        "input_bias": normal_values(arg_keys[11], (D,), 1.0, 4.0, ((0, 16),), jnp.float32),
        "decay_logit": jnp.clip(1.5 + 6.0 * jax.random.uniform(arg_keys[12], (D,), jnp.float32) ** steps_of(arg_keys[12], (D,), ((0, 16),), -0.2, 0.2), 1.5, 7.5),
        "out_weight": normal_values(arg_keys[13], (D, D), D ** -0.5, 0.125, ((1, 16),)),
        "norm2_gain": jnp.clip(1.0 + 0.18 * jax.random.normal(arg_keys[14], (D,), jnp.float32), 0.099609375, 1.8984375).astype(jnp.bfloat16),
        "group_router": normal_values(arg_keys[15], (D, GROUPS), D ** -0.5, 0.125),
        "expert_router": normal_values(arg_keys[16], (D, EXPERTS), D ** -0.5, 0.125),
        "routes": draw_routes(jax.random.fold_in(arg_keys[21], 71), 0),
        "gate_experts": normal_values(arg_keys[18], (EXPERTS, D, FF), D ** -0.5, 0.125, ((0, 16), (2, 16))),
        "up_experts": normal_values(arg_keys[19], (EXPERTS, D, FF), D ** -0.5, 0.125, ((0, 16), (2, 16))),
        "down_experts": normal_values(arg_keys[20], (EXPERTS, FF, D), (FF // 16) ** -0.5, 0.75, ((0, 16), (1, 16))),
    }


EPS = 1e-06

def rms_scale(values):
    floats = values.astype(jnp.float32)
    return lax.rsqrt(lax.optimization_barrier(jnp.mean(floats * floats, axis=-1, keepdims=True)) + EPS)

def reference(tokens, conv_state, recur_state, norm1_gain, branch_weight, gating_weight, conv_taps, conv_bias, recur_weight, recur_bias, input_weight, input_bias, decay_logit, out_weight, norm2_gain, group_router, expert_router, routes, gate_experts, up_experts, down_experts):
    batch = tokens.shape[0]
    tok_float = tokens.astype(jnp.float32)
    normed = (tok_float * rms_scale(tokens) * norm1_gain.astype(jnp.float32)).astype(jnp.bfloat16)
    branch = jnp.dot(normed, branch_weight, preferred_element_type=jnp.float32).astype(jnp.bfloat16)
    gating = jnp.dot(normed, gating_weight, preferred_element_type=jnp.float32).astype(jnp.bfloat16)
    window = jnp.concatenate([conv_state, branch[:, None, :]], axis=1)
    new_conv = window[:, 1:]
    conv_out = conv_bias.astype(jnp.float32) + lax.optimization_barrier(jnp.sum(conv_taps.astype(jnp.float32)[None] * window.astype(jnp.float32), axis=1))
    conv_low = conv_out.astype(jnp.bfloat16)
    blocks = conv_low.reshape(batch, RNN_BLOCKS, D // RNN_BLOCKS).astype(jnp.float32)
    recur_gate = jax.nn.sigmoid(jnp.einsum('bnc,ncd->bnd', blocks, recur_weight.astype(jnp.float32)).reshape(batch, D) + recur_bias)
    input_gate = jax.nn.sigmoid(jnp.einsum('bnc,ncd->bnd', blocks, input_weight.astype(jnp.float32)).reshape(batch, D) + input_bias)
    log_decay = 8.0 * recur_gate * jax.nn.log_sigmoid(decay_logit)
    new_state = jnp.exp(log_decay) * recur_state + jnp.sqrt(-jnp.expm1(2.0 * log_decay)) * (input_gate * conv_out)
    hidden_mix = (new_state * jax.nn.gelu(gating.astype(jnp.float32))).astype(jnp.bfloat16)
    mixer_out = jnp.dot(hidden_mix, out_weight, preferred_element_type=jnp.float32)
    resid = (tok_float + mixer_out).astype(jnp.bfloat16)
    normed2 = (resid.astype(jnp.float32) * rms_scale(resid) * norm2_gain.astype(jnp.float32)).astype(jnp.bfloat16)
    group_logits = jnp.dot(normed2, group_router, preferred_element_type=jnp.float32)
    expert_logits = jnp.dot(normed2, expert_router, preferred_element_type=jnp.float32)
    group_exp = jnp.exp(group_logits)
    group_prob = group_exp / lax.optimization_barrier(jnp.sum(group_exp, axis=-1, keepdims=True))
    expert_ids = jnp.arange(EXPERTS).astype(jnp.int32)
    chosen = (routes[..., None] == expert_ids).astype(jnp.float32)
    chosen_logit = lax.optimization_barrier(jnp.sum(chosen * expert_logits[:, None, :], axis=-1))
    pair_exp = jnp.exp(chosen_logit)
    share = pair_exp / lax.optimization_barrier(jnp.sum(pair_exp, axis=-1, keepdims=True))
    group_ids = jnp.arange(GROUPS).astype(jnp.int32)
    group_hit = ((routes // GROUP_SIZE)[..., None] == group_ids).astype(jnp.float32)
    route_weight = lax.optimization_barrier(jnp.sum(group_hit * group_prob[:, None, :], axis=-1)) * share
    flat = routes.reshape(N_EP, SEQS_DEV * TOPK)
    hits = (flat[..., None] == expert_ids).astype(jnp.int32)
    rank = lax.optimization_barrier(jnp.sum((jnp.cumsum(hits, axis=1) - hits) * hits, axis=-1))
    source = jnp.arange(N_EP).astype(jnp.int32)[:, None]
    slot = (flat * (N_EP * CAP) + source * CAP + rank).reshape(-1).astype(jnp.int32)
    rows = jnp.repeat(normed2, TOPK, axis=0)
    buffer = jnp.zeros((EXPERTS * N_EP * CAP, D), jnp.bfloat16).at[slot].set(rows)
    buffer = buffer.reshape(EXPERTS, N_EP * CAP, D)

    def run_expert(operands):
        rows_in, gate_w, up_w, down_w = operands
        gate = jnp.dot(rows_in, gate_w, preferred_element_type=jnp.float32)
        upper = jnp.dot(rows_in, up_w, preferred_element_type=jnp.float32)
        hidden = (jax.nn.silu(gate) * upper).astype(jnp.bfloat16)
        return jnp.dot(hidden, down_w, preferred_element_type=jnp.float32).astype(jnp.bfloat16)
    outputs = lax.map(run_expert, (buffer, gate_experts, up_experts, down_experts)).reshape(-1, D)
    picked = outputs[slot].reshape(batch, TOPK, D).astype(jnp.float32)
    moe = lax.optimization_barrier(jnp.sum(route_weight[..., None] * picked, axis=1))
    mixed = (resid.astype(jnp.float32) + moe).astype(jnp.bfloat16)
    return (mixed, new_state, new_conv)
```

```python
import functools

import jax
import jax.numpy as jnp
from jax import lax
from jax.experimental import pallas as pl
from jax.experimental.pallas import tpu as pltpu
from jax.sharding import PartitionSpec as P

EPS = 1e-06
F32 = jnp.float32
BF16 = jnp.bfloat16
MESH = pl.DeviceIdType.MESH
NT = (((1,), (1,)), ((), ()))


def mm(a, b):
    return jnp.dot(a, b, preferred_element_type=F32)


def mm_nt(a, b):
    return lax.dot_general(a, b, NT, preferred_element_type=F32)


def expm1_neg(x):
    series = x * (1.0 + x * (0.5 + x * (1.0 / 6 + x * (1.0 / 24 + x * (1.0 / 120 + x / 720)))))
    return jnp.where(x > -0.2, -series, 1.0 - jnp.exp(x))


def log_sigmoid(x):
    u = jnp.exp(-jnp.abs(x))
    w = u / (2.0 + u)
    w2 = w * w
    poly = 1.0 / 15
    for k in (13, 11, 9, 7, 5, 3, 1):
        poly = poly * w2 + 1.0 / k
    return jnp.minimum(x, 0.0) - 2.0 * w * poly


def gelu(x):
    return 0.5 * x * (1.0 + jnp.tanh(0.7978845608028654 * (x + 0.044715 * x * x * x)))


def sigmoid(x):
    return 1.0 / (1.0 + jnp.exp(-x))


def kernel(
    EP, NZ, S, CAP, GS,
    tok_h, conv_h, state_h, par_h, bw_h, gw_h, rw_h, iw_h, ow_h, grt_h, ert_h, rt_h, gt_h, ut_h, dn_h,
    mixed_h, nstate_h, nconv_h,
    tok_a, gain_a, conv_v, state_v, par_v, bw_v, gw_v, rw_v, iw_v, ow_v, grt_v, ert_v, rt_v, wcat, wdn,
    hid_b, res_c, ysel, xbuf, rexp, lg_own, lg_in, ss_own, ss_in, acc_v, pacc_v, ssx_v, pss_v,
    hid_e, y_v, back_v, mixed_v, nstate_v, branch_v, sel_v, selt_v,
    sem_ld, s_a, r_a, f_a, s_g, r_g, f_g, s_b, r_b, f_b, s_w, r_w, f_w, s_x, r_x,
    s_c, r_c, s_d, r_d, s_l, r_l, s_p, r_p, s_e, r_e, s_f, r_f, sem_o,
):
    me = lax.axis_index("ep")
    tp = lax.axis_index("tp")
    z = tp // 2
    c = tp % 2
    L = EP * CAP
    HALF = L // 2
    HS = EP // 2
    WIDTH = NZ * 256
    other = 1 - c
    partner = (me, 2 * z + other)

    def zdev(d):
        return (me, 2 * ((z + d) % NZ) + c)

    def zrel(rd):
        return (z + rd) % NZ

    def rows(j, rd):
        t = 2 * zrel(rd) + (c if j == 0 else other)
        return pl.multiple_of(t * 128, 128)

    def back_rel(d):
        return (NZ - d) % NZ

    far_first = sorted(range(1, NZ), key=lambda d: (-min(d, NZ - d), d))
    near_first = [0] + sorted(range(1, NZ), key=lambda d: (min(d, NZ - d), d))

    def wait(ref, sem):
        pltpu.make_async_copy(ref, ref, sem).wait()

    def send(src, dst, ssem, rsem, dev):
        pltpu.make_async_remote_copy(
            src_ref=src, dst_ref=dst, send_sem=ssem, recv_sem=rsem, device_id=dev, device_id_type=MESH
        ).start()

    loads = []

    def load(src, dst):
        k = len(loads)
        cp = pltpu.make_async_copy(src, dst, sem_ld.at[k])
        cp.start()
        loads.append(cp)
        return k

    k_tok = load(tok_h, tok_a.at[0, 0])
    k_par = load(par_h, par_v)
    k_rt = load(rt_h, rt_v)

    bar = pltpu.get_barrier_semaphore()

    def sig(dev):
        pl.semaphore_signal(bar, inc=1, device_id=dev, device_id_type=MESH)

    for d in range(1, NZ):
        sig(zdev(d))
    sig(partner)

    def bar_ep(i, carry):
        e = (me + i) % EP
        sig((e, tp))
        sig((e, 2 * z + other))
        return carry

    lax.fori_loop(1, EP, bar_ep, 0)

    k_conv = load(conv_h, conv_v)
    k_state = load(state_h, state_v)
    k_bw = load(bw_h, bw_v)
    k_gw = load(gw_h, gw_v)
    k_rw = load(rw_h, rw_v)
    k_iw = load(iw_h, iw_v)
    k_ow = load(ow_h, ow_v)
    k_gr = load(grt_h, grt_v)
    k_er = load(ert_h, ert_v)
    k_w = [load(dn_h.at[:, pl.ds(pl.multiple_of(z * 256, 256), 256)], wdn.at[0, 0])]
    k_x = []
    for rd in range(NZ):
        cols = pl.ds(rows(0, rd), 128)
        k_x.append(load(gt_h.at[:, cols], wcat.at[rd, 0]))
        k_x.append(load(ut_h.at[:, cols], wcat.at[rd, 2]))

    loads[k_tok].wait()
    loads[k_par].wait()
    gain_a[0, 0] = par_v[0:2, :]

    pl.semaphore_wait(bar, (NZ - 1) + 1 + 2 * (EP - 1))

    for d in far_first:
        rd = back_rel(d)
        send(gain_a.at[0, 0], gain_a.at[rd, 0], s_g.at[d], r_g.at[rd, 0], zdev(d))
        send(tok_a.at[0, 0], tok_a.at[rd, 0], s_a.at[d], r_a.at[rd, 0], zdev(d))
    send(gain_a.at[0, 0], gain_a.at[0, 1], f_g.at[0], r_g.at[0, 1], partner)
    send(tok_a.at[0, 0], tok_a.at[0, 1], f_a.at[0], r_a.at[0, 1], partner)

    for d in far_first:
        cols = pl.ds(pl.multiple_of(((z + d) % NZ) * 256, 256), 256)
        rd = back_rel(d)
        send(dn_h.at[:, cols], wdn.at[rd, 0], s_w.at[d], r_w.at[rd, 0], zdev(d))
    for rd in range(NZ):
        cols = pl.ds(rows(1, rd), 128)
        send(gt_h.at[:, cols], wcat.at[rd, 1], s_x.at[rd, 0], r_x.at[rd, 0], partner)
        send(ut_h.at[:, cols], wcat.at[rd, 3], s_x.at[rd, 1], r_x.at[rd, 1], partner)

    loads[k_rt].wait()
    loads[k_gr].wait()
    loads[k_er].wait()
    slot_row = lax.broadcasted_iota(jnp.int32, (L, S), 0)
    r0 = rt_v[0:1, :]
    r1 = rt_v[1:2, :]
    hit = ((slot_row // CAP) == r0) | ((slot_row // CAP) == r1)
    hit_f = jnp.where(hit, 1.0, 0.0)
    hit_b = hit_f.astype(BF16)
    before = jnp.where(
        lax.broadcasted_iota(jnp.int32, (S, S), 0) < lax.broadcasted_iota(jnp.int32, (S, S), 1), 1.0, 0.0
    ).astype(BF16)
    rank = mm(hit_b, before)
    sel = jnp.where(rank == (slot_row % CAP).astype(F32), hit_f, 0.0).astype(BF16)
    sel_v[...] = sel
    eye = jnp.where(
        lax.broadcasted_iota(jnp.int32, (S, S), 0) == lax.broadcasted_iota(jnp.int32, (S, S), 1), 1.0, 0.0
    ).astype(BF16)
    selt_v[0] = mm_nt(eye, sel)
    selt_v[1] = mm_nt(eye, hit_b)
    spread_e = jnp.where(
        lax.broadcasted_iota(jnp.int32, (L, EP), 0) // CAP == lax.broadcasted_iota(jnp.int32, (L, EP), 1), 1.0, 0.0
    ).astype(BF16)
    groups = grt_h.shape[0]
    spread_g = jnp.where(
        lax.broadcasted_iota(jnp.int32, (L, groups), 0) // (CAP * GS)
        == lax.broadcasted_iota(jnp.int32, (L, groups), 1),
        1.0,
        0.0,
    ).astype(BF16)
    for rd in range(NZ):
        cols = pl.ds(rows(0, rd), 128)
        rexp[rd, 0:L] = mm(spread_e, ert_v[:, cols]).astype(BF16)
        rexp[rd, L : 2 * L] = mm(spread_g, grt_v[:, cols]).astype(BF16)
    taps = par_v[6:10, :]
    bias = par_v[2:3, :]
    loads[k_conv].wait()
    conv_part = bias + sum(taps[j : j + 1, :] * conv_v[j].astype(F32) for j in range(3))

    loads[k_bw].wait()
    loads[k_gw].wait()

    def gather_and(buf, rsem, fsem, use, extra=None):
        prev = None
        for rd in near_first:
            if rd != 0:
                wait(buf.at[rd, 0], rsem.at[rd, 0])
                send(buf.at[rd, 0], buf.at[rd, 1], fsem.at[rd], rsem.at[rd, 1], partner)
                if extra is not None:
                    xb, xr, xf = extra
                    wait(xb.at[rd, 0], xr.at[rd, 0])
                    send(xb.at[rd, 0], xb.at[rd, 1], xf.at[rd], xr.at[rd, 1], partner)
            if prev is not None:
                wait(buf.at[prev, 1], rsem.at[prev, 1])
                if extra is not None:
                    wait(extra[0].at[prev, 1], extra[1].at[prev, 1])
                use(prev)
            prev = rd
        wait(buf.at[prev, 1], rsem.at[prev, 1])
        if extra is not None:
            wait(extra[0].at[prev, 1], extra[1].at[prev, 1])
        use(prev)

    sums = [jnp.zeros((S, 128), F32)] * 3

    def use_a(rd):
        x0 = tok_a[rd, 0].astype(F32)
        x1 = tok_a[rd, 1].astype(F32)
        sums[0] = sums[0] + x0 * x0 + x1 * x1
        g0 = gain_a[rd, 0][0:1, :]
        g1 = gain_a[rd, 1][0:1, :]
        xg = jnp.concatenate([(x0 * g0).astype(BF16), (x1 * g1).astype(BF16)], axis=1)
        i0 = pl.ds(rows(0, rd), 128)
        i1 = pl.ds(rows(1, rd), 128)
        sums[1] = sums[1] + mm(xg, jnp.concatenate([bw_v[i0, :], bw_v[i1, :]], axis=0))
        sums[2] = sums[2] + mm(xg, jnp.concatenate([gw_v[i0, :], gw_v[i1, :]], axis=0))

    gather_and(tok_a, r_a, f_a, use_a, (gain_a, r_g, f_g))
    rstd = lax.rsqrt(jnp.sum(sums[0], axis=1, keepdims=True) / WIDTH + EPS)
    branch = (sums[1] * rstd).astype(BF16)
    gating = (sums[2] * rstd).astype(BF16).astype(F32)
    branch_v[...] = branch

    conv_out = conv_part + taps[3:4, :] * branch.astype(F32)
    conv_low = conv_out.astype(BF16)
    loads[k_rw].wait()
    loads[k_iw].wait()
    loads[k_state].wait()
    recur_gate = sigmoid(mm(conv_low, rw_v[...]) + par_v[3:4, :])
    input_gate = sigmoid(mm(conv_low, iw_v[...]) + par_v[4:5, :])
    log_decay = 8.0 * recur_gate * log_sigmoid(par_v[5:6, :])
    new_state = jnp.exp(log_decay) * state_v[...] + jnp.sqrt(expm1_neg(2.0 * log_decay)) * (
        input_gate * conv_out
    )
    nstate_v[...] = new_state
    hid_b[0, 0] = (new_state * gelu(gating)).astype(BF16)

    for d in far_first:
        rd = back_rel(d)
        send(hid_b.at[0, 0], hid_b.at[rd, 0], s_b.at[d], r_b.at[rd, 0], zdev(d))
    send(hid_b.at[0, 0], hid_b.at[0, 1], f_b.at[0], r_b.at[0, 1], partner)
    out_state = pltpu.make_async_copy(nstate_v, nstate_h, sem_o.at[0])
    out_state.start()
    out_conv = pltpu.make_async_copy(conv_v.at[1:3], nconv_h.at[0:2], sem_o.at[1])
    out_conv.start()
    out_branch = pltpu.make_async_copy(branch_v, nconv_h.at[2], sem_o.at[2])
    out_branch.start()
    loads[k_w[0]].wait()
    send(wdn.at[0, 0], wdn.at[0, 1], f_w.at[0], r_w.at[0, 1], partner)
    for rd in near_first[1:]:
        wait(wdn.at[rd, 0], r_w.at[rd, 0])
        send(wdn.at[rd, 0], wdn.at[rd, 1], f_w.at[rd], r_w.at[rd, 1], partner)
    loads[k_ow].wait()
    proj = [jnp.zeros((S, 128), F32)]

    def use_b(rd):
        h = jnp.concatenate([hid_b[rd, 0], hid_b[rd, 1]], axis=1)
        w = jnp.concatenate([ow_v[pl.ds(rows(0, rd), 128), :], ow_v[pl.ds(rows(1, rd), 128), :]], axis=0)
        proj[0] = proj[0] + mm(h, w)

    gather_and(hid_b, r_b, f_b, use_b)
    resid = (tok_a[0, 0].astype(F32) + proj[0]).astype(BF16)
    res_c[0] = resid

    for d in far_first:
        rd = back_rel(d)
        send(res_c.at[0], res_c.at[rd], s_c.at[d], r_c.at[rd], zdev(d))
    ss_row = jnp.zeros((S, 128), F32)
    for rd in near_first:
        if rd != 0:
            wait(res_c.at[rd], r_c.at[rd])
        x = res_c[rd]
        rows_out = mm(sel_v[...], x).astype(BF16)
        ysel[rd] = rows_out.reshape(EP, CAP, 128)

        def dispatch(i, carry):
            e = (me + i) % EP
            send(ysel.at[rd, e], xbuf.at[rd, me], s_d.at[rd], r_d.at[rd], (e, tp))
            return carry

        lax.fori_loop(1, EP, dispatch, 0)
        xbuf[rd, me] = ysel[rd, me]
        xf = x.astype(F32)
        ss_row = ss_row + xf * xf
        xg = (xf * gain_a[rd, 0][1:2, :]).astype(BF16)
        part = mm_nt(xg, rexp[rd])
        if rd == 0:
            lg_own[...] = part
        else:
            lg_own[...] += part
    ss_own[...] = ss_row
    send(lg_own, lg_in, s_l.at[0], r_l.at[0], partner)
    send(ss_own, ss_in, s_l.at[1], r_l.at[1], partner)

    for k in k_x:
        loads[k].wait()
    for rd in range(NZ):
        wait(wcat.at[rd, 1], r_x.at[rd, 0])
        wait(wcat.at[rd, 3], r_x.at[rd, 1])
    for n, rd in enumerate(near_first):
        wait(xbuf.at[rd, 0 : EP - 1], r_d.at[rd])
        xf = xbuf[rd].reshape(L, 128).astype(F32)
        xg = (xf * gain_a[rd, 0][1:2, :]).astype(BF16)
        part = mm_nt(xg, wcat[rd].reshape(256, 128))
        if n == 0:
            ssx_v[...] = xf * xf
            acc_v[...] = part
        else:
            ssx_v[...] += xf * xf
            acc_v[...] += part
    theirs = pl.ds(pl.multiple_of(other * HALF, HALF), HALF)
    ours = pl.ds(pl.multiple_of(c * HALF, HALF), HALF)
    send(acc_v.at[theirs], pacc_v, s_p.at[0], r_p.at[0], partner)
    send(ssx_v.at[theirs], pss_v, s_p.at[1], r_p.at[1], partner)

    wait(lg_in, r_l.at[0])
    wait(ss_in, r_l.at[1])
    ss_tot = jnp.sum(ss_own[...] + ss_in[...], axis=1, keepdims=True)
    rstd2 = lax.rsqrt(ss_tot / WIDTH + EPS)
    logits = (lg_own[...] + lg_in[...]) * rstd2
    e_exp = jnp.exp(logits[:, 0:L])
    g_exp = jnp.exp(logits[:, L : 2 * L])
    e_den = jnp.sum(e_exp * selt_v[1], axis=1, keepdims=True) * (1.0 / CAP)
    g_den = jnp.sum(g_exp, axis=1, keepdims=True) * (1.0 / (CAP * GS))
    combine = selt_v[0] * (g_exp / g_den) * (e_exp / e_den)
    comb_hi = combine.astype(BF16)
    comb_lo = (combine - comb_hi.astype(F32)).astype(BF16)

    wait(pacc_v, r_p.at[0])
    wait(pss_v, r_p.at[1])
    ss_slot = jnp.sum(ssx_v[ours, :] + pss_v[...], axis=1, keepdims=True)
    rstd_slot = lax.rsqrt(ss_slot / WIDTH + EPS)
    mine = acc_v[ours, :]
    theirs_in = pacc_v[...]
    def reorder(v):
        return jnp.concatenate([v[:, 64:128], v[:, 0:64], v[:, 192:256], v[:, 128:192]], axis=1)

    gu = (mine + reorder(theirs_in)) * rstd_slot
    gate = gu[:, 0:128]
    hid_e[0] = (gate * sigmoid(gate) * gu[:, 128:256]).astype(BF16)

    for d in far_first:
        rd = back_rel(d)
        send(hid_e.at[0], hid_e.at[rd], s_e.at[d], r_e.at[rd], zdev(d))
    for rd in range(NZ):
        wait(wdn.at[rd, 1], r_w.at[rd, 1])
    out = [None]
    for rd in near_first:
        if rd != 0:
            wait(hid_e.at[rd], r_e.at[rd])
        part = mm(hid_e[rd], wdn[rd].reshape(128, 256))
        out[0] = part if out[0] is None else out[0] + part
    y = out[0].astype(BF16)
    y_v[0] = y[:, 0:128].reshape(HS, CAP, 128)
    y_v[1] = y[:, 128:256].reshape(HS, CAP, 128)

    def give_back(i, carry):
        s = c * HS + i

        @pl.when(s != me)
        def _():
            send(y_v.at[c, i], back_v.at[me], s_f.at[i, 0], r_f.at[0], (s, tp))

        send(y_v.at[other, i], back_v.at[me], s_f.at[i, 1], r_f.at[0], (s, 2 * z + other))
        return carry

    lax.fori_loop(0, HS, give_back, 0)
    own_half = me // HS == c

    @pl.when(own_half)
    def _():
        back_v[me] = y_v[c, me - c * HS]
        wait(back_v.at[0 : EP - 1], r_f.at[0])

    @pl.when(jnp.logical_not(own_half))
    def _():
        wait(back_v, r_f.at[0])

    back = back_v[...].reshape(L, 128)
    moe = mm(comb_hi, back) + mm(comb_lo, back)
    mixed_v[...] = (res_c[0].astype(F32) + moe).astype(BF16)
    out_mixed = pltpu.make_async_copy(mixed_v, mixed_h, sem_o.at[3])
    out_mixed.start()

    for d in range(1, NZ):
        wait(gain_a.at[0, 0], s_g.at[d])
        wait(tok_a.at[0, 0], s_a.at[d])
        wait(wdn.at[0, 0], s_w.at[d])
        wait(hid_b.at[0, 0], s_b.at[d])
        wait(res_c.at[0], s_c.at[d])
        wait(hid_e.at[0], s_e.at[d])
    for rd in range(NZ):
        wait(gain_a.at[0, 0], f_g.at[rd])
        wait(tok_a.at[0, 0], f_a.at[rd])
        wait(wdn.at[0, 0], f_w.at[rd])
        wait(hid_b.at[0, 0], f_b.at[rd])
        wait(wcat.at[0, 0], s_x.at[rd, 0])
        wait(wcat.at[0, 0], s_x.at[rd, 1])
        wait(ysel.at[rd, 0 : EP - 1], s_d.at[rd])
    wait(lg_own, s_l.at[0])
    wait(ss_own, s_l.at[1])
    wait(pacc_v, s_p.at[0])
    wait(pss_v, s_p.at[1])

    def left(i, carry):
        @pl.when(c * HS + i != me)
        def _():
            wait(y_v.at[0, 0], s_f.at[i, 0])

        wait(y_v.at[0, 0], s_f.at[i, 1])
        return carry

    lax.fori_loop(0, HS, left, 0)
    out_state.wait()
    out_conv.wait()
    out_branch.wait()
    out_mixed.wait()


def on_device(
    tokens, conv_state, recur_state, norm1_gain, branch_weight, gating_weight, conv_taps, conv_bias,
    recur_weight, recur_bias, input_weight, input_bias, decay_logit, out_weight, norm2_gain,
    group_router, expert_router, routes, gate_experts, up_experts, down_experts,
):
    EP = lax.axis_size("ep")
    TPN = lax.axis_size("tp")
    NZ = TPN // 2
    S = tokens.shape[0]
    CAP = 2 * routes.shape[1] * S // EP
    GS = expert_router.shape[1] // group_router.shape[1]
    L = EP * CAP
    par = jnp.concatenate(
        [
            jnp.stack(
                [
                    norm1_gain.astype(F32),
                    norm2_gain.astype(F32),
                    conv_bias.astype(F32),
                    recur_bias,
                    input_bias,
                    decay_logit,
                ]
            ),
            conv_taps.astype(F32),
            jnp.zeros((6, 128), F32),
        ],
        axis=0,
    )
    args = (
        tokens,
        jnp.transpose(conv_state, (1, 0, 2)),
        recur_state,
        par,
        branch_weight,
        gating_weight,
        recur_weight[0],
        input_weight[0],
        out_weight,
        group_router.T,
        expert_router.T,
        routes.T,
        gate_experts[0].T,
        up_experts[0].T,
        down_experts[0],
    )
    D = TPN * 128
    V = pltpu.VMEM
    dma = pltpu.SemaphoreType.DMA
    scratch = [
        V((NZ, 2, S, 128), BF16),
        V((NZ, 2, 2, 128), F32),
        V((3, S, 128), BF16),
        V((S, 128), F32),
        V((16, 128), F32),
        V((D, 128), BF16),
        V((D, 128), BF16),
        V((128, 128), BF16),
        V((128, 128), BF16),
        V((D, 128), BF16),
        V(args[9].shape, BF16),
        V(args[10].shape, BF16),
        V((2, S), jnp.int32),
        V((NZ, 4, 64, 128), BF16),
        V((NZ, 2, 64, 256), BF16),
        V((NZ, 2, S, 128), BF16),
        V((NZ, S, 128), BF16),
        V((NZ, EP, CAP, 128), BF16),
        V((NZ, EP, CAP, 128), BF16),
        V((NZ, 2 * L, 128), BF16),
        V((S, 2 * L), F32),
        V((S, 2 * L), F32),
        V((S, 128), F32),
        V((S, 128), F32),
        V((L, 256), F32),
        V((L // 2, 256), F32),
        V((L, 128), F32),
        V((L // 2, 128), F32),
        V((NZ, L // 2, 128), BF16),
        V((2, EP // 2, CAP, 128), BF16),
        V((EP, CAP, 128), BF16),
        V((S, 128), BF16),
        V((S, 128), F32),
        V((S, 128), BF16),
        V((L, S), BF16),
        V((2, S, L), F32),
        dma((13 + 2 * NZ,)),
        dma((NZ,)), dma((NZ, 2)), dma((NZ,)),
        dma((NZ,)), dma((NZ, 2)), dma((NZ,)),
        dma((NZ,)), dma((NZ, 2)), dma((NZ,)),
        dma((NZ,)), dma((NZ, 2)), dma((NZ,)),
        dma((NZ, 2)), dma((NZ, 2)),
        dma((NZ,)), dma((NZ,)),
        dma((NZ,)), dma((NZ,)),
        dma((2,)), dma((2,)),
        dma((2,)), dma((2,)),
        dma((NZ,)), dma((NZ,)),
        dma((EP // 2, 2)), dma((1,)),
        dma((4,)),
    ]
    anyspace = pl.BlockSpec(memory_space=pl.ANY)
    mixed, new_state, new_conv = pl.pallas_call(
        functools.partial(kernel, EP, NZ, S, CAP, GS),
        out_shape=(
            jax.ShapeDtypeStruct((S, 128), BF16),
            jax.ShapeDtypeStruct((S, 128), F32),
            jax.ShapeDtypeStruct((3, S, 128), BF16),
        ),
        in_specs=[anyspace] * len(args),
        out_specs=[anyspace] * 3,
        scratch_shapes=scratch,
        compiler_params=pltpu.CompilerParams(
            collective_id=0, has_side_effects=True, vmem_limit_bytes=40 * 1024 * 1024
        ),
        name="layer",
    )(*args)
    return mixed, new_state, jnp.transpose(new_conv, (1, 0, 2))


def solution(mesh):
    return jax.shard_map(
        on_device,
        mesh=mesh,
        in_specs=(
            P("ep", "tp"),
            P("ep", None, "tp"),
            P("ep", "tp"),
            P("tp"),
            P(None, "tp"),
            P(None, "tp"),
            P(None, "tp"),
            P("tp"),
            P("tp", None, None),
            P("tp"),
            P("tp", None, None),
            P("tp"),
            P("tp"),
            P(None, "tp"),
            P("tp"),
            P(),
            P(),
            P("ep", None),
            P("ep", None, "tp"),
            P("ep", None, "tp"),
            P("ep", "tp", None),
        ),
        out_specs=(P("ep", "tp"), P("ep", "tp"), P("ep", None, "tp")),
        check_vma=False,
    )
```

```python
import functools

import jax
import jax.numpy as jnp
from jax import lax
from jax.experimental import pallas as pl
from jax.experimental.pallas import tpu as pltpu
from jax.sharding import PartitionSpec as P

EPS = 1e-06
F32 = jnp.float32
BF16 = jnp.bfloat16
MESH = pl.DeviceIdType.MESH
NT = (((1,), (1,)), ((), ()))


def mm(a, b):
    return jnp.dot(a, b, preferred_element_type=F32)


def mm_nt(a, b):
    return lax.dot_general(a, b, NT, preferred_element_type=F32)


def expm1_neg(x):
    series = x * (1.0 + x * (0.5 + x * (1.0 / 6 + x * (1.0 / 24 + x * (1.0 / 120 + x / 720)))))
    return jnp.where(x > -0.2, -series, 1.0 - jnp.exp(x))


def log_sigmoid(x):
    u = jnp.exp(-jnp.abs(x))
    w = u / (2.0 + u)
    w2 = w * w
    poly = 1.0 / 15
    for k in (13, 11, 9, 7, 5, 3, 1):
        poly = poly * w2 + 1.0 / k
    return jnp.minimum(x, 0.0) - 2.0 * w * poly


def gelu(x):
    return 0.5 * x * (1.0 + jnp.tanh(0.7978845608028654 * (x + 0.044715 * x * x * x)))


def sigmoid(x):
    return 1.0 / (1.0 + jnp.exp(-x))


def kernel(
    EP, NZ, S, CAP, GS,
    tok_h, conv_h, state_h, n1_h, n2_h, cb_h, rb_h, ib_h, dl_h, taps_h, bw_h, gw_h, rw_h, iw_h, ow_h, grt_h, ert_h, rt_h, gt_h, ut_h, dn_h,
    mixed_h, nstate_h, nconv_h,
    tok_a, gain_a, conv_v, state_v, n1_v, n2_v, cb_v, rb_v, ib_v, dl_v, taps_v, bw_v, gw_v, rw_v, iw_v, ow_v, grt_v, ert_v, rt_v, wcat, wdn,
    hid_b, res_c, ysel, xbuf, rexp, lg_own, lg_in, ss_own, ss_in, acc_v, pacc_v, ssx_v, pss_v,
    hid_e, y_v, back_v, mixed_v, nstate_v, branch_v, sel_v, selt_v,
    sem_ld, s_a, r_a, f_a, s_g, r_g, f_g, s_b, r_b, f_b, s_w, r_w, f_w, s_x, r_x,
    s_c, r_c, s_d, r_d, s_l, r_l, s_p, r_p, s_e, r_e, s_f, r_f, sem_o,
):
    me = lax.axis_index("ep")
    tp = lax.axis_index("tp")
    z = tp // 2
    c = tp % 2
    L = EP * CAP
    HALF = L // 2
    HS = EP // 2
    WIDTH = NZ * 256
    other = 1 - c
    partner = (me, 2 * z + other)

    def zdev(d):
        return (me, 2 * ((z + d) % NZ) + c)

    def zrel(rd):
        return (z + rd) % NZ

    def rows(j, rd):
        t = 2 * zrel(rd) + (c if j == 0 else other)
        return pl.multiple_of(t * 128, 128)

    def back_rel(d):
        return (NZ - d) % NZ

    far_first = sorted(range(1, NZ), key=lambda d: (-min(d, NZ - d), d))
    near_first = [0] + sorted(range(1, NZ), key=lambda d: (min(d, NZ - d), d))

    def row(ref):
        return ref[...].astype(F32).reshape(1, 128)

    def wait(ref, sem):
        pltpu.make_async_copy(ref, ref, sem).wait()

    def send(src, dst, ssem, rsem, dev):
        pltpu.make_async_remote_copy(
            src_ref=src, dst_ref=dst, send_sem=ssem, recv_sem=rsem, device_id=dev, device_id_type=MESH
        ).start()

    loads = []

    def load(src, dst):
        k = len(loads)
        cp = pltpu.make_async_copy(src, dst, sem_ld.at[k])
        cp.start()
        loads.append(cp)
        return k

    k_tok = load(tok_h, tok_a.at[0, 0])
    k_n1 = load(n1_h, n1_v)
    k_n2 = load(n2_h, n2_v)
    k_rt = load(rt_h, rt_v)

    bar = pltpu.get_barrier_semaphore()

    def sig(dev):
        pl.semaphore_signal(bar, inc=1, device_id=dev, device_id_type=MESH)

    for d in range(1, NZ):
        sig(zdev(d))
    sig(partner)

    def bar_ep(i, carry):
        e = (me + i) % EP
        sig((e, tp))
        sig((e, 2 * z + other))
        return carry

    lax.fori_loop(1, EP, bar_ep, 0)

    k_small = [load(a, b) for a, b in ((cb_h, cb_v), (rb_h, rb_v), (ib_h, ib_v), (dl_h, dl_v), (taps_h, taps_v))]
    k_conv = load(conv_h, conv_v)
    k_state = load(state_h, state_v)
    k_bw = load(bw_h, bw_v)
    k_gw = load(gw_h, gw_v)
    k_rw = load(rw_h, rw_v)
    k_iw = load(iw_h, iw_v)
    k_ow = load(ow_h, ow_v)
    k_gr = load(grt_h, grt_v)
    k_er = load(ert_h, ert_v)
    k_w = [load(dn_h.at[:, pl.ds(pl.multiple_of(z * 256, 256), 256)], wdn.at[0, 0])]
    k_x = []
    for rd in range(NZ):
        cols = pl.ds(rows(0, rd), 128)
        k_x.append(load(gt_h.at[:, cols], wcat.at[rd, 0]))
        k_x.append(load(ut_h.at[:, cols], wcat.at[rd, 2]))

    loads[k_tok].wait()
    loads[k_n1].wait()
    loads[k_n2].wait()
    gain_a[0, 0] = jnp.concatenate([row(n1_v), row(n2_v)], axis=0)

    pl.semaphore_wait(bar, (NZ - 1) + 1 + 2 * (EP - 1))

    for d in far_first:
        rd = back_rel(d)
        send(gain_a.at[0, 0], gain_a.at[rd, 0], s_g.at[d], r_g.at[rd, 0], zdev(d))
        send(tok_a.at[0, 0], tok_a.at[rd, 0], s_a.at[d], r_a.at[rd, 0], zdev(d))
    send(gain_a.at[0, 0], gain_a.at[0, 1], f_g.at[0], r_g.at[0, 1], partner)
    send(tok_a.at[0, 0], tok_a.at[0, 1], f_a.at[0], r_a.at[0, 1], partner)

    for d in far_first:
        cols = pl.ds(pl.multiple_of(((z + d) % NZ) * 256, 256), 256)
        rd = back_rel(d)
        send(dn_h.at[:, cols], wdn.at[rd, 0], s_w.at[d], r_w.at[rd, 0], zdev(d))
    for rd in range(NZ):
        cols = pl.ds(rows(1, rd), 128)
        send(gt_h.at[:, cols], wcat.at[rd, 1], s_x.at[rd, 0], r_x.at[rd, 0], partner)
        send(ut_h.at[:, cols], wcat.at[rd, 3], s_x.at[rd, 1], r_x.at[rd, 1], partner)

    loads[k_rt].wait()
    loads[k_gr].wait()
    loads[k_er].wait()
    slot_row = lax.broadcasted_iota(jnp.int32, (L, S), 0)
    r0 = rt_v[0:1, :]
    r1 = rt_v[1:2, :]
    hit = ((slot_row // CAP) == r0) | ((slot_row // CAP) == r1)
    hit_f = jnp.where(hit, 1.0, 0.0)
    hit_b = hit_f.astype(BF16)
    before = jnp.where(
        lax.broadcasted_iota(jnp.int32, (S, S), 0) < lax.broadcasted_iota(jnp.int32, (S, S), 1), 1.0, 0.0
    ).astype(BF16)
    rank = mm(hit_b, before)
    sel = jnp.where(rank == (slot_row % CAP).astype(F32), hit_f, 0.0).astype(BF16)
    sel_v[...] = sel
    eye = jnp.where(
        lax.broadcasted_iota(jnp.int32, (S, S), 0) == lax.broadcasted_iota(jnp.int32, (S, S), 1), 1.0, 0.0
    ).astype(BF16)
    selt_v[0] = mm_nt(eye, sel)
    selt_v[1] = mm_nt(eye, hit_b)
    spread_e = jnp.where(
        lax.broadcasted_iota(jnp.int32, (L, EP), 0) // CAP == lax.broadcasted_iota(jnp.int32, (L, EP), 1), 1.0, 0.0
    ).astype(BF16)
    groups = grt_h.shape[0]
    spread_g = jnp.where(
        lax.broadcasted_iota(jnp.int32, (L, groups), 0) // (CAP * GS)
        == lax.broadcasted_iota(jnp.int32, (L, groups), 1),
        1.0,
        0.0,
    ).astype(BF16)
    for rd in range(NZ):
        cols = pl.ds(rows(0, rd), 128)
        rexp[rd, 0:L] = mm(spread_e, ert_v[:, cols]).astype(BF16)
        rexp[rd, L : 2 * L] = mm(spread_g, grt_v[:, cols]).astype(BF16)
    for k in k_small:
        loads[k].wait()
    taps = taps_v[...].astype(F32)
    bias = row(cb_v)
    loads[k_conv].wait()
    conv_part = bias + sum(taps[j : j + 1, :] * conv_v[j].astype(F32) for j in range(3))

    loads[k_bw].wait()
    loads[k_gw].wait()

    def gather_and(buf, rsem, fsem, use, extra=None):
        prev = None
        for rd in near_first:
            if rd != 0:
                wait(buf.at[rd, 0], rsem.at[rd, 0])
                send(buf.at[rd, 0], buf.at[rd, 1], fsem.at[rd], rsem.at[rd, 1], partner)
                if extra is not None:
                    xb, xr, xf = extra
                    wait(xb.at[rd, 0], xr.at[rd, 0])
                    send(xb.at[rd, 0], xb.at[rd, 1], xf.at[rd], xr.at[rd, 1], partner)
            if prev is not None:
                wait(buf.at[prev, 1], rsem.at[prev, 1])
                if extra is not None:
                    wait(extra[0].at[prev, 1], extra[1].at[prev, 1])
                use(prev)
            prev = rd
        wait(buf.at[prev, 1], rsem.at[prev, 1])
        if extra is not None:
            wait(extra[0].at[prev, 1], extra[1].at[prev, 1])
        use(prev)

    sums = [jnp.zeros((S, 128), F32)] * 3

    def use_a(rd):
        x0 = tok_a[rd, 0].astype(F32)
        x1 = tok_a[rd, 1].astype(F32)
        sums[0] = sums[0] + x0 * x0 + x1 * x1
        g0 = gain_a[rd, 0][0:1, :]
        g1 = gain_a[rd, 1][0:1, :]
        xg = jnp.concatenate([(x0 * g0).astype(BF16), (x1 * g1).astype(BF16)], axis=1)
        i0 = pl.ds(rows(0, rd), 128)
        i1 = pl.ds(rows(1, rd), 128)
        sums[1] = sums[1] + mm(xg, jnp.concatenate([bw_v[i0, :], bw_v[i1, :]], axis=0))
        sums[2] = sums[2] + mm(xg, jnp.concatenate([gw_v[i0, :], gw_v[i1, :]], axis=0))

    gather_and(tok_a, r_a, f_a, use_a, (gain_a, r_g, f_g))
    rstd = lax.rsqrt(jnp.sum(sums[0], axis=1, keepdims=True) / WIDTH + EPS)
    branch = (sums[1] * rstd).astype(BF16)
    gating = (sums[2] * rstd).astype(BF16).astype(F32)
    branch_v[...] = branch

    conv_out = conv_part + taps[3:4, :] * branch.astype(F32)
    conv_low = conv_out.astype(BF16)
    loads[k_rw].wait()
    loads[k_iw].wait()
    loads[k_state].wait()
    recur_gate = sigmoid(mm(conv_low, rw_v[...]) + row(rb_v))
    input_gate = sigmoid(mm(conv_low, iw_v[...]) + row(ib_v))
    log_decay = 8.0 * recur_gate * log_sigmoid(row(dl_v))
    new_state = jnp.exp(log_decay) * state_v[...] + jnp.sqrt(expm1_neg(2.0 * log_decay)) * (
        input_gate * conv_out
    )
    nstate_v[...] = new_state
    hid_b[0, 0] = (new_state * gelu(gating)).astype(BF16)

    for d in far_first:
        rd = back_rel(d)
        send(hid_b.at[0, 0], hid_b.at[rd, 0], s_b.at[d], r_b.at[rd, 0], zdev(d))
    send(hid_b.at[0, 0], hid_b.at[0, 1], f_b.at[0], r_b.at[0, 1], partner)
    out_state = pltpu.make_async_copy(nstate_v, nstate_h, sem_o.at[0])
    out_state.start()
    out_conv = pltpu.make_async_copy(conv_v.at[1:3], nconv_h.at[0:2], sem_o.at[1])
    out_conv.start()
    out_branch = pltpu.make_async_copy(branch_v, nconv_h.at[2], sem_o.at[2])
    out_branch.start()
    loads[k_w[0]].wait()
    send(wdn.at[0, 0], wdn.at[0, 1], f_w.at[0], r_w.at[0, 1], partner)
    for rd in near_first[1:]:
        wait(wdn.at[rd, 0], r_w.at[rd, 0])
        send(wdn.at[rd, 0], wdn.at[rd, 1], f_w.at[rd], r_w.at[rd, 1], partner)
    loads[k_ow].wait()
    proj = [jnp.zeros((S, 128), F32)]

    def use_b(rd):
        h = jnp.concatenate([hid_b[rd, 0], hid_b[rd, 1]], axis=1)
        w = jnp.concatenate([ow_v[pl.ds(rows(0, rd), 128), :], ow_v[pl.ds(rows(1, rd), 128), :]], axis=0)
        proj[0] = proj[0] + mm(h, w)

    gather_and(hid_b, r_b, f_b, use_b)
    resid = (tok_a[0, 0].astype(F32) + proj[0]).astype(BF16)
    res_c[0] = resid

    for d in far_first:
        rd = back_rel(d)
        send(res_c.at[0], res_c.at[rd], s_c.at[d], r_c.at[rd], zdev(d))
    ss_row = jnp.zeros((S, 128), F32)
    for rd in near_first:
        if rd != 0:
            wait(res_c.at[rd], r_c.at[rd])
        x = res_c[rd]
        rows_out = mm(sel_v[...], x).astype(BF16)
        ysel[rd] = rows_out.reshape(EP, CAP, 128)

        def dispatch(i, carry):
            e = (me + i) % EP
            send(ysel.at[rd, e], xbuf.at[rd, me], s_d.at[rd], r_d.at[rd], (e, tp))
            return carry

        lax.fori_loop(1, EP, dispatch, 0)
        xbuf[rd, me] = ysel[rd, me]
        xf = x.astype(F32)
        ss_row = ss_row + xf * xf
        xg = (xf * gain_a[rd, 0][1:2, :]).astype(BF16)
        part = mm_nt(xg, rexp[rd])
        if rd == 0:
            lg_own[...] = part
        else:
            lg_own[...] += part
    ss_own[...] = ss_row
    send(lg_own, lg_in, s_l.at[0], r_l.at[0], partner)
    send(ss_own, ss_in, s_l.at[1], r_l.at[1], partner)

    for k in k_x:
        loads[k].wait()
    for rd in range(NZ):
        wait(wcat.at[rd, 1], r_x.at[rd, 0])
        wait(wcat.at[rd, 3], r_x.at[rd, 1])
    for n, rd in enumerate(near_first):
        wait(xbuf.at[rd, 0 : EP - 1], r_d.at[rd])
        xf = xbuf[rd].reshape(L, 128).astype(F32)
        xg = (xf * gain_a[rd, 0][1:2, :]).astype(BF16)
        part = mm_nt(xg, wcat[rd].reshape(256, 128))
        if n == 0:
            ssx_v[...] = xf * xf
            acc_v[...] = part
        else:
            ssx_v[...] += xf * xf
            acc_v[...] += part
    theirs = pl.ds(pl.multiple_of(other * HALF, HALF), HALF)
    ours = pl.ds(pl.multiple_of(c * HALF, HALF), HALF)
    send(acc_v.at[theirs], pacc_v, s_p.at[0], r_p.at[0], partner)
    send(ssx_v.at[theirs], pss_v, s_p.at[1], r_p.at[1], partner)

    wait(lg_in, r_l.at[0])
    wait(ss_in, r_l.at[1])
    ss_tot = jnp.sum(ss_own[...] + ss_in[...], axis=1, keepdims=True)
    rstd2 = lax.rsqrt(ss_tot / WIDTH + EPS)
    logits = (lg_own[...] + lg_in[...]) * rstd2
    e_exp = jnp.exp(logits[:, 0:L])
    g_exp = jnp.exp(logits[:, L : 2 * L])
    e_den = jnp.sum(e_exp * selt_v[1], axis=1, keepdims=True) * (1.0 / CAP)
    g_den = jnp.sum(g_exp, axis=1, keepdims=True) * (1.0 / (CAP * GS))
    combine = selt_v[0] * (g_exp / g_den) * (e_exp / e_den)
    comb_hi = combine.astype(BF16)
    comb_lo = (combine - comb_hi.astype(F32)).astype(BF16)

    wait(pacc_v, r_p.at[0])
    wait(pss_v, r_p.at[1])
    ss_slot = jnp.sum(ssx_v[ours, :] + pss_v[...], axis=1, keepdims=True)
    rstd_slot = lax.rsqrt(ss_slot / WIDTH + EPS)
    mine = acc_v[ours, :]
    theirs_in = pacc_v[...]
    def reorder(v):
        return jnp.concatenate([v[:, 64:128], v[:, 0:64], v[:, 192:256], v[:, 128:192]], axis=1)

    gu = (mine + reorder(theirs_in)) * rstd_slot
    gate = gu[:, 0:128]
    hid_e[0] = (gate * sigmoid(gate) * gu[:, 128:256]).astype(BF16)

    for d in far_first:
        rd = back_rel(d)
        send(hid_e.at[0], hid_e.at[rd], s_e.at[d], r_e.at[rd], zdev(d))
    for rd in range(NZ):
        wait(wdn.at[rd, 1], r_w.at[rd, 1])
    out = [None]
    for rd in near_first:
        if rd != 0:
            wait(hid_e.at[rd], r_e.at[rd])
        part = mm(hid_e[rd], wdn[rd].reshape(128, 256))
        out[0] = part if out[0] is None else out[0] + part
    y = out[0].astype(BF16)
    y_v[0] = y[:, 0:128].reshape(HS, CAP, 128)
    y_v[1] = y[:, 128:256].reshape(HS, CAP, 128)

    def give_back(i, carry):
        s = c * HS + i

        @pl.when(s != me)
        def _():
            send(y_v.at[c, i], back_v.at[me], s_f.at[i, 0], r_f.at[0], (s, tp))

        send(y_v.at[other, i], back_v.at[me], s_f.at[i, 1], r_f.at[0], (s, 2 * z + other))
        return carry

    lax.fori_loop(0, HS, give_back, 0)
    own_half = me // HS == c

    @pl.when(own_half)
    def _():
        back_v[me] = y_v[c, me - c * HS]
        wait(back_v.at[0 : EP - 1], r_f.at[0])

    @pl.when(jnp.logical_not(own_half))
    def _():
        wait(back_v, r_f.at[0])

    back = back_v[...].reshape(L, 128)
    moe = mm(comb_hi, back) + mm(comb_lo, back)
    mixed_v[...] = (res_c[0].astype(F32) + moe).astype(BF16)
    out_mixed = pltpu.make_async_copy(mixed_v, mixed_h, sem_o.at[3])
    out_mixed.start()

    for d in range(1, NZ):
        wait(gain_a.at[0, 0], s_g.at[d])
        wait(tok_a.at[0, 0], s_a.at[d])
        wait(wdn.at[0, 0], s_w.at[d])
        wait(hid_b.at[0, 0], s_b.at[d])
        wait(res_c.at[0], s_c.at[d])
        wait(hid_e.at[0], s_e.at[d])
    for rd in range(NZ):
        wait(gain_a.at[0, 0], f_g.at[rd])
        wait(tok_a.at[0, 0], f_a.at[rd])
        wait(wdn.at[0, 0], f_w.at[rd])
        wait(hid_b.at[0, 0], f_b.at[rd])
        wait(wcat.at[0, 0], s_x.at[rd, 0])
        wait(wcat.at[0, 0], s_x.at[rd, 1])
        wait(ysel.at[rd, 0 : EP - 1], s_d.at[rd])
    wait(lg_own, s_l.at[0])
    wait(ss_own, s_l.at[1])
    wait(pacc_v, s_p.at[0])
    wait(pss_v, s_p.at[1])

    def left(i, carry):
        @pl.when(c * HS + i != me)
        def _():
            wait(y_v.at[0, 0], s_f.at[i, 0])

        wait(y_v.at[0, 0], s_f.at[i, 1])
        return carry

    lax.fori_loop(0, HS, left, 0)
    out_state.wait()
    out_conv.wait()
    out_branch.wait()
    out_mixed.wait()


def on_device(
    tokens, conv_state, recur_state, norm1_gain, branch_weight, gating_weight, conv_taps, conv_bias,
    recur_weight, recur_bias, input_weight, input_bias, decay_logit, out_weight, norm2_gain,
    group_router, expert_router, routes, gate_experts, up_experts, down_experts,
):
    EP = lax.axis_size("ep")
    TPN = lax.axis_size("tp")
    NZ = TPN // 2
    S = tokens.shape[0]
    CAP = 2 * routes.shape[1] * S // EP
    GS = expert_router.shape[1] // group_router.shape[1]
    L = EP * CAP
    args = (
        tokens,
        jnp.transpose(conv_state, (1, 0, 2)),
        recur_state,
        norm1_gain,
        norm2_gain,
        conv_bias,
        recur_bias,
        input_bias,
        decay_logit,
        conv_taps,
        branch_weight,
        gating_weight,
        recur_weight[0],
        input_weight[0],
        out_weight,
        group_router.T,
        expert_router.T,
        routes.T,
        gate_experts[0].T,
        up_experts[0].T,
        down_experts[0],
    )
    D = TPN * 128
    V = pltpu.VMEM
    dma = pltpu.SemaphoreType.DMA
    scratch = [
        V((NZ, 2, S, 128), BF16),
        V((NZ, 2, 2, 128), F32),
        V((3, S, 128), BF16),
        V((S, 128), F32),
        V((128,), BF16), V((128,), BF16), V((128,), BF16),
        V((128,), F32), V((128,), F32), V((128,), F32),
        V((4, 128), BF16),
        V((D, 128), BF16),
        V((D, 128), BF16),
        V((128, 128), BF16),
        V((128, 128), BF16),
        V((D, 128), BF16),
        V(group_router.T.shape, BF16),
        V(expert_router.T.shape, BF16),
        V((2, S), jnp.int32),
        V((NZ, 4, 64, 128), BF16),
        V((NZ, 2, 64, 256), BF16),
        V((NZ, 2, S, 128), BF16),
        V((NZ, S, 128), BF16),
        V((NZ, EP, CAP, 128), BF16),
        V((NZ, EP, CAP, 128), BF16),
        V((NZ, 2 * L, 128), BF16),
        V((S, 2 * L), F32),
        V((S, 2 * L), F32),
        V((S, 128), F32),
        V((S, 128), F32),
        V((L, 256), F32),
        V((L // 2, 256), F32),
        V((L, 128), F32),
        V((L // 2, 128), F32),
        V((NZ, L // 2, 128), BF16),
        V((2, EP // 2, CAP, 128), BF16),
        V((EP, CAP, 128), BF16),
        V((S, 128), BF16),
        V((S, 128), F32),
        V((S, 128), BF16),
        V((L, S), BF16),
        V((2, S, L), F32),
        dma((20 + 2 * NZ,)),
        dma((NZ,)), dma((NZ, 2)), dma((NZ,)),
        dma((NZ,)), dma((NZ, 2)), dma((NZ,)),
        dma((NZ,)), dma((NZ, 2)), dma((NZ,)),
        dma((NZ,)), dma((NZ, 2)), dma((NZ,)),
        dma((NZ, 2)), dma((NZ, 2)),
        dma((NZ,)), dma((NZ,)),
        dma((NZ,)), dma((NZ,)),
        dma((2,)), dma((2,)),
        dma((2,)), dma((2,)),
        dma((NZ,)), dma((NZ,)),
        dma((EP // 2, 2)), dma((1,)),
        dma((4,)),
    ]
    anyspace = pl.BlockSpec(memory_space=pl.ANY)
    mixed, new_state, new_conv = pl.pallas_call(
        functools.partial(kernel, EP, NZ, S, CAP, GS),
        out_shape=(
            jax.ShapeDtypeStruct((S, 128), BF16),
            jax.ShapeDtypeStruct((S, 128), F32),
            jax.ShapeDtypeStruct((3, S, 128), BF16),
        ),
        in_specs=[anyspace] * len(args),
        out_specs=[anyspace] * 3,
        scratch_shapes=scratch,
        compiler_params=pltpu.CompilerParams(
            collective_id=0, has_side_effects=True, vmem_limit_bytes=67_000_000
        ),
        name="layer",
    )(*args)
    return mixed, new_state, jnp.transpose(new_conv, (1, 0, 2))


def solution(mesh):
    return jax.shard_map(
        on_device,
        mesh=mesh,
        in_specs=(
            P("ep", "tp"),
            P("ep", None, "tp"),
            P("ep", "tp"),
            P("tp"),
            P(None, "tp"),
            P(None, "tp"),
            P(None, "tp"),
            P("tp"),
            P("tp", None, None),
            P("tp"),
            P("tp", None, None),
            P("tp"),
            P("tp"),
            P(None, "tp"),
            P("tp"),
            P(),
            P(),
            P("ep", None),
            P("ep", None, "tp"),
            P("ep", None, "tp"),
            P("ep", "tp", None),
        ),
        out_specs=(P("ep", "tp"), P("ep", "tp"), P("ep", None, "tp")),
        check_vma=False,
    )
```

```python
import functools

import jax
import jax.numpy as jnp
from jax import lax
from jax.experimental import pallas as pl
from jax.experimental.pallas import tpu as pltpu
from jax.sharding import PartitionSpec as P

EPS = 1e-06
NEAR = 2
F32 = jnp.float32
BF16 = jnp.bfloat16
MESH = pl.DeviceIdType.MESH
NT = (((1,), (1,)), ((), ()))


def mm(a, b):
    return jnp.dot(a, b, preferred_element_type=F32)


def mm_nt(a, b):
    return lax.dot_general(a, b, NT, preferred_element_type=F32)


def expm1_neg(x):
    series = x * (1.0 + x * (0.5 + x * (1.0 / 6 + x * (1.0 / 24 + x * (1.0 / 120 + x / 720)))))
    return jnp.where(x > -0.2, -series, 1.0 - jnp.exp(x))


def log_sigmoid(x):
    u = jnp.exp(-jnp.abs(x))
    w = u / (2.0 + u)
    w2 = w * w
    poly = 1.0 / 15
    for k in (13, 11, 9, 7, 5, 3, 1):
        poly = poly * w2 + 1.0 / k
    return jnp.minimum(x, 0.0) - 2.0 * w * poly


def gelu(x):
    return 0.5 * x * (1.0 + jnp.tanh(0.7978845608028654 * (x + 0.044715 * x * x * x)))


def sigmoid(x):
    return 1.0 / (1.0 + jnp.exp(-x))


def kernel(
    EP, NZ, S, CAP, GS,
    tok_h, conv_h, state_h, n1_h, n2_h, cb_h, rb_h, ib_h, dl_h, taps_h, bw_h, gw_h, rw_h, iw_h, ow_h,
    grt_h, ert_h, rt_h, gt_h, ut_h, dn_h,
    mixed_h, nstate_h, nconv_h,
    tok_v, tok_a, gain_a, conv_v, conv_p, state_p, n1_v, n2_v, cb_v, rb_v, ib_v, dl_v, taps_v, par_v,
    bw_p, gw_p, rw_p, iw_p, ow_p, grt_v, ert_v, rt_v, wcat, wdn,
    hid_b, res_c, res_x, ysel, yfar, xbuf, xfar, rexp, lg_own, lg_in, ss_own, ss_in, acc_v, ssx_v,
    hid_e, y_v, back_v, mixed_v, nstate_v, ns_x, branch_v, br_x, sel_v, selt_v,
    sem_ld, s_a, r_a, s_g, r_g, s_b, r_b, s_w, r_w, f_w, s_x, r_x,
    s_c, r_c, s_d, r_d, s_h, r_h, s_l, r_l, s_o, r_o, s_e, r_e, s_f, r_f, sem_o,
):
    me = lax.axis_index("ep")
    tp = lax.axis_index("tp")
    z = tp // 2
    c = tp % 2
    H = S // 2
    L = EP * CAP
    HS = EP // 2
    WIDTH = NZ * 256
    other = 1 - c
    partner = (me, 2 * z + other)
    home = me // HS
    own_half = home == c
    at_me = me - home * HS
    my_rows = pl.ds(pl.multiple_of(c * H, H), H)
    its_rows = pl.ds(pl.multiple_of(other * H, H), H)

    def zdev(d):
        return (me, 2 * ((z + d) % NZ) + c)

    def zcross(d):
        return (me, 2 * ((z + d) % NZ) + other)

    def zrel(rd):
        return (z + rd) % NZ

    def rows(j, rd):
        t = 2 * zrel(rd) + (c if j == 0 else other)
        return pl.multiple_of(t * 128, 128)

    def back_rel(d):
        return (NZ - d) % NZ

    far_first = sorted(range(1, NZ), key=lambda d: (-min(d, NZ - d), d))
    near_first = [0] + sorted(range(1, NZ), key=lambda d: (min(d, NZ - d), d))
    near = [rd for rd in near_first[1:] if min(rd, NZ - rd) <= NEAR]
    far = [rd for rd in near_first[1:] if min(rd, NZ - rd) > NEAR]

    def row(ref):
        return ref[...].astype(F32).reshape(1, 128)

    def wait(ref, sem):
        pltpu.make_async_copy(ref, ref, sem).wait()

    def send(src, dst, ssem, rsem, dev):
        pltpu.make_async_remote_copy(
            src_ref=src, dst_ref=dst, send_sem=ssem, recv_sem=rsem, device_id=dev, device_id_type=MESH
        ).start()

    loads = []

    def load(src, dst):
        k = len(loads)
        cp = pltpu.make_async_copy(src, dst, sem_ld.at[k])
        cp.start()
        loads.append(cp)
        return k

    k_tok = load(tok_h, tok_v)
    k_own = load(tok_h.at[my_rows], tok_a.at[0, 0])
    k_small = [
        load(a, b)
        for a, b in (
            (n1_h, n1_v), (n2_h, n2_v), (cb_h, cb_v), (rb_h, rb_v), (ib_h, ib_v), (dl_h, dl_v), (taps_h, taps_v)
        )
    ]
    k_rt = load(rt_h, rt_v)

    bar = pltpu.get_barrier_semaphore()

    def sig(dev):
        pl.semaphore_signal(bar, inc=1, device_id=dev, device_id_type=MESH)

    for d in range(1, NZ):
        sig(zdev(d))
        sig(zcross(d))
    sig(partner)

    def bar_ep(i, carry):
        e = (me + i) % EP
        sig((e, tp))
        sig((e, 2 * z + other))
        return carry

    lax.fori_loop(1, EP, bar_ep, 0)

    k_gr = load(grt_h, grt_v)
    k_er = load(ert_h, ert_v)
    k_conv = load(conv_h.at[:, my_rows], conv_p.at[0])
    k_convo = load(conv_h.at[1:3], conv_v)
    k_state = load(state_h.at[my_rows], state_p.at[0])
    k_bw = load(bw_h, bw_p.at[0])
    k_gw = load(gw_h, gw_p.at[0])
    k_rw = load(rw_h, rw_p.at[0])
    k_iw = load(iw_h, iw_p.at[0])
    k_ow = load(ow_h, ow_p.at[0])
    k_w = load(dn_h.at[:, pl.ds(pl.multiple_of(z * 256, 256), 256)], wdn.at[0, 0])
    k_g = load(gt_h, wcat.at[0])
    k_u = load(ut_h, wcat.at[2])

    loads[k_tok].wait()
    for k in k_small:
        loads[k].wait()
    gain_a[0, 0] = jnp.concatenate([row(n1_v), row(n2_v)], axis=0)
    par_v[0, 0:4] = jnp.concatenate([row(cb_v), row(rb_v), row(ib_v), row(dl_v)], axis=0)
    par_v[0, 4:8] = taps_v[...].astype(F32)

    pl.semaphore_wait(bar, 2 * (NZ - 1) + 1 + 2 * (EP - 1))

    for d in far_first:
        rd = back_rel(d)
        send(tok_v.at[my_rows], tok_a.at[rd, 0], s_a.at[d, 0], r_a.at[rd, 0], zdev(d))
        send(tok_v.at[its_rows], tok_a.at[rd, 1], s_a.at[d, 1], r_a.at[rd, 1], zcross(d))
        send(gain_a.at[0, 0], gain_a.at[rd, 0], s_g.at[d, 0], r_g.at[rd, 0], zdev(d))
        send(gain_a.at[0, 0], gain_a.at[rd, 1], s_g.at[d, 1], r_g.at[rd, 1], zcross(d))
    send(gain_a.at[0, 0], gain_a.at[0, 1], s_g.at[0, 1], r_g.at[0, 1], partner)
    send(tok_v.at[its_rows], tok_a.at[0, 1], s_a.at[0, 1], r_a.at[0, 1], partner)

    shared = []

    def share(src, dst):
        k = len(shared)
        send(src, dst, s_x.at[k], r_x.at[k], partner)
        shared.append(dst)
        return k

    x_bw = share(bw_h, bw_p.at[1])
    x_gw = share(gw_h, gw_p.at[1])
    x_par = share(par_v.at[0], par_v.at[1])
    x_conv = share(conv_h.at[:, its_rows], conv_p.at[1])
    x_rw = share(rw_h, rw_p.at[1])
    x_iw = share(iw_h, iw_p.at[1])
    x_state = share(state_h.at[its_rows], state_p.at[1])
    x_ow = share(ow_h, ow_p.at[1])
    x_g = share(gt_h, wcat.at[1])
    x_u = share(ut_h, wcat.at[3])

    def take(*ks):
        for k in ks:
            wait(shared[k], r_x.at[k])

    def send_down(dists):
        for d in dists:
            cols = pl.ds(pl.multiple_of(((z + d) % NZ) * 256, 256), 256)
            rd = back_rel(d)
            send(dn_h.at[:, cols], wdn.at[rd, 0], s_w.at[d], r_w.at[rd, 0], zdev(d))

    send_down([d for d in far_first if min(d, NZ - d) > 2])

    loads[k_rt].wait()
    loads[k_gr].wait()
    loads[k_er].wait()
    slot_row = lax.broadcasted_iota(jnp.int32, (L, S), 0)
    r0 = rt_v[0:1, :]
    r1 = rt_v[1:2, :]
    hit = ((slot_row // CAP) == r0) | ((slot_row // CAP) == r1)
    hit_f = jnp.where(hit, 1.0, 0.0)
    hit_b = hit_f.astype(BF16)
    before = jnp.where(
        lax.broadcasted_iota(jnp.int32, (S, S), 0) < lax.broadcasted_iota(jnp.int32, (S, S), 1), 1.0, 0.0
    ).astype(BF16)
    rank = mm(hit_b, before)
    sel = jnp.where(rank == (slot_row % CAP).astype(F32), hit_f, 0.0).astype(BF16)
    sel_v[...] = sel
    eye = jnp.where(
        lax.broadcasted_iota(jnp.int32, (S, S), 0) == lax.broadcasted_iota(jnp.int32, (S, S), 1), 1.0, 0.0
    ).astype(BF16)
    selt_v[0] = mm_nt(eye, sel)
    selt_v[1] = mm_nt(eye, hit_b)
    spread_e = jnp.where(
        lax.broadcasted_iota(jnp.int32, (L, EP), 0) // CAP == lax.broadcasted_iota(jnp.int32, (L, EP), 1), 1.0, 0.0
    ).astype(BF16)
    groups = grt_h.shape[0]
    spread_g = jnp.where(
        lax.broadcasted_iota(jnp.int32, (L, groups), 0) // (CAP * GS)
        == lax.broadcasted_iota(jnp.int32, (L, groups), 1),
        1.0,
        0.0,
    ).astype(BF16)
    for rd in range(NZ):
        cols = pl.ds(rows(0, rd), 128)
        rexp[rd, 0:L] = mm(spread_e, ert_v[:, cols]).astype(BF16)
        rexp[rd, L : 2 * L] = mm(spread_g, grt_v[:, cols]).astype(BF16)
    loads[k_conv].wait()
    loads[k_own].wait()
    take(x_par, x_conv)

    def par(i):
        return jnp.concatenate([par_v[0, i : i + 1, :], par_v[1, i : i + 1, :]], axis=1)

    conv_part = par(0) + sum(
        par(4 + j) * jnp.concatenate([conv_p[0, j], conv_p[1, j]], axis=1).astype(F32) for j in range(3)
    )
    loads[k_bw].wait()
    loads[k_gw].wait()
    take(x_bw, x_gw)

    def both(w_p, rd):
        i0 = pl.ds(rows(0, rd), 128)
        i1 = pl.ds(rows(1, rd), 128)
        return jnp.concatenate(
            [
                jnp.concatenate([w_p[0, i0, :], w_p[1, i0, :]], axis=1),
                jnp.concatenate([w_p[0, i1, :], w_p[1, i1, :]], axis=1),
            ],
            axis=0,
        )

    sums = [jnp.zeros((H, 128), F32), jnp.zeros((H, 256), F32), jnp.zeros((H, 256), F32)]
    for rd in near_first:
        parts = []
        for j in range(2):
            if (rd, j) != (0, 0):
                wait(gain_a.at[rd, j], r_g.at[rd, j])
                wait(tok_a.at[rd, j], r_a.at[rd, j])
            x = tok_a[rd, j].astype(F32)
            sums[0] = sums[0] + x * x
            parts.append((x * gain_a[rd, j][0:1, :]).astype(BF16))
        xg = jnp.concatenate(parts, axis=1)
        sums[1] = sums[1] + mm(xg, both(bw_p, rd))
        sums[2] = sums[2] + mm(xg, both(gw_p, rd))
    rstd = lax.rsqrt(jnp.sum(sums[0], axis=1, keepdims=True) / WIDTH + EPS)
    branch = (sums[1] * rstd).astype(BF16)
    gating = (sums[2] * rstd).astype(BF16).astype(F32)

    conv_out = conv_part + par(7) * branch.astype(F32)
    conv_low = conv_out.astype(BF16)
    loads[k_rw].wait()
    loads[k_iw].wait()
    loads[k_state].wait()
    take(x_rw, x_iw, x_state)

    def block_map(w_p):
        return jnp.concatenate([mm(conv_low[:, 0:128], w_p[0]), mm(conv_low[:, 128:256], w_p[1])], axis=1)

    recur_gate = sigmoid(block_map(rw_p) + par(1))
    input_gate = sigmoid(block_map(iw_p) + par(2))
    log_decay = 8.0 * recur_gate * log_sigmoid(par(3))
    state = jnp.concatenate([state_p[0], state_p[1]], axis=1)
    new_state = jnp.exp(log_decay) * state + jnp.sqrt(expm1_neg(2.0 * log_decay)) * (input_gate * conv_out)
    hid_b[0] = (new_state * gelu(gating)).astype(BF16)

    for d in far_first:
        rd = back_rel(d)
        send(hid_b.at[0], hid_b.at[rd], s_b.at[d], r_b.at[rd], zdev(d))
    nstate_v[my_rows, :] = new_state[:, 0:128]
    ns_x[...] = new_state[:, 128:256]
    branch_v[my_rows, :] = branch[:, 0:128]
    br_x[...] = branch[:, 128:256]
    send_down([d for d in far_first if min(d, NZ - d) <= 2])
    send(ns_x, nstate_v.at[my_rows], s_o.at[0], r_o.at[0], partner)
    send(br_x, branch_v.at[my_rows], s_o.at[1], r_o.at[1], partner)
    loads[k_convo].wait()
    out_conv = pltpu.make_async_copy(conv_v, nconv_h.at[0:2], sem_o.at[1])
    out_conv.start()
    loads[k_ow].wait()
    take(x_ow)
    proj = None
    for rd in near_first:
        if rd != 0:
            wait(hid_b.at[rd], r_b.at[rd])
        part = mm(hid_b[rd], both(ow_p, rd))
        proj = part if proj is None else proj + part
    resid = (jnp.concatenate([tok_a[0, 0], tok_a[0, 1]], axis=1).astype(F32) + proj).astype(BF16)
    res_c[0, c] = resid[:, 0:128]
    res_x[...] = resid[:, 128:256]

    send(res_x, res_c.at[0, c], s_c.at[0, 1], r_c.at[0, 1], partner)
    for d in far_first:
        rd = back_rel(d)
        send(res_c.at[0, c], res_c.at[rd, c], s_c.at[d, 0], r_c.at[rd, 0], zdev(d))
        send(res_x, res_c.at[rd, c], s_c.at[d, 1], r_c.at[rd, 1], zcross(d))

    def select(rd):
        return mm(sel_v[...], res_c[rd].reshape(S, 128)).astype(BF16).reshape(EP, CAP, 128)

    def dispatch(src, dst, ssem, rsem):
        def one(i, carry):
            e = (me + i) % EP
            send(src.at[e], dst.at[c * HS + at_me], ssem, rsem, (e, 2 * z + home))
            return carry

        lax.fori_loop(1, EP, one, 0)

        @pl.when(own_half)
        def _():
            dst[c * HS + at_me] = src[me]

        @pl.when(jnp.logical_not(own_half))
        def _():
            send(src.at[me], dst.at[c * HS + at_me], ssem, rsem, partner)

    def wait_blocks(ref, n_own, sem):
        @pl.when(n_own)
        def _():
            wait(ref.at[0 : EP - 1], sem)

        @pl.when(jnp.logical_not(n_own))
        def _():
            wait(ref, sem)

    wait(res_c.at[0, other], r_c.at[0, 1])
    ysel[...] = select(0)
    dispatch(ysel, xbuf.at[0], s_d.at[0], r_d.at[0])
    wait_blocks(xbuf.at[0], own_half, r_d.at[0])
    for rd in sorted(near, key=lambda d: -min(d, NZ - d)):
        send(xbuf.at[0], xbuf.at[rd], s_h.at[rd], r_h.at[rd], zdev(back_rel(rd)))
    for n, rd in enumerate(far):
        wait(res_c.at[rd, c], r_c.at[rd, 0])
        wait(res_c.at[rd, other], r_c.at[rd, 1])
        yfar[:, n] = select(rd)
    if far:
        dispatch(yfar, xfar, s_d.at[1], r_d.at[1])
    for rd in near:
        wait(res_c.at[rd, c], r_c.at[rd, 0])
        wait(res_c.at[rd, other], r_c.at[rd, 1])
    ss_row = jnp.zeros((S, 128), F32)
    for rd in near_first:
        xf = res_c[rd].reshape(S, 128).astype(F32)
        ss_row = ss_row + xf * xf
        xg = (xf * gain_a[rd, 0][1:2, :]).astype(BF16)
        part = mm_nt(xg, rexp[rd])
        if rd == 0:
            lg_own[...] = part
        else:
            lg_own[...] += part
    ss_own[...] = ss_row
    send(lg_own, lg_in, s_l.at[0], r_l.at[0], partner)
    send(ss_own, ss_in, s_l.at[1], r_l.at[1], partner)
    loads[k_w].wait()
    send(wdn.at[0, 0], wdn.at[0, 1], f_w.at[0], r_w.at[0, 1], partner)
    for rd in near_first[1:]:
        wait(wdn.at[rd, 0], r_w.at[rd, 0])
        send(wdn.at[rd, 0], wdn.at[rd, 1], f_w.at[rd], r_w.at[rd, 1], partner)
    wait(ns_x, r_o.at[0])
    wait(br_x, r_o.at[1])
    out_state = pltpu.make_async_copy(nstate_v, nstate_h, sem_o.at[0])
    out_state.start()
    out_branch = pltpu.make_async_copy(branch_v, nconv_h.at[2], sem_o.at[2])
    out_branch.start()

    loads[k_g].wait()
    loads[k_u].wait()
    take(x_g, x_u)

    def expert(n, rd, halves):
        parts = []
        for p in range(2):
            xf = halves[p].astype(F32)
            if n == 0 and p == 0:
                ssx_v[...] = xf * xf
            else:
                ssx_v[...] += xf * xf
            parts.append((xf * gain_a[rd, (p + c) % 2][1:2, :]).astype(BF16))
        cols = pl.ds(pl.multiple_of(zrel(rd) * 256, 256), 256)
        part = mm_nt(jnp.concatenate(parts, axis=1), wcat[:, :, cols].reshape(256, 256))
        if n == 0:
            acc_v[...] = part
        else:
            acc_v[...] += part

    def halves_of(ref):
        return [ref[p * HS : (p + 1) * HS].reshape(HS * CAP, 128) for p in range(2)]

    expert(0, 0, halves_of(xbuf.at[0]))
    if far:
        wait_blocks(xfar, own_half, r_d.at[1])
    for n, rd in enumerate(far):
        expert(1, rd, [xfar[p * HS : (p + 1) * HS, n].reshape(HS * CAP, 128) for p in range(2)])
    for rd in near:
        wait(xbuf.at[rd], r_h.at[rd])
        expert(1, rd, halves_of(xbuf.at[rd]))
    ss_slot = jnp.sum(ssx_v[...], axis=1, keepdims=True)
    gu = acc_v[...] * lax.rsqrt(ss_slot / WIDTH + EPS)
    gate = gu[:, 0:128]
    hid_e[0] = (gate * sigmoid(gate) * gu[:, 128:256]).astype(BF16)

    for d in far_first:
        rd = back_rel(d)
        send(hid_e.at[0], hid_e.at[rd], s_e.at[d], r_e.at[rd], zdev(d))

    wait(lg_in, r_l.at[0])
    wait(ss_in, r_l.at[1])
    ss_tot = jnp.sum(ss_own[...] + ss_in[...], axis=1, keepdims=True)
    rstd2 = lax.rsqrt(ss_tot / WIDTH + EPS)
    logits = (lg_own[...] + lg_in[...]) * rstd2
    e_exp = jnp.exp(logits[:, 0:L])
    g_exp = jnp.exp(logits[:, L : 2 * L])
    e_den = jnp.sum(e_exp * selt_v[1], axis=1, keepdims=True) * (1.0 / CAP)
    g_den = jnp.sum(g_exp, axis=1, keepdims=True) * (1.0 / (CAP * GS))
    combine = selt_v[0] * (g_exp / g_den) * (e_exp / e_den)
    comb_hi = combine.astype(BF16)
    comb_lo = (combine - comb_hi.astype(F32)).astype(BF16)
    for rd in range(NZ):
        wait(wdn.at[rd, 1], r_w.at[rd, 1])
    out = None
    for rd in near_first:
        if rd != 0:
            wait(hid_e.at[rd], r_e.at[rd])
        part = mm(hid_e[rd], wdn[rd].reshape(128, 256))
        out = part if out is None else out + part
    y = out.astype(BF16)
    y_v[0] = y[:, 0:128].reshape(HS, CAP, 128)
    y_v[1] = y[:, 128:256].reshape(HS, CAP, 128)

    def give_back(i, carry):
        s = c * HS + i

        @pl.when(s != me)
        def _():
            send(y_v.at[c, i], back_v.at[me], s_f.at[i, 0], r_f.at[0], (s, tp))

        send(y_v.at[other, i], back_v.at[me], s_f.at[i, 1], r_f.at[0], (s, 2 * z + other))
        return carry

    lax.fori_loop(0, HS, give_back, 0)

    @pl.when(own_half)
    def _():
        back_v[me] = y_v[c, at_me]

    wait_blocks(back_v, own_half, r_f.at[0])
    back = back_v[...].reshape(L, 128)
    moe = mm(comb_hi, back) + mm(comb_lo, back)
    mixed_v[...] = (res_c[0].reshape(S, 128).astype(F32) + moe).astype(BF16)
    out_mixed = pltpu.make_async_copy(mixed_v, mixed_h, sem_o.at[3])
    out_mixed.start()

    for d in range(1, NZ):
        for j in range(2):
            wait(gain_a.at[0, 0], s_g.at[d, j])
            wait(tok_a.at[0, 0], s_a.at[d, j])
            wait(res_x, s_c.at[d, j])
        wait(wdn.at[0, 0], s_w.at[d])
        wait(hid_b.at[0], s_b.at[d])
        wait(hid_e.at[0], s_e.at[d])
    for rd in range(NZ):
        wait(wdn.at[0, 0], f_w.at[rd])
    wait(gain_a.at[0, 0], s_g.at[0, 1])
    wait(tok_a.at[0, 0], s_a.at[0, 1])
    wait(res_x, s_c.at[0, 1])
    for k, dst in enumerate(shared):
        wait(dst, s_x.at[k])
    wait_blocks(ysel, own_half, s_d.at[0])
    if far:
        wait_blocks(yfar, own_half, s_d.at[1])
    for rd in near:
        wait(xbuf.at[0], s_h.at[rd])
    wait(ns_x, s_o.at[0])
    wait(br_x, s_o.at[1])
    wait(lg_own, s_l.at[0])
    wait(ss_own, s_l.at[1])

    def left(i, carry):
        @pl.when(c * HS + i != me)
        def _():
            wait(y_v.at[0, 0], s_f.at[i, 0])

        wait(y_v.at[0, 0], s_f.at[i, 1])
        return carry

    lax.fori_loop(0, HS, left, 0)
    out_state.wait()
    out_conv.wait()
    out_branch.wait()
    out_mixed.wait()


def emit(a_h, b_h, c_h, ao_h, bo_h, co_h, a_v, b_v, c_v, sem):
    trios = ((a_h, a_v, ao_h), (b_h, b_v, bo_h), (c_h, c_v, co_h))
    for k, (src, mid, _) in enumerate(trios):
        pltpu.make_async_copy(src, mid, sem.at[0, k]).start()
    for k, (src, mid, dst) in enumerate(trios):
        pltpu.make_async_copy(src, mid, sem.at[0, k]).wait()
        pltpu.make_async_copy(mid, dst, sem.at[1, k]).start()
    for k, (_, mid, dst) in enumerate(trios):
        pltpu.make_async_copy(mid, dst, sem.at[1, k]).wait()


def on_device(
    tokens, conv_state, recur_state, norm1_gain, branch_weight, gating_weight, conv_taps, conv_bias,
    recur_weight, recur_bias, input_weight, input_bias, decay_logit, out_weight, norm2_gain,
    group_router, expert_router, routes, gate_experts, up_experts, down_experts,
):
    EP = lax.axis_size("ep")
    TPN = lax.axis_size("tp")
    NZ = TPN // 2
    S = tokens.shape[0]
    CAP = 2 * routes.shape[1] * S // EP
    GS = expert_router.shape[1] // group_router.shape[1]
    L = EP * CAP
    args = (
        tokens,
        jnp.transpose(conv_state, (1, 0, 2)),
        recur_state,
        norm1_gain,
        norm2_gain,
        conv_bias,
        recur_bias,
        input_bias,
        decay_logit,
        conv_taps,
        branch_weight,
        gating_weight,
        recur_weight[0],
        input_weight[0],
        out_weight,
        group_router.T,
        expert_router.T,
        routes.T,
        gate_experts[0].T,
        up_experts[0].T,
        down_experts[0],
    )
    D = TPN * 128
    V = pltpu.VMEM
    dma = pltpu.SemaphoreType.DMA
    H = S // 2
    near_count = len([d for d in range(1, NZ) if min(d, NZ - d) <= NEAR])
    NF = max(NZ - 1 - near_count, 1)
    scratch = [
        V((S, 128), BF16),
        V((NZ, 2, H, 128), BF16),
        V((NZ, 2, 2, 128), F32),
        V((2, S, 128), BF16),
        V((2, 3, H, 128), BF16),
        V((2, H, 128), F32),
        V((128,), BF16), V((128,), BF16), V((128,), BF16),
        V((128,), F32), V((128,), F32), V((128,), F32),
        V((4, 128), BF16),
        V((2, 8, 128), F32),
        V((2, D, 128), BF16),
        V((2, D, 128), BF16),
        V((2, 128, 128), BF16),
        V((2, 128, 128), BF16),
        V((2, D, 128), BF16),
        V(group_router.T.shape, BF16),
        V(expert_router.T.shape, BF16),
        V((2, S), jnp.int32),
        V((4, 64, D), BF16),
        V((NZ, 2, 64, 256), BF16),
        V((NZ, H, 256), BF16),
        V((NZ, 2, H, 128), BF16),
        V((H, 128), BF16),
        V((EP, CAP, 128), BF16),
        V((EP, NF, CAP, 128), BF16),
        V((NZ, EP, CAP, 128), BF16),
        V((EP, NF, CAP, 128), BF16),
        V((NZ, 2 * L, 128), BF16),
        V((S, 2 * L), F32),
        V((S, 2 * L), F32),
        V((S, 128), F32),
        V((S, 128), F32),
        V((L // 2, 256), F32),
        V((L // 2, 128), F32),
        V((NZ, L // 2, 128), BF16),
        V((2, EP // 2, CAP, 128), BF16),
        V((EP, CAP, 128), BF16),
        V((S, 128), BF16),
        V((S, 128), F32),
        V((H, 128), F32),
        V((S, 128), BF16),
        V((H, 128), BF16),
        V((L, S), BF16),
        V((2, S, L), F32),
        dma((24,)),
        dma((NZ, 2)), dma((NZ, 2)),
        dma((NZ, 2)), dma((NZ, 2)),
        dma((NZ,)), dma((NZ,)),
        dma((NZ,)), dma((NZ, 2)), dma((NZ,)),
        dma((10,)), dma((10,)),
        dma((NZ, 2)), dma((NZ, 2)),
        dma((2,)), dma((2,)),
        dma((NZ,)), dma((NZ,)),
        dma((2,)), dma((2,)),
        dma((2,)), dma((2,)),
        dma((NZ,)), dma((NZ,)),
        dma((EP // 2, 2)), dma((1,)),
        dma((4,)),
    ]
    anyspace = pl.BlockSpec(memory_space=pl.ANY)
    mixed, new_state, new_conv = pl.pallas_call(
        functools.partial(kernel, EP, NZ, S, CAP, GS),
        out_shape=(
            jax.ShapeDtypeStruct((S, 128), BF16),
            jax.ShapeDtypeStruct((S, 128), F32),
            jax.ShapeDtypeStruct((3, S, 128), BF16),
        ),
        in_specs=[anyspace] * len(args),
        out_specs=[anyspace] * 3,
        scratch_shapes=scratch,
        compiler_params=pltpu.CompilerParams(
            collective_id=0, has_side_effects=True, vmem_limit_bytes=67_000_000
        ),
        name="layer",
    )(*args)
    shapes = ((S, 128), (S, 128), (3, S, 128))
    types = (BF16, F32, BF16)
    mixed, new_state, new_conv = pl.pallas_call(
        emit,
        out_shape=tuple(jax.ShapeDtypeStruct(a, b) for a, b in zip(shapes, types)),
        in_specs=[anyspace] * 3,
        out_specs=[anyspace] * 3,
        scratch_shapes=[V(a, b) for a, b in zip(shapes, types)] + [dma((2, 3))],
        name="emit",
    )(mixed, new_state, new_conv)
    return mixed, new_state, jnp.transpose(new_conv, (1, 0, 2))


def solution(mesh):
    return jax.shard_map(
        on_device,
        mesh=mesh,
        in_specs=(
            P("ep", "tp"),
            P("ep", None, "tp"),
            P("ep", "tp"),
            P("tp"),
            P(None, "tp"),
            P(None, "tp"),
            P(None, "tp"),
            P("tp"),
            P("tp", None, None),
            P("tp"),
            P("tp", None, None),
            P("tp"),
            P("tp"),
            P(None, "tp"),
            P("tp"),
            P(),
            P(),
            P("ep", None),
            P("ep", None, "tp"),
            P("ep", None, "tp"),
            P("ep", "tp", None),
        ),
        out_specs=(P("ep", "tp"), P("ep", "tp"), P("ep", None, "tp")),
        check_vma=False,
    )
```

```python
import functools

import jax
import jax.numpy as jnp
from jax import lax
from jax.experimental import pallas as pl
from jax.experimental.pallas import tpu as pltpu
from jax.sharding import PartitionSpec as P

EPS = 1e-06
NEAR = 2
ENEAR = 2
BATCH_AT = 3
F32 = jnp.float32
BF16 = jnp.bfloat16
MESH = pl.DeviceIdType.MESH
NT = (((1,), (1,)), ((), ()))


def mm(a, b):
    return jnp.dot(a, b, preferred_element_type=F32)


def mm_nt(a, b):
    return lax.dot_general(a, b, NT, preferred_element_type=F32)


def expm1_neg(x):
    series = x * (1.0 + x * (0.5 + x * (1.0 / 6 + x * (1.0 / 24 + x * (1.0 / 120 + x / 720)))))
    return jnp.where(x > -0.2, -series, 1.0 - jnp.exp(x))


def log_sigmoid(x):
    u = jnp.exp(-jnp.abs(x))
    w = u / (2.0 + u)
    w2 = w * w
    poly = 1.0 / 15
    for k in (13, 11, 9, 7, 5, 3, 1):
        poly = poly * w2 + 1.0 / k
    return jnp.minimum(x, 0.0) - 2.0 * w * poly


def gelu(x):
    return 0.5 * x * (1.0 + jnp.tanh(0.7978845608028654 * (x + 0.044715 * x * x * x)))


def sigmoid(x):
    return 1.0 / (1.0 + jnp.exp(-x))


def kernel(
    EP, NZ, S, CAP, GS,
    tok_h, conv_h, state_h, n1_h, n2_h, cb_h, rb_h, ib_h, dl_h, taps_h, bw_h, gw_h, rw_h, iw_h, ow_h,
    grt_h, ert_h, rt_h, gt_h, ut_h, dn_h,
    mixed_h, nstate_h, nconv_h,
    tok_v, tok_a, gain_a, conv_v, conv_p, state_p, n1_v, n2_v, cb_v, rb_v, ib_v, dl_v, taps_v, par_v,
    bw_p, gw_p, rw_p, iw_p, ow_p, grt_v, ert_v, rt_v, wcat, dnp, wdn,
    hid_b, res_c, res_x, ysel, yfar, xbuf, xfar, rexp, lg_own, lg_in, ss_own, ss_in, acc_v, ssx_v,
    hid_e, y_v, yf_v, back_v, backf_v, moe_v, moe_in, mixed_v, nstate_v, ns_x, branch_v, br_x, sel_v, selt_v,
    sem_ld, s_a, r_a, s_g, r_g, s_b, r_b, s_w, r_w, f_w, s_x, r_x,
    s_c, r_c, s_d, r_d, s_h, r_h, s_l, r_l, s_o, r_o, s_e, r_e, s_f, r_f, s_k, r_k, s_m, r_m, sem_o,
):
    me = lax.axis_index("ep")
    tp = lax.axis_index("tp")
    z = tp // 2
    c = tp % 2
    H = S // 2
    L = EP * CAP
    HS = EP // 2
    WIDTH = NZ * 256
    other = 1 - c
    partner = (me, 2 * z + other)
    home = me // HS
    own_half = home == c
    at_me = me - home * HS
    my_rows = pl.ds(pl.multiple_of(c * H, H), H)
    its_rows = pl.ds(pl.multiple_of(other * H, H), H)

    def zdev(d):
        return (me, 2 * ((z + d) % NZ) + c)

    def zcross(d):
        return (me, 2 * ((z + d) % NZ) + other)

    def zrel(rd):
        return (z + rd) % NZ

    def rows(j, rd):
        t = 2 * zrel(rd) + (c if j == 0 else other)
        return pl.multiple_of(t * 128, 128)

    def back_rel(d):
        return (NZ - d) % NZ

    far_first = sorted(range(1, NZ), key=lambda d: (-min(d, NZ - d), d))
    near_first = [0] + sorted(range(1, NZ), key=lambda d: (min(d, NZ - d), d))
    near = [rd for rd in near_first[1:] if min(rd, NZ - rd) <= NEAR]
    far = [rd for rd in near_first[1:] if min(rd, NZ - rd) > NEAR]
    step = max(BATCH_AT, 1)
    batches = [(lo, min(lo + step, len(far))) for lo in range(0, len(far), step)]

    e_near = [rd for rd in near_first[1:] if min(rd, NZ - rd) <= ENEAR]
    e_far = [rd for rd in near_first[1:] if min(rd, NZ - rd) > ENEAR]

    def row(ref):
        return ref[...].astype(F32).reshape(1, 128)

    def wait(ref, sem):
        pltpu.make_async_copy(ref, ref, sem).wait()

    def send(src, dst, ssem, rsem, dev):
        pltpu.make_async_remote_copy(
            src_ref=src, dst_ref=dst, send_sem=ssem, recv_sem=rsem, device_id=dev, device_id_type=MESH
        ).start()

    loads = []

    def load(src, dst):
        k = len(loads)
        cp = pltpu.make_async_copy(src, dst, sem_ld.at[k])
        cp.start()
        loads.append(cp)
        return k

    k_tok = load(tok_h, tok_v)
    k_own = load(tok_h.at[my_rows], tok_a.at[0, 0])
    k_small = [
        load(a, b)
        for a, b in (
            (n1_h, n1_v), (n2_h, n2_v), (cb_h, cb_v), (rb_h, rb_v), (ib_h, ib_v), (dl_h, dl_v), (taps_h, taps_v)
        )
    ]
    k_rt = load(rt_h, rt_v)

    bar = pltpu.get_barrier_semaphore()

    def sig(dev):
        pl.semaphore_signal(bar, inc=1, device_id=dev, device_id_type=MESH)

    for d in range(1, NZ):
        sig(zdev(d))
        sig(zcross(d))
    sig(partner)

    def bar_ep(i, carry):
        e = (me + i) % EP
        sig((e, tp))
        sig((e, 2 * z + other))
        return carry

    lax.fori_loop(1, EP, bar_ep, 0)

    k_gr = load(grt_h, grt_v)
    k_er = load(ert_h, ert_v)
    k_conv = load(conv_h.at[:, my_rows], conv_p.at[0])
    k_convo = load(conv_h.at[1:3], conv_v)
    k_state = load(state_h.at[my_rows], state_p.at[0])
    k_bw = load(bw_h, bw_p.at[0])
    k_gw = load(gw_h, gw_p.at[0])
    k_rw = load(rw_h, rw_p.at[0])
    k_iw = load(iw_h, iw_p.at[0])
    k_ow = load(ow_h, ow_p.at[0])
    k_w = load(dn_h, dnp.at[0])
    k_g = load(gt_h, wcat.at[0])
    k_u = load(ut_h, wcat.at[2])

    loads[k_tok].wait()
    for k in k_small:
        loads[k].wait()
    gain_a[0, 0] = jnp.concatenate([row(n1_v), row(n2_v)], axis=0)
    par_v[0, 0:4] = jnp.concatenate([row(cb_v), row(rb_v), row(ib_v), row(dl_v)], axis=0)
    par_v[0, 4:8] = taps_v[...].astype(F32)

    pl.semaphore_wait(bar, 2 * (NZ - 1) + 1 + 2 * (EP - 1))

    for d in far_first:
        rd = back_rel(d)
        send(tok_v.at[my_rows], tok_a.at[rd, 0], s_a.at[d, 0], r_a.at[rd, 0], zdev(d))
        send(tok_v.at[its_rows], tok_a.at[rd, 1], s_a.at[d, 1], r_a.at[rd, 1], zcross(d))
        send(gain_a.at[0, 0], gain_a.at[rd, 0], s_g.at[d, 0], r_g.at[rd, 0], zdev(d))
        send(gain_a.at[0, 0], gain_a.at[rd, 1], s_g.at[d, 1], r_g.at[rd, 1], zcross(d))
    send(gain_a.at[0, 0], gain_a.at[0, 1], s_g.at[0, 1], r_g.at[0, 1], partner)
    send(tok_v.at[its_rows], tok_a.at[0, 1], s_a.at[0, 1], r_a.at[0, 1], partner)

    shared = []

    def share(src, dst):
        k = len(shared)
        send(src, dst, s_x.at[k], r_x.at[k], partner)
        shared.append(dst)
        return k

    x_bw = share(bw_h, bw_p.at[1])
    x_gw = share(gw_h, gw_p.at[1])
    x_par = share(par_v.at[0], par_v.at[1])
    x_conv = share(conv_h.at[:, its_rows], conv_p.at[1])
    x_rw = share(rw_h, rw_p.at[1])
    x_iw = share(iw_h, iw_p.at[1])
    x_state = share(state_h.at[its_rows], state_p.at[1])

    def take(*ks):
        for k in ks:
            wait(shared[k], r_x.at[k])

    def send_down(dists):
        for d in dists:
            cols = pl.ds(pl.multiple_of(((z + d) % NZ) * 256, 256), 256)
            rd = back_rel(d)
            send(dn_h.at[:, cols], wdn.at[rd, 0], s_w.at[d], r_w.at[rd, 0], zdev(d))


    loads[k_rt].wait()
    loads[k_gr].wait()
    loads[k_er].wait()
    slot_row = lax.broadcasted_iota(jnp.int32, (L, S), 0)
    r0 = rt_v[0:1, :]
    r1 = rt_v[1:2, :]
    hit = ((slot_row // CAP) == r0) | ((slot_row // CAP) == r1)
    hit_f = jnp.where(hit, 1.0, 0.0)
    hit_b = hit_f.astype(BF16)
    before = jnp.where(
        lax.broadcasted_iota(jnp.int32, (S, S), 0) < lax.broadcasted_iota(jnp.int32, (S, S), 1), 1.0, 0.0
    ).astype(BF16)
    rank = mm(hit_b, before)
    sel = jnp.where(rank == (slot_row % CAP).astype(F32), hit_f, 0.0).astype(BF16)
    sel_v[...] = sel
    eye = jnp.where(
        lax.broadcasted_iota(jnp.int32, (S, S), 0) == lax.broadcasted_iota(jnp.int32, (S, S), 1), 1.0, 0.0
    ).astype(BF16)
    selt_v[0] = mm_nt(eye, sel)
    selt_v[1] = mm_nt(eye, hit_b)
    spread_e = jnp.where(
        lax.broadcasted_iota(jnp.int32, (L, EP), 0) // CAP == lax.broadcasted_iota(jnp.int32, (L, EP), 1), 1.0, 0.0
    ).astype(BF16)
    groups = grt_h.shape[0]
    spread_g = jnp.where(
        lax.broadcasted_iota(jnp.int32, (L, groups), 0) // (CAP * GS)
        == lax.broadcasted_iota(jnp.int32, (L, groups), 1),
        1.0,
        0.0,
    ).astype(BF16)
    for rd in range(NZ):
        cols = pl.ds(rows(0, rd), 128)
        rexp[rd, 0:L] = mm(spread_e, ert_v[:, cols]).astype(BF16)
        rexp[rd, L : 2 * L] = mm(spread_g, grt_v[:, cols]).astype(BF16)
    loads[k_conv].wait()
    loads[k_own].wait()
    take(x_par, x_conv)

    def par(i):
        return jnp.concatenate([par_v[0, i : i + 1, :], par_v[1, i : i + 1, :]], axis=1)

    conv_part = par(0) + sum(
        par(4 + j) * jnp.concatenate([conv_p[0, j], conv_p[1, j]], axis=1).astype(F32) for j in range(3)
    )
    loads[k_bw].wait()
    loads[k_gw].wait()
    take(x_bw, x_gw)

    def both(w_p, rd):
        i0 = pl.ds(rows(0, rd), 128)
        i1 = pl.ds(rows(1, rd), 128)
        return jnp.concatenate(
            [
                jnp.concatenate([w_p[0, i0, :], w_p[1, i0, :]], axis=1),
                jnp.concatenate([w_p[0, i1, :], w_p[1, i1, :]], axis=1),
            ],
            axis=0,
        )

    sums = [jnp.zeros((H, 128), F32), jnp.zeros((H, 256), F32), jnp.zeros((H, 256), F32)]
    for rd in near_first:
        parts = []
        for j in range(2):
            if (rd, j) != (0, 0):
                wait(gain_a.at[rd, j], r_g.at[rd, j])
                wait(tok_a.at[rd, j], r_a.at[rd, j])
            x = tok_a[rd, j].astype(F32)
            sums[0] = sums[0] + x * x
            parts.append((x * gain_a[rd, j][0:1, :]).astype(BF16))
        xg = jnp.concatenate(parts, axis=1)
        sums[1] = sums[1] + mm(xg, both(bw_p, rd))
        sums[2] = sums[2] + mm(xg, both(gw_p, rd))
    rstd = lax.rsqrt(jnp.sum(sums[0], axis=1, keepdims=True) / WIDTH + EPS)
    branch = (sums[1] * rstd).astype(BF16)
    gating = (sums[2] * rstd).astype(BF16).astype(F32)

    conv_out = conv_part + par(7) * branch.astype(F32)
    conv_low = conv_out.astype(BF16)
    loads[k_rw].wait()
    loads[k_iw].wait()
    loads[k_state].wait()
    take(x_rw, x_iw, x_state)

    def block_map(w_p):
        return jnp.concatenate([mm(conv_low[:, 0:128], w_p[0]), mm(conv_low[:, 128:256], w_p[1])], axis=1)

    recur_gate = sigmoid(block_map(rw_p) + par(1))
    input_gate = sigmoid(block_map(iw_p) + par(2))
    log_decay = 8.0 * recur_gate * log_sigmoid(par(3))
    state = jnp.concatenate([state_p[0], state_p[1]], axis=1)
    new_state = jnp.exp(log_decay) * state + jnp.sqrt(expm1_neg(2.0 * log_decay)) * (input_gate * conv_out)
    hid_b[0] = (new_state * gelu(gating)).astype(BF16)

    for d in far_first:
        rd = back_rel(d)
        send(hid_b.at[0], hid_b.at[rd], s_b.at[d], r_b.at[rd], zdev(d))
    nstate_v[my_rows, :] = new_state[:, 0:128]
    ns_x[...] = new_state[:, 128:256]
    branch_v[my_rows, :] = branch[:, 0:128]
    br_x[...] = branch[:, 128:256]
    send_down([d for d in far_first if min(d, NZ - d) in (1, 2)])
    send(ns_x, nstate_v.at[my_rows], s_o.at[0], r_o.at[0], partner)
    send(br_x, branch_v.at[my_rows], s_o.at[1], r_o.at[1], partner)
    x_ow = share(ow_h, ow_p.at[1])
    loads[k_convo].wait()
    out_conv = pltpu.make_async_copy(conv_v, nconv_h.at[0:2], sem_o.at[1])
    out_conv.start()
    loads[k_ow].wait()
    take(x_ow)
    proj = None
    for rd in near_first:
        if rd != 0:
            wait(hid_b.at[rd], r_b.at[rd])
        part = mm(hid_b[rd], both(ow_p, rd))
        proj = part if proj is None else proj + part
    resid = (jnp.concatenate([tok_a[0, 0], tok_a[0, 1]], axis=1).astype(F32) + proj).astype(BF16)
    res_c[0, c] = resid[:, 0:128]
    res_x[...] = resid[:, 128:256]

    send(res_x, res_c.at[0, c], s_c.at[0, 1], r_c.at[0, 1], partner)
    for d in far_first:
        rd = back_rel(d)
        send(res_c.at[0, c], res_c.at[rd, c], s_c.at[d, 0], r_c.at[rd, 0], zdev(d))
        send(res_x, res_c.at[rd, c], s_c.at[d, 1], r_c.at[rd, 1], zcross(d))

    x_g = share(gt_h, wcat.at[1])
    x_u = share(ut_h, wcat.at[3])
    x_dn = share(dn_h, dnp.at[1])
    def select(rd):
        return mm(sel_v[...], res_c[rd].reshape(S, 128)).astype(BF16).reshape(EP, CAP, 128)

    def dispatch(src, dst, ssem, rsem, part=None):
        slot = c * HS + at_me

        def piece(ref, e):
            return ref.at[e] if part is None else ref.at[e, part[0] : part[1]]

        def one(i, carry):
            e = (me + i) % EP
            send(piece(src, e), piece(dst, slot), ssem, rsem, (e, 2 * z + home))
            return carry

        lax.fori_loop(1, EP, one, 0)

        @pl.when(own_half)
        def _():
            piece(dst, slot)[...] = piece(src, me)[...]

        @pl.when(jnp.logical_not(own_half))
        def _():
            send(piece(src, me), piece(dst, slot), ssem, rsem, partner)

    def wait_blocks(ref, n_own, sem, part=None):
        @pl.when(n_own)
        def _():
            wait(ref.at[0 : EP - 1] if part is None else ref.at[0 : EP - 1, part[0] : part[1]], sem)

        @pl.when(jnp.logical_not(n_own))
        def _():
            wait(ref if part is None else ref.at[:, part[0] : part[1]], sem)

    wait(res_c.at[0, other], r_c.at[0, 1])
    ysel[...] = select(0)
    dispatch(ysel, xbuf.at[0], s_d.at[0], r_d.at[0])
    for b, (lo, hi) in enumerate(batches):
        for n in range(lo, hi):
            rd = far[n]
            wait(res_c.at[rd, c], r_c.at[rd, 0])
            wait(res_c.at[rd, other], r_c.at[rd, 1])
            yfar[:, n] = select(rd)
        dispatch(yfar, xfar, s_d.at[1 + b], r_d.at[1 + b], (lo, hi))
    wait_blocks(xbuf.at[0], own_half, r_d.at[0])
    for rd in sorted(near, key=lambda d: -min(d, NZ - d)):
        send(xbuf.at[0], xbuf.at[rd], s_h.at[rd], r_h.at[rd], zdev(back_rel(rd)))
    for rd in near:
        wait(res_c.at[rd, c], r_c.at[rd, 0])
        wait(res_c.at[rd, other], r_c.at[rd, 1])
    ss_row = jnp.zeros((S, 128), F32)
    for rd in near_first:
        xf = res_c[rd].reshape(S, 128).astype(F32)
        ss_row = ss_row + xf * xf
        xg = (xf * gain_a[rd, 0][1:2, :]).astype(BF16)
        part = mm_nt(xg, rexp[rd])
        if rd == 0:
            lg_own[...] = part
        else:
            lg_own[...] += part
    ss_own[...] = ss_row
    send(lg_own, lg_in, s_l.at[0], r_l.at[0], partner)
    send(ss_own, ss_in, s_l.at[1], r_l.at[1], partner)
    for rd in e_near:
        wait(wdn.at[rd, 0], r_w.at[rd, 0])
        send(wdn.at[rd, 0], wdn.at[rd, 1], f_w.at[rd], r_w.at[rd, 1], partner)
    wait(ns_x, r_o.at[0])
    wait(br_x, r_o.at[1])
    out_state = pltpu.make_async_copy(nstate_v, nstate_h, sem_o.at[0])
    out_state.start()
    out_branch = pltpu.make_async_copy(branch_v, nconv_h.at[2], sem_o.at[2])
    out_branch.start()

    wait(lg_in, r_l.at[0])
    wait(ss_in, r_l.at[1])
    ss_tot = jnp.sum(ss_own[...] + ss_in[...], axis=1, keepdims=True)
    rstd2 = lax.rsqrt(ss_tot / WIDTH + EPS)
    logits = (lg_own[...] + lg_in[...]) * rstd2
    e_exp = jnp.exp(logits[:, 0:L])
    g_exp = jnp.exp(logits[:, L : 2 * L])
    e_den = jnp.sum(e_exp * selt_v[1], axis=1, keepdims=True) * (1.0 / CAP)
    g_den = jnp.sum(g_exp, axis=1, keepdims=True) * (1.0 / (CAP * GS))
    combine = selt_v[0] * (g_exp / g_den) * (e_exp / e_den)
    comb_hi = combine.astype(BF16)
    comb_lo = (combine - comb_hi.astype(F32)).astype(BF16)
    loads[k_g].wait()
    loads[k_u].wait()
    take(x_g, x_u)

    def expert(n, rd, halves):
        parts = []
        for p in range(2):
            xf = halves[p].astype(F32)
            if n == 0 and p == 0:
                ssx_v[...] = xf * xf
            else:
                ssx_v[...] += xf * xf
            parts.append((xf * gain_a[rd, (p + c) % 2][1:2, :]).astype(BF16))
        cols = pl.ds(pl.multiple_of(zrel(rd) * 256, 256), 256)
        part = mm_nt(jnp.concatenate(parts, axis=1), wcat[:, :, cols].reshape(256, 256))
        if n == 0:
            acc_v[...] = part
        else:
            acc_v[...] += part

    def halves_of(ref):
        return [ref[p * HS : (p + 1) * HS].reshape(HS * CAP, 128) for p in range(2)]

    expert(0, 0, halves_of(xbuf.at[0]))
    for b, (lo, hi) in enumerate(batches):
        wait_blocks(xfar, own_half, r_d.at[1 + b], (lo, hi))
        for n in range(lo, hi):
            expert(1, far[n], [xfar[p * HS : (p + 1) * HS, n].reshape(HS * CAP, 128) for p in range(2)])
    for rd in near:
        wait(xbuf.at[rd], r_h.at[rd])
        expert(1, rd, halves_of(xbuf.at[rd]))
    ss_slot = jnp.sum(ssx_v[...], axis=1, keepdims=True)
    gu = acc_v[...] * lax.rsqrt(ss_slot / WIDTH + EPS)
    gate = gu[:, 0:128]
    hid_e[0] = (gate * sigmoid(gate) * gu[:, 128:256]).astype(BF16)

    for d in far_first:
        rd = back_rel(d)
        if rd in e_near:
            send(hid_e.at[0], hid_e.at[rd], s_e.at[d], r_e.at[rd], zdev(d))

    def put(dst, y, at=()):
        for p in range(2):
            dst[(p, slice(None)) + at] = y[:, p * 128 : (p + 1) * 128].astype(BF16).reshape(HS, CAP, 128)

    def give_back(src, dst, ssem, rsem):
        def one(i, carry):
            s = c * HS + i

            @pl.when(s != me)
            def _():
                send(src.at[c, i], dst.at[me], ssem.at[i, 0], rsem, (s, tp))

            send(src.at[other, i], dst.at[me], ssem.at[i, 1], rsem, (s, 2 * z + other))
            return carry

        lax.fori_loop(0, HS, one, 0)

        @pl.when(own_half)
        def _():
            dst[me] = src[c, at_me]

    def own_down(d):
        cols = pl.ds(pl.multiple_of(zrel(d) * 256, 256), 256)
        return dnp[:, :, cols].reshape(128, 256)

    loads[k_w].wait()
    take(x_dn)
    for n, d in enumerate(e_far):
        put(yf_v, mm(hid_e[0], own_down(d)), (n,))
    if e_far:
        give_back(yf_v, backf_v, s_k, r_k.at[0])
    out = mm(hid_e[0], own_down(0))
    for rd in e_near:
        wait(wdn.at[rd, 1], r_w.at[rd, 1])
        wait(hid_e.at[rd], r_e.at[rd])
        out = out + mm(hid_e[rd], wdn[rd].reshape(128, 256))
    put(y_v, out)

    give_back(y_v, back_v, s_f, r_f.at[0])

    def combined(back):
        return mm(comb_hi, back) + mm(comb_lo, back)

    if e_far:
        wait_blocks(backf_v, own_half, r_k.at[0])
    for n, d in sorted(enumerate(e_far), key=lambda p: -min(p[1], NZ - p[1])):
        moe_v[d] = combined(backf_v[:, n].reshape(L, 128)).astype(BF16)
        rd = back_rel(d)
        send(moe_v.at[d], moe_in.at[rd], s_m.at[d], r_m.at[rd], zdev(d))
    wait_blocks(back_v, own_half, r_f.at[0])
    moe = combined(back_v[...].reshape(L, 128))
    for rd in e_far:
        wait(moe_in.at[rd], r_m.at[rd])
        moe = moe + moe_in[rd].astype(F32)
    mixed_v[...] = (res_c[0].reshape(S, 128).astype(F32) + moe).astype(BF16)
    out_mixed = pltpu.make_async_copy(mixed_v, mixed_h, sem_o.at[3])
    out_mixed.start()

    for d in range(1, NZ):
        for j in range(2):
            wait(gain_a.at[0, 0], s_g.at[d, j])
            wait(tok_a.at[0, 0], s_a.at[d, j])
            wait(res_x, s_c.at[d, j])
        if min(d, NZ - d) <= ENEAR:
            wait(wdn.at[0, 0], s_w.at[d])
            wait(hid_e.at[0], s_e.at[d])
        else:
            wait(moe_v.at[d], s_m.at[d])
        wait(hid_b.at[0], s_b.at[d])
    for rd in e_near:
        wait(wdn.at[0, 0], f_w.at[rd])
    wait(gain_a.at[0, 0], s_g.at[0, 1])
    wait(tok_a.at[0, 0], s_a.at[0, 1])
    wait(res_x, s_c.at[0, 1])
    for k, dst in enumerate(shared):
        wait(dst, s_x.at[k])
    wait_blocks(ysel, own_half, s_d.at[0])
    for b, part in enumerate(batches):
        wait_blocks(yfar, own_half, s_d.at[1 + b], part)
    for rd in near:
        wait(xbuf.at[0], s_h.at[rd])
    wait(ns_x, s_o.at[0])
    wait(br_x, s_o.at[1])
    wait(lg_own, s_l.at[0])
    wait(ss_own, s_l.at[1])

    def left(i, carry):
        @pl.when(c * HS + i != me)
        def _():
            wait(y_v.at[0, 0], s_f.at[i, 0])
            if e_far:
                wait(yf_v.at[0, 0], s_k.at[i, 0])

        wait(y_v.at[0, 0], s_f.at[i, 1])
        if e_far:
            wait(yf_v.at[0, 0], s_k.at[i, 1])
        return carry

    lax.fori_loop(0, HS, left, 0)
    out_state.wait()
    out_conv.wait()
    out_branch.wait()
    out_mixed.wait()


def emit(a_h, b_h, c_h, ao_h, bo_h, co_h, a_v, b_v, c_v, sem):
    trios = ((a_h, a_v, ao_h), (b_h, b_v, bo_h), (c_h, c_v, co_h))
    for k, (src, mid, _) in enumerate(trios):
        pltpu.make_async_copy(src, mid, sem.at[0, k]).start()
    for k, (src, mid, dst) in enumerate(trios):
        pltpu.make_async_copy(src, mid, sem.at[0, k]).wait()
        pltpu.make_async_copy(mid, dst, sem.at[1, k]).start()
    for k, (_, mid, dst) in enumerate(trios):
        pltpu.make_async_copy(mid, dst, sem.at[1, k]).wait()


def on_device(
    tokens, conv_state, recur_state, norm1_gain, branch_weight, gating_weight, conv_taps, conv_bias,
    recur_weight, recur_bias, input_weight, input_bias, decay_logit, out_weight, norm2_gain,
    group_router, expert_router, routes, gate_experts, up_experts, down_experts,
):
    EP = lax.axis_size("ep")
    TPN = lax.axis_size("tp")
    NZ = TPN // 2
    S = tokens.shape[0]
    CAP = 2 * routes.shape[1] * S // EP
    GS = expert_router.shape[1] // group_router.shape[1]
    L = EP * CAP
    args = (
        tokens,
        jnp.transpose(conv_state, (1, 0, 2)),
        recur_state,
        norm1_gain,
        norm2_gain,
        conv_bias,
        recur_bias,
        input_bias,
        decay_logit,
        conv_taps,
        branch_weight,
        gating_weight,
        recur_weight[0],
        input_weight[0],
        out_weight,
        group_router.T,
        expert_router.T,
        routes.T,
        gate_experts[0].T,
        up_experts[0].T,
        down_experts[0],
    )
    D = TPN * 128
    V = pltpu.VMEM
    dma = pltpu.SemaphoreType.DMA
    H = S // 2
    near_count = len([d for d in range(1, NZ) if min(d, NZ - d) <= NEAR])
    NF = max(NZ - 1 - near_count, 1)
    NFE = max(len([d for d in range(1, NZ) if min(d, NZ - d) > ENEAR]), 1)
    scratch = [
        V((S, 128), BF16),
        V((NZ, 2, H, 128), BF16),
        V((NZ, 2, 2, 128), F32),
        V((2, S, 128), BF16),
        V((2, 3, H, 128), BF16),
        V((2, H, 128), F32),
        V((128,), BF16), V((128,), BF16), V((128,), BF16),
        V((128,), F32), V((128,), F32), V((128,), F32),
        V((4, 128), BF16),
        V((2, 8, 128), F32),
        V((2, D, 128), BF16),
        V((2, D, 128), BF16),
        V((2, 128, 128), BF16),
        V((2, 128, 128), BF16),
        V((2, D, 128), BF16),
        V(group_router.T.shape, BF16),
        V(expert_router.T.shape, BF16),
        V((2, S), jnp.int32),
        V((4, 64, D), BF16),
        V((2, 64, D), BF16),
        V((NZ, 2, 64, 256), BF16),
        V((NZ, H, 256), BF16),
        V((NZ, 2, H, 128), BF16),
        V((H, 128), BF16),
        V((EP, CAP, 128), BF16),
        V((EP, NF, CAP, 128), BF16),
        V((NZ, EP, CAP, 128), BF16),
        V((EP, NF, CAP, 128), BF16),
        V((NZ, 2 * L, 128), BF16),
        V((S, 2 * L), F32),
        V((S, 2 * L), F32),
        V((S, 128), F32),
        V((S, 128), F32),
        V((L // 2, 256), F32),
        V((L // 2, 128), F32),
        V((NZ, L // 2, 128), BF16),
        V((2, EP // 2, CAP, 128), BF16),
        V((2, EP // 2, NFE, CAP, 128), BF16),
        V((EP, CAP, 128), BF16),
        V((EP, NFE, CAP, 128), BF16),
        V((NZ, S, 128), BF16),
        V((NZ, S, 128), BF16),
        V((S, 128), BF16),
        V((S, 128), F32),
        V((H, 128), F32),
        V((S, 128), BF16),
        V((H, 128), BF16),
        V((L, S), BF16),
        V((2, S, L), F32),
        dma((24,)),
        dma((NZ, 2)), dma((NZ, 2)),
        dma((NZ, 2)), dma((NZ, 2)),
        dma((NZ,)), dma((NZ,)),
        dma((NZ,)), dma((NZ, 2)), dma((NZ,)),
        dma((11,)), dma((11,)),
        dma((NZ, 2)), dma((NZ, 2)),
        dma((NZ,)), dma((NZ,)),
        dma((NZ,)), dma((NZ,)),
        dma((2,)), dma((2,)),
        dma((2,)), dma((2,)),
        dma((NZ,)), dma((NZ,)),
        dma((EP // 2, 2)), dma((1,)),
        dma((EP // 2, 2)), dma((1,)),
        dma((NZ,)), dma((NZ,)),
        dma((4,)),
    ]
    anyspace = pl.BlockSpec(memory_space=pl.ANY)
    mixed, new_state, new_conv = pl.pallas_call(
        functools.partial(kernel, EP, NZ, S, CAP, GS),
        out_shape=(
            jax.ShapeDtypeStruct((S, 128), BF16),
            jax.ShapeDtypeStruct((S, 128), F32),
            jax.ShapeDtypeStruct((3, S, 128), BF16),
        ),
        in_specs=[anyspace] * len(args),
        out_specs=[anyspace] * 3,
        scratch_shapes=scratch,
        compiler_params=pltpu.CompilerParams(
            collective_id=0, has_side_effects=True, vmem_limit_bytes=67_000_000
        ),
        name="layer",
    )(*args)
    shapes = ((S, 128), (S, 128), (3, S, 128))
    types = (BF16, F32, BF16)
    mixed, new_state, new_conv = pl.pallas_call(
        emit,
        out_shape=tuple(jax.ShapeDtypeStruct(a, b) for a, b in zip(shapes, types)),
        in_specs=[anyspace] * 3,
        out_specs=[anyspace] * 3,
        scratch_shapes=[V(a, b) for a, b in zip(shapes, types)] + [dma((2, 3))],
        name="emit",
    )(mixed, new_state, new_conv)
    return mixed, new_state, jnp.transpose(new_conv, (1, 0, 2))


def solution(mesh):
    return jax.shard_map(
        on_device,
        mesh=mesh,
        in_specs=(
            P("ep", "tp"),
            P("ep", None, "tp"),
            P("ep", "tp"),
            P("tp"),
            P(None, "tp"),
            P(None, "tp"),
            P(None, "tp"),
            P("tp"),
            P("tp", None, None),
            P("tp"),
            P("tp", None, None),
            P("tp"),
            P("tp"),
            P(None, "tp"),
            P("tp"),
            P(),
            P(),
            P("ep", None),
            P("ep", None, "tp"),
            P("ep", None, "tp"),
            P("ep", "tp", None),
        ),
        out_specs=(P("ep", "tp"), P("ep", "tp"), P("ep", None, "tp")),
        check_vma=False,
    )
```

```python
import functools

import jax
import jax.numpy as jnp
from jax import lax
from jax.experimental import pallas as pl
from jax.experimental.pallas import tpu as pltpu
from jax.sharding import PartitionSpec as P

EPS = 1e-06
NEAR = 2
ENEAR = 2
BATCH_AT = 3
F32 = jnp.float32
BF16 = jnp.bfloat16
MESH = pl.DeviceIdType.MESH
NT = (((1,), (1,)), ((), ()))


def mm(a, b):
    return jnp.dot(a, b, preferred_element_type=F32)


def mm_nt(a, b):
    return lax.dot_general(a, b, NT, preferred_element_type=F32)


def expm1_neg(x):
    series = x * (1.0 + x * (0.5 + x * (1.0 / 6 + x * (1.0 / 24 + x * (1.0 / 120 + x / 720)))))
    return jnp.where(x > -0.2, -series, 1.0 - jnp.exp(x))


def log_sigmoid(x):
    u = jnp.exp(-jnp.abs(x))
    w = u / (2.0 + u)
    w2 = w * w
    poly = 1.0 / 15
    for k in (13, 11, 9, 7, 5, 3, 1):
        poly = poly * w2 + 1.0 / k
    return jnp.minimum(x, 0.0) - 2.0 * w * poly


def gelu(x):
    return 0.5 * x * (1.0 + jnp.tanh(0.7978845608028654 * (x + 0.044715 * x * x * x)))


def sigmoid(x):
    return 1.0 / (1.0 + jnp.exp(-x))


def kernel(
    EP, NZ, S, CAP, GS,
    tok_h, conv_h, state_h, n1_h, n2_h, cb_h, rb_h, ib_h, dl_h, taps_h, bw_h, gw_h, rw_h, iw_h, ow_h,
    grt_h, ert_h, rt_h, gt_h, ut_h, dn_h,
    mixed_o, nstate_o, nconv_o,
    tok_v, tok_a, gain_a, conv_v, conv_p, state_p, n1_v, n2_v, cb_v, rb_v, ib_v, dl_v, taps_v, par_v,
    bw_p, gw_p, rw_p, iw_p, ow_p, grt_v, ert_v, rt_v, wcat, dnp, wdn,
    hid_b, res_c, res_x, ysel, yfar, xown, xbuf, xfar, rexp, lg_own, lg_in, ss_own, ss_in, acc_v, ssx_v,
    hid_e, y_v, yf_v, back_v, backf_v, moe_v, moe_in, nstate_v, ns_x, branch_v, br_x, sel_v, selh_v, selt_v,
    sem_ld, s_a, r_a, s_g, r_g, s_b, r_b, s_w, r_w, f_w, s_x, r_x,
    s_c, r_c, s_d, r_d, s_h, r_h, s_l, r_l, s_o, r_o, s_e, r_e, s_f, r_f, s_k, r_k, s_m, r_m,
):
    me = lax.axis_index("ep")
    tp = lax.axis_index("tp")
    z = tp // 2
    c = tp % 2
    H = S // 2
    L = EP * CAP
    HS = EP // 2
    WIDTH = NZ * 256
    other = 1 - c
    partner = (me, 2 * z + other)
    home = me // HS
    own_half = home == c
    at_me = me - home * HS
    my_rows = pl.ds(pl.multiple_of(c * H, H), H)
    its_rows = pl.ds(pl.multiple_of(other * H, H), H)

    def zdev(d):
        return (me, 2 * ((z + d) % NZ) + c)

    def zcross(d):
        return (me, 2 * ((z + d) % NZ) + other)

    def zrel(rd):
        return (z + rd) % NZ

    def rows(j, rd):
        t = 2 * zrel(rd) + (c if j == 0 else other)
        return pl.multiple_of(t * 128, 128)

    def back_rel(d):
        return (NZ - d) % NZ

    far_first = sorted(range(1, NZ), key=lambda d: (-min(d, NZ - d), d))
    near_first = [0] + sorted(range(1, NZ), key=lambda d: (min(d, NZ - d), d))
    near = [rd for rd in near_first[1:] if min(rd, NZ - rd) <= NEAR]
    far = [rd for rd in near_first[1:] if min(rd, NZ - rd) > NEAR]
    step = max(BATCH_AT, 1)
    batches = [(lo, min(lo + step, len(far))) for lo in range(0, len(far), step)]

    e_near = [rd for rd in near_first[1:] if min(rd, NZ - rd) <= ENEAR]
    e_far = [rd for rd in near_first[1:] if min(rd, NZ - rd) > ENEAR]

    def row(ref):
        return ref[...].astype(F32).reshape(1, 128)

    def wait(ref, sem):
        pltpu.make_async_copy(ref, ref, sem).wait()

    def send(src, dst, ssem, rsem, dev):
        pltpu.make_async_remote_copy(
            src_ref=src, dst_ref=dst, send_sem=ssem, recv_sem=rsem, device_id=dev, device_id_type=MESH
        ).start()

    bar = pltpu.get_barrier_semaphore()

    def sig(dev):
        pl.semaphore_signal(bar, inc=1, device_id=dev, device_id_type=MESH)

    for d in range(1, NZ):
        sig(zdev(d))
        sig(zcross(d))
    sig(partner)

    def bar_ep(i, carry):
        e = (me + i) % EP
        sig((e, tp))
        sig((e, 2 * z + other))
        return carry

    lax.fori_loop(1, EP, bar_ep, 0, unroll=True)

    loads = []

    def load(src, dst):
        k = len(loads)
        cp = pltpu.make_async_copy(src, dst, sem_ld.at[k])
        cp.start()
        loads.append(cp)
        return k

    k_tok = load(tok_h, tok_v)
    k_own = load(tok_h.at[my_rows], tok_a.at[0, 0])
    k_small = [
        load(a, b)
        for a, b in (
            (n1_h, n1_v), (n2_h, n2_v), (cb_h, cb_v), (rb_h, rb_v), (ib_h, ib_v), (dl_h, dl_v), (taps_h, taps_v)
        )
    ]
    k_rt = load(rt_h, rt_v)

    k_gr = load(grt_h, grt_v)
    k_er = load(ert_h, ert_v)
    k_conv = load(conv_h.at[:, my_rows], conv_p.at[0])
    k_convo = load(conv_h.at[1:3], conv_v)
    k_state = load(state_h.at[my_rows], state_p.at[0])
    k_bw = load(bw_h, bw_p.at[0])
    k_gw = load(gw_h, gw_p.at[0])
    k_rw = load(rw_h, rw_p.at[0])
    k_iw = load(iw_h, iw_p.at[0])
    k_ow = load(ow_h, ow_p.at[0])
    k_w = load(dn_h, dnp.at[0])
    k_g = load(gt_h, wcat.at[0])
    k_u = load(ut_h, wcat.at[2])

    loads[k_tok].wait()
    for k in k_small:
        loads[k].wait()
    gain_a[0, 0] = jnp.concatenate([row(n1_v), row(n2_v)], axis=0)
    par_v[0, 0:4] = jnp.concatenate([row(cb_v), row(rb_v), row(ib_v), row(dl_v)], axis=0)
    par_v[0, 4:8] = taps_v[...].astype(F32)

    pl.semaphore_wait(bar, 2 * (NZ - 1) + 1 + 2 * (EP - 1))

    for d in far_first:
        rd = back_rel(d)
        send(gain_a.at[0, 0], gain_a.at[rd, 0], s_g.at[d, 0], r_g.at[rd, 0], zdev(d))
        send(gain_a.at[0, 0], gain_a.at[rd, 1], s_g.at[d, 1], r_g.at[rd, 1], zcross(d))
    for d in far_first:
        rd = back_rel(d)
        send(tok_v.at[my_rows], tok_a.at[rd, 0], s_a.at[d, 0], r_a.at[rd, 0], zdev(d))
        send(tok_v.at[its_rows], tok_a.at[rd, 1], s_a.at[d, 1], r_a.at[rd, 1], zcross(d))
    send(gain_a.at[0, 0], gain_a.at[0, 1], s_g.at[0, 1], r_g.at[0, 1], partner)
    send(tok_v.at[its_rows], tok_a.at[0, 1], s_a.at[0, 1], r_a.at[0, 1], partner)

    shared = []

    def share(src, dst):
        k = len(shared)
        send(src, dst, s_x.at[k], r_x.at[k], partner)
        shared.append(dst)
        return k

    x_bw = share(bw_h, bw_p.at[1])
    x_gw = share(gw_h, gw_p.at[1])
    x_par = share(par_v.at[0], par_v.at[1])
    x_conv = share(conv_h.at[:, its_rows], conv_p.at[1])
    x_rw = share(rw_h, rw_p.at[1])
    x_iw = share(iw_h, iw_p.at[1])
    x_state = share(state_h.at[its_rows], state_p.at[1])

    def take(*ks):
        for k in ks:
            wait(shared[k], r_x.at[k])

    def send_down(dists):
        for d in dists:
            cols = pl.ds(pl.multiple_of(((z + d) % NZ) * 256, 256), 256)
            rd = back_rel(d)
            send(dn_h.at[:, cols], wdn.at[rd, 0], s_w.at[d], r_w.at[rd, 0], zdev(d))


    loads[k_rt].wait()
    loads[k_gr].wait()
    loads[k_er].wait()
    slot_row = lax.broadcasted_iota(jnp.int32, (L, S), 0)
    r0 = rt_v[0:1, :]
    r1 = rt_v[1:2, :]
    hit = ((slot_row // CAP) == r0) | ((slot_row // CAP) == r1)
    hit_f = jnp.where(hit, 1.0, 0.0)
    hit_b = hit_f.astype(BF16)
    before = jnp.where(
        lax.broadcasted_iota(jnp.int32, (S, S), 0) < lax.broadcasted_iota(jnp.int32, (S, S), 1), 1.0, 0.0
    ).astype(BF16)
    rank = mm(hit_b, before)
    sel = jnp.where(rank == (slot_row % CAP).astype(F32), hit_f, 0.0).astype(BF16)
    sel_v[...] = sel
    pick = jnp.where(
        lax.broadcasted_iota(jnp.int32, (S, H), 0) == lax.broadcasted_iota(jnp.int32, (S, H), 1) + c * H, 1.0, 0.0
    ).astype(BF16)
    selh_v[...] = mm(sel, pick).astype(BF16)
    eye = jnp.where(
        lax.broadcasted_iota(jnp.int32, (S, S), 0) == lax.broadcasted_iota(jnp.int32, (S, S), 1), 1.0, 0.0
    ).astype(BF16)
    selt_v[0] = mm_nt(eye, sel)
    selt_v[1] = mm_nt(eye, hit_b)
    spread_e = jnp.where(
        lax.broadcasted_iota(jnp.int32, (L, EP), 0) // CAP == lax.broadcasted_iota(jnp.int32, (L, EP), 1), 1.0, 0.0
    ).astype(BF16)
    groups = grt_h.shape[0]
    spread_g = jnp.where(
        lax.broadcasted_iota(jnp.int32, (L, groups), 0) // (CAP * GS)
        == lax.broadcasted_iota(jnp.int32, (L, groups), 1),
        1.0,
        0.0,
    ).astype(BF16)
    for rd in range(NZ):
        cols = pl.ds(rows(0, rd), 128)
        rexp[rd, 0:L] = mm(spread_e, ert_v[:, cols]).astype(BF16)
        rexp[rd, L : 2 * L] = mm(spread_g, grt_v[:, cols]).astype(BF16)
    loads[k_conv].wait()
    loads[k_own].wait()
    take(x_par, x_conv)

    def par(i):
        return jnp.concatenate([par_v[0, i : i + 1, :], par_v[1, i : i + 1, :]], axis=1)

    conv_part = par(0) + sum(
        par(4 + j) * jnp.concatenate([conv_p[0, j], conv_p[1, j]], axis=1).astype(F32) for j in range(3)
    )
    loads[k_bw].wait()
    loads[k_gw].wait()
    take(x_bw, x_gw)

    def both(w_p, rd):
        i0 = pl.ds(rows(0, rd), 128)
        i1 = pl.ds(rows(1, rd), 128)
        return jnp.concatenate(
            [
                jnp.concatenate([w_p[0, i0, :], w_p[1, i0, :]], axis=1),
                jnp.concatenate([w_p[0, i1, :], w_p[1, i1, :]], axis=1),
            ],
            axis=0,
        )

    sums = [jnp.zeros((H, 128), F32), jnp.zeros((H, 256), F32), jnp.zeros((H, 256), F32)]
    for rd in near_first:
        parts = []
        for j in range(2):
            if (rd, j) != (0, 0):
                wait(gain_a.at[rd, j], r_g.at[rd, j])
                wait(tok_a.at[rd, j], r_a.at[rd, j])
            x = tok_a[rd, j].astype(F32)
            sums[0] = sums[0] + x * x
            parts.append((x * gain_a[rd, j][0:1, :]).astype(BF16))
        xg = jnp.concatenate(parts, axis=1)
        sums[1] = sums[1] + mm(xg, both(bw_p, rd))
        sums[2] = sums[2] + mm(xg, both(gw_p, rd))
    rstd = lax.rsqrt(jnp.sum(sums[0], axis=1, keepdims=True) / WIDTH + EPS)
    branch = (sums[1] * rstd).astype(BF16)
    gating = (sums[2] * rstd).astype(BF16).astype(F32)

    conv_out = conv_part + par(7) * branch.astype(F32)
    conv_low = conv_out.astype(BF16)
    loads[k_rw].wait()
    loads[k_iw].wait()
    loads[k_state].wait()
    take(x_rw, x_iw, x_state)

    def block_map(w_p):
        return jnp.concatenate([mm(conv_low[:, 0:128], w_p[0]), mm(conv_low[:, 128:256], w_p[1])], axis=1)

    recur_gate = sigmoid(block_map(rw_p) + par(1))
    input_gate = sigmoid(block_map(iw_p) + par(2))
    log_decay = 8.0 * recur_gate * log_sigmoid(par(3))
    state = jnp.concatenate([state_p[0], state_p[1]], axis=1)
    new_state = jnp.exp(log_decay) * state + jnp.sqrt(expm1_neg(2.0 * log_decay)) * (input_gate * conv_out)
    hid_b[0] = (new_state * gelu(gating)).astype(BF16)

    for d in far_first:
        rd = back_rel(d)
        send(hid_b.at[0], hid_b.at[rd], s_b.at[d], r_b.at[rd], zdev(d))
    nstate_v[my_rows, :] = new_state[:, 0:128]
    ns_x[...] = new_state[:, 128:256]
    branch_v[my_rows, :] = branch[:, 0:128]
    br_x[...] = branch[:, 128:256]
    send_down([d for d in far_first if min(d, NZ - d) in (1, 2)])
    send(ns_x, nstate_v.at[my_rows], s_o.at[0], r_o.at[0], partner)
    send(br_x, branch_v.at[my_rows], s_o.at[1], r_o.at[1], partner)
    x_ow = share(ow_h, ow_p.at[1])
    loads[k_convo].wait()
    nconv_o[0:2] = conv_v[...]
    loads[k_ow].wait()
    take(x_ow)
    proj = None
    for rd in near_first:
        if rd != 0:
            wait(hid_b.at[rd], r_b.at[rd])
        part = mm(hid_b[rd], both(ow_p, rd))
        proj = part if proj is None else proj + part
    resid = (jnp.concatenate([tok_a[0, 0], tok_a[0, 1]], axis=1).astype(F32) + proj).astype(BF16)
    res_c[0, c] = resid[:, 0:128]
    res_x[...] = resid[:, 128:256]

    send(res_x, res_c.at[0, c], s_c.at[0, 1], r_c.at[0, 1], partner)
    for d in far_first:
        rd = back_rel(d)
        send(res_c.at[0, c], res_c.at[rd, c], s_c.at[d, 0], r_c.at[rd, 0], zdev(d))
        send(res_x, res_c.at[rd, c], s_c.at[d, 1], r_c.at[rd, 1], zcross(d))

    x_g = share(gt_h, wcat.at[1])
    x_u = share(ut_h, wcat.at[3])
    x_dn = share(dn_h, dnp.at[1])
    def dispatch(src, dst, ssem, rsem, part=None):
        slot = c * HS + at_me

        def piece(ref, e):
            return ref.at[e] if part is None else ref.at[e, part[0] : part[1]]

        def one(i, carry):
            e = (me + i) % EP
            send(piece(src, e), piece(dst, slot), ssem, rsem, (e, 2 * z + home))
            return carry

        lax.fori_loop(1, EP, one, 0, unroll=True)

        @pl.when(own_half)
        def _():
            piece(dst, slot)[...] = piece(src, me)[...]

        @pl.when(jnp.logical_not(own_half))
        def _():
            send(piece(src, me), piece(dst, slot), ssem, rsem, partner)

    def wait_blocks(ref, n_own, sem, part=None):
        @pl.when(n_own)
        def _():
            wait(ref.at[0 : EP - 1] if part is None else ref.at[0 : EP - 1, part[0] : part[1]], sem)

        @pl.when(jnp.logical_not(n_own))
        def _():
            wait(ref if part is None else ref.at[:, part[0] : part[1]], sem)

    for j in range(2):
        half = mm(selh_v[...], resid[:, j * 128 : (j + 1) * 128]).astype(BF16)
        ysel[:, c if j == 0 else other] = half.reshape(EP, CAP, 128)
    dispatch(ysel, xown, s_d.at[0], r_d.at[0])
    wait_blocks(xown, own_half, r_d.at[0])
    for p in range(2):
        xbuf[0, p * HS : (p + 1) * HS] = xown[0:HS, p] + xown[HS : 2 * HS, p]
    for rd in sorted(near, key=lambda d: -min(d, NZ - d)):
        send(xbuf.at[0], xbuf.at[rd], s_h.at[rd], r_h.at[rd], zdev(back_rel(rd)))
    for b, (lo, hi) in enumerate(batches):
        for n in range(lo, hi):
            rd = far[n]
            wait(res_c.at[rd, c], r_c.at[rd, 0])
            wait(res_c.at[rd, other], r_c.at[rd, 1])
        chunks = jnp.concatenate([res_c[far[n]].reshape(S, 128) for n in range(lo, hi)], axis=1)
        rows_out = mm(sel_v[...], chunks).astype(BF16)
        for n in range(lo, hi):
            yfar[:, n] = rows_out[:, (n - lo) * 128 : (n - lo + 1) * 128].reshape(EP, CAP, 128)
        dispatch(yfar, xfar, s_d.at[1 + b], r_d.at[1 + b], (lo, hi))
    wait(res_c.at[0, other], r_c.at[0, 1])
    for rd in near:
        wait(res_c.at[rd, c], r_c.at[rd, 0])
        wait(res_c.at[rd, other], r_c.at[rd, 1])
    ss_row = jnp.zeros((S, 128), F32)
    for rd in near_first:
        xf = res_c[rd].reshape(S, 128).astype(F32)
        ss_row = ss_row + xf * xf
        xg = (xf * gain_a[rd, 0][1:2, :]).astype(BF16)
        part = mm_nt(xg, rexp[rd])
        if rd == 0:
            lg_own[...] = part
        else:
            lg_own[...] += part
    ss_own[...] = ss_row
    send(lg_own, lg_in, s_l.at[0], r_l.at[0], partner)
    send(ss_own, ss_in, s_l.at[1], r_l.at[1], partner)
    for rd in e_near:
        wait(wdn.at[rd, 0], r_w.at[rd, 0])
        send(wdn.at[rd, 0], wdn.at[rd, 1], f_w.at[rd], r_w.at[rd, 1], partner)
    wait(ns_x, r_o.at[0])
    wait(br_x, r_o.at[1])
    nstate_o[...] = nstate_v[...]
    nconv_o[2] = branch_v[...]

    wait(lg_in, r_l.at[0])
    wait(ss_in, r_l.at[1])
    ss_tot = jnp.sum(ss_own[...] + ss_in[...], axis=1, keepdims=True)
    rstd2 = lax.rsqrt(ss_tot / WIDTH + EPS)
    logits = (lg_own[...] + lg_in[...]) * rstd2
    e_exp = jnp.exp(logits[:, 0:L])
    g_exp = jnp.exp(logits[:, L : 2 * L])
    e_den = jnp.sum(e_exp * selt_v[1], axis=1, keepdims=True) * (1.0 / CAP)
    g_den = jnp.sum(g_exp, axis=1, keepdims=True) * (1.0 / (CAP * GS))
    combine = selt_v[0] * (g_exp / g_den) * (e_exp / e_den)
    comb_hi = combine.astype(BF16)
    comb_lo = (combine - comb_hi.astype(F32)).astype(BF16)
    comb = jnp.concatenate([comb_hi, comb_lo], axis=0)
    loads[k_g].wait()
    loads[k_u].wait()
    take(x_g, x_u)

    def expert(first, chunks):
        squares = None if first else ssx_v[...]
        parts, weights = [], []
        for rd, halves in chunks:
            for p in range(2):
                xf = halves[p].astype(F32)
                squares = xf * xf if squares is None else squares + xf * xf
                parts.append((xf * gain_a[rd, (p + c) % 2][1:2, :]).astype(BF16))
            cols = pl.ds(pl.multiple_of(zrel(rd) * 256, 256), 256)
            weights.append(wcat[:, :, cols].reshape(256, 256))
        ssx_v[...] = squares
        part = mm_nt(jnp.concatenate(parts, axis=1), jnp.concatenate(weights, axis=1))
        if first:
            acc_v[...] = part
        else:
            acc_v[...] += part

    def halves_of(ref):
        return [ref[p * HS : (p + 1) * HS].reshape(HS * CAP, 128) for p in range(2)]

    expert(True, [(0, halves_of(xbuf.at[0]))])
    for b, (lo, hi) in enumerate(batches):
        wait_blocks(xfar, own_half, r_d.at[1 + b], (lo, hi))
        expert(
            False,
            [
                (far[n], [xfar[p * HS : (p + 1) * HS, n].reshape(HS * CAP, 128) for p in range(2)])
                for n in range(lo, hi)
            ],
        )
    for rd in near:
        wait(xbuf.at[rd], r_h.at[rd])
    if near:
        expert(False, [(rd, halves_of(xbuf.at[rd])) for rd in near])
    ss_slot = jnp.sum(ssx_v[...], axis=1, keepdims=True)
    gu = acc_v[...] * lax.rsqrt(ss_slot / WIDTH + EPS)
    gate = gu[:, 0:128]
    hid_e[0] = (gate * sigmoid(gate) * gu[:, 128:256]).astype(BF16)

    for d in far_first:
        rd = back_rel(d)
        if rd in e_near:
            send(hid_e.at[0], hid_e.at[rd], s_e.at[d], r_e.at[rd], zdev(d))

    def put(dst, y, at=()):
        for p in range(2):
            dst[(p, slice(None)) + at] = y[:, p * 128 : (p + 1) * 128].astype(BF16).reshape(HS, CAP, 128)

    def give_back(src, dst, ssem, rsem):
        def one(i, carry):
            s = c * HS + i

            @pl.when(s != me)
            def _():
                send(src.at[c, i], dst.at[me], ssem.at[i, 0], rsem, (s, tp))

            send(src.at[other, i], dst.at[me], ssem.at[i, 1], rsem, (s, 2 * z + other))
            return carry

        lax.fori_loop(0, HS, one, 0, unroll=True)

        @pl.when(own_half)
        def _():
            dst[me] = src[c, at_me]

    def own_down(d):
        cols = pl.ds(pl.multiple_of(zrel(d) * 256, 256), 256)
        return dnp[:, :, cols].reshape(128, 256)

    loads[k_w].wait()
    take(x_dn)
    for n, d in enumerate(e_far):
        put(yf_v, mm(hid_e[0], own_down(d)), (n,))
    if e_far:
        give_back(yf_v, backf_v, s_k, r_k.at[0])
    out = mm(hid_e[0], own_down(0))
    for rd in e_near:
        wait(wdn.at[rd, 1], r_w.at[rd, 1])
        wait(hid_e.at[rd], r_e.at[rd])
        out = out + mm(hid_e[rd], wdn[rd].reshape(128, 256))
    put(y_v, out)

    give_back(y_v, back_v, s_f, r_f.at[0])

    def combined(back):
        pair = mm(comb, back)
        return pair[0:S] + pair[S : 2 * S]

    if e_far:
        wait_blocks(backf_v, own_half, r_k.at[0])
        parts = combined(jnp.concatenate([backf_v[:, n].reshape(L, 128) for n in range(len(e_far))], axis=1))
    for n, d in sorted(enumerate(e_far), key=lambda p: -min(p[1], NZ - p[1])):
        moe_v[d] = parts[:, n * 128 : (n + 1) * 128].astype(BF16)
        rd = back_rel(d)
        send(moe_v.at[d], moe_in.at[rd], s_m.at[d], r_m.at[rd], zdev(d))
    for d in range(1, NZ):
        for j in range(2):
            wait(gain_a.at[0, 0], s_g.at[d, j])
            wait(tok_a.at[0, 0], s_a.at[d, j])
            wait(res_x, s_c.at[d, j])
        if min(d, NZ - d) <= ENEAR:
            wait(wdn.at[0, 0], s_w.at[d])
            wait(hid_e.at[0], s_e.at[d])
        else:
            wait(moe_v.at[d], s_m.at[d])
        wait(hid_b.at[0], s_b.at[d])
    for rd in e_near:
        wait(wdn.at[0, 0], f_w.at[rd])
    wait(gain_a.at[0, 0], s_g.at[0, 1])
    wait(tok_a.at[0, 0], s_a.at[0, 1])
    wait(res_x, s_c.at[0, 1])
    for k, dst in enumerate(shared):
        wait(dst, s_x.at[k])
    wait_blocks(ysel, own_half, s_d.at[0])
    for b, part in enumerate(batches):
        wait_blocks(yfar, own_half, s_d.at[1 + b], part)
    for rd in near:
        wait(xbuf.at[0], s_h.at[rd])
    wait(ns_x, s_o.at[0])
    wait(br_x, s_o.at[1])
    wait(lg_own, s_l.at[0])
    wait(ss_own, s_l.at[1])

    def left(i, carry):
        @pl.when(c * HS + i != me)
        def _():
            wait(y_v.at[0, 0], s_f.at[i, 0])
            if e_far:
                wait(yf_v.at[0, 0], s_k.at[i, 0])

        wait(y_v.at[0, 0], s_f.at[i, 1])
        if e_far:
            wait(yf_v.at[0, 0], s_k.at[i, 1])
        return carry

    lax.fori_loop(0, HS, left, 0)
    wait_blocks(back_v, own_half, r_f.at[0])
    moe = combined(back_v[...].reshape(L, 128))
    for rd in e_far:
        wait(moe_in.at[rd], r_m.at[rd])
        moe = moe + moe_in[rd].astype(F32)
    mixed_o[...] = (res_c[0].reshape(S, 128).astype(F32) + moe).astype(BF16)


def emit(a_v, b_v, c_v, ao_h, bo_h, co_h, sem):
    copies = [
        pltpu.make_async_copy(src, dst, sem.at[k])
        for k, (src, dst) in enumerate(((a_v, ao_h), (b_v, bo_h), (c_v, co_h)))
    ]
    for copy in copies:
        copy.start()
    for copy in copies:
        copy.wait()


def on_device(
    tokens, conv_state, recur_state, norm1_gain, branch_weight, gating_weight, conv_taps, conv_bias,
    recur_weight, recur_bias, input_weight, input_bias, decay_logit, out_weight, norm2_gain,
    group_router, expert_router, routes, gate_experts, up_experts, down_experts,
):
    EP = lax.axis_size("ep")
    TPN = lax.axis_size("tp")
    NZ = TPN // 2
    S = tokens.shape[0]
    CAP = 2 * routes.shape[1] * S // EP
    GS = expert_router.shape[1] // group_router.shape[1]
    L = EP * CAP
    args = (
        tokens,
        jnp.transpose(conv_state, (1, 0, 2)),
        recur_state,
        norm1_gain,
        norm2_gain,
        conv_bias,
        recur_bias,
        input_bias,
        decay_logit,
        conv_taps,
        branch_weight,
        gating_weight,
        recur_weight[0],
        input_weight[0],
        out_weight,
        group_router.T,
        expert_router.T,
        routes.T,
        gate_experts[0].T,
        up_experts[0].T,
        down_experts[0],
    )
    D = TPN * 128
    V = pltpu.VMEM
    dma = pltpu.SemaphoreType.DMA
    H = S // 2
    near_count = len([d for d in range(1, NZ) if min(d, NZ - d) <= NEAR])
    NF = max(NZ - 1 - near_count, 1)
    NFE = max(len([d for d in range(1, NZ) if min(d, NZ - d) > ENEAR]), 1)
    scratch = [
        V((S, 128), BF16),
        V((NZ, 2, H, 128), BF16),
        V((NZ, 2, 2, 128), F32),
        V((2, S, 128), BF16),
        V((2, 3, H, 128), BF16),
        V((2, H, 128), F32),
        V((128,), BF16), V((128,), BF16), V((128,), BF16),
        V((128,), F32), V((128,), F32), V((128,), F32),
        V((4, 128), BF16),
        V((2, 8, 128), F32),
        V((2, D, 128), BF16),
        V((2, D, 128), BF16),
        V((2, 128, 128), BF16),
        V((2, 128, 128), BF16),
        V((2, D, 128), BF16),
        V(group_router.T.shape, BF16),
        V(expert_router.T.shape, BF16),
        V((2, S), jnp.int32),
        V((4, 64, D), BF16),
        V((2, 64, D), BF16),
        V((NZ, 2, 64, 256), BF16),
        V((NZ, H, 256), BF16),
        V((NZ, 2, H, 128), BF16),
        V((H, 128), BF16),
        V((EP, 2, CAP, 128), BF16),
        V((EP, NF, CAP, 128), BF16),
        V((EP, 2, CAP, 128), BF16),
        V((NZ, EP, CAP, 128), BF16),
        V((EP, NF, CAP, 128), BF16),
        V((NZ, 2 * L, 128), BF16),
        V((S, 2 * L), F32),
        V((S, 2 * L), F32),
        V((S, 128), F32),
        V((S, 128), F32),
        V((L // 2, 256), F32),
        V((L // 2, 128), F32),
        V((NZ, L // 2, 128), BF16),
        V((2, EP // 2, CAP, 128), BF16),
        V((2, EP // 2, NFE, CAP, 128), BF16),
        V((EP, CAP, 128), BF16),
        V((EP, NFE, CAP, 128), BF16),
        V((NZ, S, 128), BF16),
        V((NZ, S, 128), BF16),
        V((S, 128), F32),
        V((H, 128), F32),
        V((S, 128), BF16),
        V((H, 128), BF16),
        V((L, S), BF16),
        V((L, H), BF16),
        V((2, S, L), F32),
        dma((24,)),
        dma((NZ, 2)), dma((NZ, 2)),
        dma((NZ, 2)), dma((NZ, 2)),
        dma((NZ,)), dma((NZ,)),
        dma((NZ,)), dma((NZ, 2)), dma((NZ,)),
        dma((11,)), dma((11,)),
        dma((NZ, 2)), dma((NZ, 2)),
        dma((NZ,)), dma((NZ,)),
        dma((NZ,)), dma((NZ,)),
        dma((2,)), dma((2,)),
        dma((2,)), dma((2,)),
        dma((NZ,)), dma((NZ,)),
        dma((EP // 2, 2)), dma((1,)),
        dma((EP // 2, 2)), dma((1,)),
        dma((NZ,)), dma((NZ,)),
    ]
    anyspace = pl.BlockSpec(memory_space=pl.ANY)
    mixed, new_state, new_conv = pl.pallas_call(
        functools.partial(kernel, EP, NZ, S, CAP, GS),
        out_shape=(
            V((S, 128), BF16),
            V((S, 128), F32),
            V((3, S, 128), BF16),
        ),
        in_specs=[anyspace] * len(args),
        out_specs=[pl.BlockSpec(memory_space=pltpu.VMEM)] * 3,
        scratch_shapes=scratch,
        compiler_params=pltpu.CompilerParams(
            collective_id=0, has_side_effects=True, vmem_limit_bytes=57000000
        ),
        name="layer",
    )(*args)
    shapes = ((S, 128), (S, 128), (3, S, 128))
    types = (BF16, F32, BF16)
    mixed, new_state, new_conv = pl.pallas_call(
        emit,
        out_shape=tuple(jax.ShapeDtypeStruct(a, b) for a, b in zip(shapes, types)),
        in_specs=[pl.BlockSpec(memory_space=pltpu.VMEM)] * 3,
        out_specs=[anyspace] * 3,
        scratch_shapes=[dma((3,))],
        compiler_params=pltpu.CompilerParams(vmem_limit_bytes=2 * 1024 * 1024),
        name="emit",
    )(mixed, new_state, new_conv)
    return mixed, new_state, jnp.transpose(new_conv, (1, 0, 2))


def solution(mesh):
    return jax.shard_map(
        on_device,
        mesh=mesh,
        in_specs=(
            P("ep", "tp"),
            P("ep", None, "tp"),
            P("ep", "tp"),
            P("tp"),
            P(None, "tp"),
            P(None, "tp"),
            P(None, "tp"),
            P("tp"),
            P("tp", None, None),
            P("tp"),
            P("tp", None, None),
            P("tp"),
            P("tp"),
            P(None, "tp"),
            P("tp"),
            P(),
            P(),
            P("ep", None),
            P("ep", None, "tp"),
            P("ep", None, "tp"),
            P("ep", "tp", None),
        ),
        out_specs=(P("ep", "tp"), P("ep", "tp"), P("ep", None, "tp")),
        check_vma=False,
    )
```

```python
import functools

import jax
import jax.numpy as jnp
from jax import lax
from jax.experimental import pallas as pl
from jax.experimental.pallas import tpu as pltpu
from jax.sharding import PartitionSpec as P

EPS = 1e-06
ENEAR = 2
BATCH_AT = 4
F32 = jnp.float32
BF16 = jnp.bfloat16
MESH = pl.DeviceIdType.MESH
NT = (((1,), (1,)), ((), ()))


def mm(a, b):
    return jnp.dot(a, b, preferred_element_type=F32)


def mm_nt(a, b):
    return lax.dot_general(a, b, NT, preferred_element_type=F32)


def expm1_neg(x):
    series = x * (1.0 + x * (0.5 + x * (1.0 / 6 + x * (1.0 / 24 + x * (1.0 / 120 + x / 720)))))
    return jnp.where(x > -0.2, -series, 1.0 - jnp.exp(x))


def log_sigmoid(x):
    u = jnp.exp(-jnp.abs(x))
    w = u / (2.0 + u)
    w2 = w * w
    poly = 1.0 / 15
    for k in (13, 11, 9, 7, 5, 3, 1):
        poly = poly * w2 + 1.0 / k
    return jnp.minimum(x, 0.0) - 2.0 * w * poly


def gelu(x):
    return 0.5 * x * (1.0 + jnp.tanh(0.7978845608028654 * (x + 0.044715 * x * x * x)))


def sigmoid(x):
    return 1.0 / (1.0 + jnp.exp(-x))


def kernel(
    EP, NZ, S, CAP, GS,
    tok_h, conv_h, state_h, n1_h, n2_h, cb_h, rb_h, ib_h, dl_h, taps_h, bw_h, gw_h, rw_h, iw_h, ow_h,
    grt_h, ert_h, rt_h, gt_h, ut_h, dn_h,
    mixed_o, nstate_o, nconv_o,
    tok_v, tok_a, gain_a, conv_v, conv_p, state_p, n1_v, n2_v, cb_v, rb_v, ib_v, dl_v, taps_v, par_v,
    bw_p, gw_p, rw_p, iw_p, ow_p, grt_v, ert_v, rt_v, wcat, dnp, wdn,
    hid_b, res_c, res_x, ysel, yfar, xown, xbuf, xfar, rexp, lg_own, lg_in, ss_own, ss_in, acc_v, ssx_v,
    hid_e, y_v, yf_v, back_v, backf_v, moe_v, moe_in, nstate_v, ns_x, branch_v, br_x, sel_v, selh_v, selt_v,
    sem_ld, s_a, r_a, s_g, r_g, s_b, r_b, s_w, r_w, f_w, s_x, r_x,
    s_c, r_c, s_d, r_d, s_h, r_h, s_l, r_l, s_o, r_o, s_e, r_e, s_f, r_f, s_k, r_k, s_m, r_m,
):
    me = lax.axis_index("ep")
    tp = lax.axis_index("tp")
    z = tp // 2
    c = tp % 2
    H = S // 2
    L = EP * CAP
    HS = EP // 2
    WIDTH = NZ * 256
    other = 1 - c
    partner = (me, 2 * z + other)
    home = me // HS
    own_half = home == c
    at_me = me - home * HS
    my_rows = pl.ds(pl.multiple_of(c * H, H), H)
    its_rows = pl.ds(pl.multiple_of(other * H, H), H)

    def zdev(d):
        return (me, 2 * ((z + d) % NZ) + c)

    def zcross(d):
        return (me, 2 * ((z + d) % NZ) + other)

    def zrel(rd):
        return (z + rd) % NZ

    def rows(j, rd):
        t = 2 * zrel(rd) + (c if j == 0 else other)
        return pl.multiple_of(t * 128, 128)

    def back_rel(d):
        return (NZ - d) % NZ

    far_first = sorted(range(1, NZ), key=lambda d: (-min(d, NZ - d), d))
    near_first = [0] + sorted(range(1, NZ), key=lambda d: (min(d, NZ - d), d))
    near = [rd for rd in near_first[1:] if min(rd, NZ - rd) <= 1]
    far = [rd for rd in near_first[1:] if min(rd, NZ - rd) > 1]
    if NZ > 4:
        by_parity = 2 + (z % 2) * (NZ - 4)
        near = [by_parity] + near
        far = [NZ - by_parity] + [rd for rd in far if min(rd, NZ - rd) > 2]
    step = max(BATCH_AT, 1)
    batches = [(lo, min(lo + step, len(far))) for lo in range(0, len(far), step)]

    e_near = [rd for rd in near_first[1:] if min(rd, NZ - rd) <= ENEAR]
    e_far = [rd for rd in near_first[1:] if min(rd, NZ - rd) > ENEAR]

    def row(ref):
        return ref[...].astype(F32).reshape(1, 128)

    def wait(ref, sem):
        pltpu.make_async_copy(ref, ref, sem).wait()

    def send(src, dst, ssem, rsem, dev):
        pltpu.make_async_remote_copy(
            src_ref=src, dst_ref=dst, send_sem=ssem, recv_sem=rsem, device_id=dev, device_id_type=MESH
        ).start()

    bar = pltpu.get_barrier_semaphore()

    def sig(dev):
        pl.semaphore_signal(bar, inc=1, device_id=dev, device_id_type=MESH)

    for d in far_first:
        sig(zdev(d))
        sig(zcross(d))

    def bar_ep(i, carry):
        e = (me + i) % EP
        sig((e, tp))
        sig((e, 2 * z + other))
        return carry

    lax.fori_loop(1, EP, bar_ep, 0, unroll=True)
    sig(partner)

    loads = []

    def load(src, dst):
        k = len(loads)
        cp = pltpu.make_async_copy(src, dst, sem_ld.at[k])
        cp.start()
        loads.append(cp)
        return k

    k_tok = load(tok_h, tok_v)
    k_own = load(tok_h.at[my_rows], tok_a.at[0, 0])
    k_small = [
        load(a, b)
        for a, b in (
            (n1_h, n1_v), (n2_h, n2_v), (cb_h, cb_v), (rb_h, rb_v), (ib_h, ib_v), (dl_h, dl_v), (taps_h, taps_v)
        )
    ]
    k_rt = load(rt_h, rt_v)

    k_gr = load(grt_h, grt_v)
    k_er = load(ert_h, ert_v)
    k_conv = load(conv_h.at[:, my_rows], conv_p.at[0])
    k_convo = load(conv_h.at[1:3], conv_v)
    k_state = load(state_h.at[my_rows], state_p.at[0])
    k_bw = load(bw_h, bw_p.at[0])
    k_gw = load(gw_h, gw_p.at[0])
    k_rw = load(rw_h, rw_p.at[0])
    k_iw = load(iw_h, iw_p.at[0])
    k_ow = load(ow_h, ow_p.at[0])
    k_w = load(dn_h, dnp.at[0])
    k_g = load(gt_h, wcat.at[0])
    k_u = load(ut_h, wcat.at[2])

    loads[k_tok].wait()
    for k in k_small:
        loads[k].wait()
    gain_a[0, 0] = jnp.concatenate([row(n1_v), row(n2_v)], axis=0)
    par_v[0, 0:4] = jnp.concatenate([row(cb_v), row(rb_v), row(ib_v), row(dl_v)], axis=0)
    par_v[0, 4:8] = taps_v[...].astype(F32)

    pl.semaphore_wait(bar, 2 * (NZ - 1) + 1 + 2 * (EP - 1))

    for d in far_first:
        rd = back_rel(d)
        send(gain_a.at[0, 0], gain_a.at[rd, 0], s_g.at[d, 0], r_g.at[rd, 0], zdev(d))
        send(gain_a.at[0, 0], gain_a.at[rd, 1], s_g.at[d, 1], r_g.at[rd, 1], zcross(d))
    for d in far_first:
        rd = back_rel(d)
        send(tok_v.at[my_rows], tok_a.at[rd, 0], s_a.at[d, 0], r_a.at[rd, 0], zdev(d))
        send(tok_v.at[its_rows], tok_a.at[rd, 1], s_a.at[d, 1], r_a.at[rd, 1], zcross(d))
    send(gain_a.at[0, 0], gain_a.at[0, 1], s_g.at[0, 1], r_g.at[0, 1], partner)
    send(tok_v.at[its_rows], tok_a.at[0, 1], s_a.at[0, 1], r_a.at[0, 1], partner)

    shared = []

    def share(src, dst):
        k = len(shared)
        send(src, dst, s_x.at[k], r_x.at[k], partner)
        shared.append(dst)
        return k

    x_bw = share(bw_h, bw_p.at[1])
    x_gw = share(gw_h, gw_p.at[1])
    x_par = share(par_v.at[0], par_v.at[1])
    x_conv = share(conv_h.at[:, its_rows], conv_p.at[1])
    x_rw = share(rw_h, rw_p.at[1])
    x_iw = share(iw_h, iw_p.at[1])
    x_state = share(state_h.at[its_rows], state_p.at[1])

    def take(*ks):
        for k in ks:
            wait(shared[k], r_x.at[k])

    def send_down(dists):
        for d in dists:
            cols = pl.ds(pl.multiple_of(((z + d) % NZ) * 256, 256), 256)
            rd = back_rel(d)
            send(dn_h.at[:, cols], wdn.at[rd, 0], s_w.at[d], r_w.at[rd, 0], zdev(d))


    loads[k_rt].wait()
    loads[k_gr].wait()
    loads[k_er].wait()
    slot_row = lax.broadcasted_iota(jnp.int32, (L, S), 0)
    r0 = rt_v[0:1, :]
    r1 = rt_v[1:2, :]
    hit = ((slot_row // CAP) == r0) | ((slot_row // CAP) == r1)
    hit_f = jnp.where(hit, 1.0, 0.0)
    hit_b = hit_f.astype(BF16)
    before = jnp.where(
        lax.broadcasted_iota(jnp.int32, (S, S), 0) < lax.broadcasted_iota(jnp.int32, (S, S), 1), 1.0, 0.0
    ).astype(BF16)
    rank = mm(hit_b, before)
    sel = jnp.where(rank == (slot_row % CAP).astype(F32), hit_f, 0.0).astype(BF16)
    sel_v[...] = sel
    pick = jnp.where(
        lax.broadcasted_iota(jnp.int32, (S, H), 0) == lax.broadcasted_iota(jnp.int32, (S, H), 1) + c * H, 1.0, 0.0
    ).astype(BF16)
    selh_v[...] = mm(sel, pick).astype(BF16)
    eye = jnp.where(
        lax.broadcasted_iota(jnp.int32, (S, S), 0) == lax.broadcasted_iota(jnp.int32, (S, S), 1), 1.0, 0.0
    ).astype(BF16)
    selt_v[0] = mm_nt(eye, sel)
    selt_v[1] = mm_nt(eye, hit_b)
    spread_e = jnp.where(
        lax.broadcasted_iota(jnp.int32, (L, EP), 0) // CAP == lax.broadcasted_iota(jnp.int32, (L, EP), 1), 1.0, 0.0
    ).astype(BF16)
    groups = grt_h.shape[0]
    spread_g = jnp.where(
        lax.broadcasted_iota(jnp.int32, (L, groups), 0) // (CAP * GS)
        == lax.broadcasted_iota(jnp.int32, (L, groups), 1),
        1.0,
        0.0,
    ).astype(BF16)
    for rd in range(NZ):
        cols = pl.ds(rows(0, rd), 128)
        rexp[rd, 0:L] = mm(spread_e, ert_v[:, cols]).astype(BF16)
        rexp[rd, L : 2 * L] = mm(spread_g, grt_v[:, cols]).astype(BF16)
    loads[k_conv].wait()
    loads[k_own].wait()
    take(x_par, x_conv)

    def par(i):
        return jnp.concatenate([par_v[0, i : i + 1, :], par_v[1, i : i + 1, :]], axis=1)

    conv_part = par(0) + sum(
        par(4 + j) * jnp.concatenate([conv_p[0, j], conv_p[1, j]], axis=1).astype(F32) for j in range(3)
    )
    base_decay = 8.0 * log_sigmoid(par(3))
    loads[k_bw].wait()
    loads[k_gw].wait()
    take(x_bw, x_gw)

    def both(w_p, rd):
        i0 = pl.ds(rows(0, rd), 128)
        i1 = pl.ds(rows(1, rd), 128)
        return jnp.concatenate(
            [
                jnp.concatenate([w_p[0, i0, :], w_p[1, i0, :]], axis=1),
                jnp.concatenate([w_p[0, i1, :], w_p[1, i1, :]], axis=1),
            ],
            axis=0,
        )

    sums = [jnp.zeros((H, 128), F32), jnp.zeros((H, 256), F32), jnp.zeros((H, 256), F32)]
    for rd in near_first:
        parts = []
        for j in range(2):
            if (rd, j) != (0, 0):
                wait(gain_a.at[rd, j], r_g.at[rd, j])
                wait(tok_a.at[rd, j], r_a.at[rd, j])
            x = tok_a[rd, j].astype(F32)
            sums[0] = sums[0] + x * x
            parts.append((x * gain_a[rd, j][0:1, :]).astype(BF16))
        xg = jnp.concatenate(parts, axis=1)
        sums[1] = sums[1] + mm(xg, both(bw_p, rd))
        sums[2] = sums[2] + mm(xg, both(gw_p, rd))
    rstd = lax.rsqrt(jnp.sum(sums[0], axis=1, keepdims=True) / WIDTH + EPS)
    branch = (sums[1] * rstd).astype(BF16)
    gating = (sums[2] * rstd).astype(BF16).astype(F32)

    conv_out = conv_part + par(7) * branch.astype(F32)
    conv_low = conv_out.astype(BF16)
    loads[k_rw].wait()
    loads[k_iw].wait()
    loads[k_state].wait()
    take(x_rw, x_iw, x_state)

    def block_map(w_p):
        return jnp.concatenate([mm(conv_low[:, 0:128], w_p[0]), mm(conv_low[:, 128:256], w_p[1])], axis=1)

    recur_gate = sigmoid(block_map(rw_p) + par(1))
    input_gate = sigmoid(block_map(iw_p) + par(2))
    log_decay = recur_gate * base_decay
    state = jnp.concatenate([state_p[0], state_p[1]], axis=1)
    new_state = jnp.exp(log_decay) * state + jnp.sqrt(expm1_neg(2.0 * log_decay)) * (input_gate * conv_out)
    hid_b[0] = (new_state * gelu(gating)).astype(BF16)

    for d in far_first:
        rd = back_rel(d)
        send(hid_b.at[0], hid_b.at[rd], s_b.at[d], r_b.at[rd], zdev(d))
    nstate_v[my_rows, :] = new_state[:, 0:128]
    ns_x[...] = new_state[:, 128:256]
    branch_v[my_rows, :] = branch[:, 0:128]
    br_x[...] = branch[:, 128:256]
    send_down([d for d in far_first if min(d, NZ - d) in (1, 2)])
    send(ns_x, nstate_v.at[my_rows], s_o.at[0], r_o.at[0], partner)
    send(br_x, branch_v.at[my_rows], s_o.at[1], r_o.at[1], partner)
    x_ow = share(ow_h, ow_p.at[1])
    loads[k_convo].wait()
    nconv_o[0:2] = conv_v[...]
    loads[k_ow].wait()
    take(x_ow)
    proj = None
    for rd in near_first:
        if rd != 0:
            wait(hid_b.at[rd], r_b.at[rd])
        part = mm(hid_b[rd], both(ow_p, rd))
        proj = part if proj is None else proj + part
    resid = (jnp.concatenate([tok_a[0, 0], tok_a[0, 1]], axis=1).astype(F32) + proj).astype(BF16)
    res_c[0, c] = resid[:, 0:128]
    res_x[...] = resid[:, 128:256]

    send(res_x, res_c.at[0, c], s_c.at[0, 1], r_c.at[0, 1], partner)
    for d in far_first:
        rd = back_rel(d)
        send(res_c.at[0, c], res_c.at[rd, c], s_c.at[d, 0], r_c.at[rd, 0], zdev(d))
        send(res_x, res_c.at[rd, c], s_c.at[d, 1], r_c.at[rd, 1], zcross(d))

    x_g = share(gt_h, wcat.at[1])
    x_u = share(ut_h, wcat.at[3])
    x_dn = share(dn_h, dnp.at[1])
    def dispatch(src, dst, ssem, rsem, part=None):
        slot = c * HS + at_me

        def piece(ref, e):
            return ref.at[e] if part is None else ref.at[e, part[0] : part[1]]

        def one(i, carry):
            e = (me + i) % EP
            send(piece(src, e), piece(dst, slot), ssem, rsem, (e, 2 * z + home))
            return carry

        lax.fori_loop(1, EP, one, 0, unroll=True)

        @pl.when(own_half)
        def _():
            piece(dst, slot)[...] = piece(src, me)[...]

        @pl.when(jnp.logical_not(own_half))
        def _():
            send(piece(src, me), piece(dst, slot), ssem, rsem, partner)

    def wait_blocks(ref, n_own, sem, part=None):
        @pl.when(n_own)
        def _():
            wait(ref.at[0 : EP - 1] if part is None else ref.at[0 : EP - 1, part[0] : part[1]], sem)

        @pl.when(jnp.logical_not(n_own))
        def _():
            wait(ref if part is None else ref.at[:, part[0] : part[1]], sem)

    for j in range(2):
        half = mm(selh_v[...], resid[:, j * 128 : (j + 1) * 128]).astype(BF16)
        ysel[:, c if j == 0 else other] = half.reshape(EP, CAP, 128)
    dispatch(ysel, xown, s_d.at[0], r_d.at[0])
    for b, (lo, hi) in enumerate(batches):
        for n in range(lo, hi):
            rd = far[n]
            wait(res_c.at[rd, c], r_c.at[rd, 0])
            wait(res_c.at[rd, other], r_c.at[rd, 1])
        chunks = jnp.concatenate([res_c[far[n]].reshape(S, 128) for n in range(lo, hi)], axis=1)
        rows_out = mm(sel_v[...], chunks).astype(BF16)
        for n in range(lo, hi):
            yfar[:, n] = rows_out[:, (n - lo) * 128 : (n - lo + 1) * 128].reshape(EP, CAP, 128)
        dispatch(yfar, xfar, s_d.at[1 + b], r_d.at[1 + b], (lo, hi))
    wait_blocks(xown, own_half, r_d.at[0])
    for p in range(2):
        xbuf[0, p * HS : (p + 1) * HS] = xown[0:HS, p] + xown[HS : 2 * HS, p]
    for rd in near:
        send(xbuf.at[0], xbuf.at[rd], s_h.at[rd], r_h.at[rd], zdev(back_rel(rd)))
    wait(res_c.at[0, other], r_c.at[0, 1])
    for rd in near:
        wait(res_c.at[rd, c], r_c.at[rd, 0])
        wait(res_c.at[rd, other], r_c.at[rd, 1])
    ss_row = jnp.zeros((S, 128), F32)
    for rd in near_first:
        xf = res_c[rd].reshape(S, 128).astype(F32)
        ss_row = ss_row + xf * xf
        xg = (xf * gain_a[rd, 0][1:2, :]).astype(BF16)
        part = mm_nt(xg, rexp[rd])
        if rd == 0:
            lg_own[...] = part
        else:
            lg_own[...] += part
    ss_own[...] = ss_row
    send(lg_own, lg_in, s_l.at[0], r_l.at[0], partner)
    send(ss_own, ss_in, s_l.at[1], r_l.at[1], partner)
    for rd in e_near:
        wait(wdn.at[rd, 0], r_w.at[rd, 0])
        send(wdn.at[rd, 0], wdn.at[rd, 1], f_w.at[rd], r_w.at[rd, 1], partner)
    wait(ns_x, r_o.at[0])
    wait(br_x, r_o.at[1])
    nstate_o[...] = nstate_v[...]
    nconv_o[2] = branch_v[...]

    wait(lg_in, r_l.at[0])
    wait(ss_in, r_l.at[1])
    ss_tot = jnp.sum(ss_own[...] + ss_in[...], axis=1, keepdims=True)
    rstd2 = lax.rsqrt(ss_tot / WIDTH + EPS)
    logits = (lg_own[...] + lg_in[...]) * rstd2
    e_exp = jnp.where(selt_v[1] > 0.0, jnp.exp(logits[:, 0:L]), 0.0)
    g_exp = jnp.exp(logits[:, L : 2 * L])
    e_den = jnp.sum(e_exp * (1.0 / CAP), axis=1, keepdims=True)
    g_den = jnp.sum(g_exp * (1.0 / (CAP * GS)), axis=1, keepdims=True)
    combine = selt_v[0] * (g_exp / g_den) * (e_exp / e_den)
    comb_hi = combine.astype(BF16)
    comb_lo = (combine - comb_hi.astype(F32)).astype(BF16)
    comb = jnp.concatenate([comb_hi, comb_lo], axis=0)
    loads[k_g].wait()
    loads[k_u].wait()
    take(x_g, x_u)

    def expert(first, chunks):
        squares = None if first else ssx_v[...]
        parts, weights = [], []
        for rd, halves in chunks:
            for p in range(2):
                xf = halves[p].astype(F32)
                squares = xf * xf if squares is None else squares + xf * xf
                parts.append((xf * gain_a[rd, (p + c) % 2][1:2, :]).astype(BF16))
            cols = pl.ds(pl.multiple_of(zrel(rd) * 256, 256), 256)
            weights.append(wcat[:, :, cols].reshape(256, 256))
        ssx_v[...] = squares
        part = mm_nt(jnp.concatenate(parts, axis=1), jnp.concatenate(weights, axis=1))
        if first:
            acc_v[...] = part
        else:
            acc_v[...] += part

    def halves_of(ref):
        return [ref[p * HS : (p + 1) * HS].reshape(HS * CAP, 128) for p in range(2)]

    expert(True, [(0, halves_of(xbuf.at[0]))])
    for b, (lo, hi) in enumerate(batches):
        wait_blocks(xfar, own_half, r_d.at[1 + b], (lo, hi))
        expert(
            False,
            [
                (far[n], [xfar[p * HS : (p + 1) * HS, n].reshape(HS * CAP, 128) for p in range(2)])
                for n in range(lo, hi)
            ],
        )
    for rd in near:
        wait(xbuf.at[rd], r_h.at[rd])
    if near:
        expert(False, [(rd, halves_of(xbuf.at[rd])) for rd in near])
    ss_slot = jnp.sum(ssx_v[...], axis=1, keepdims=True)
    gu = acc_v[...] * lax.rsqrt(ss_slot / WIDTH + EPS)
    gate = gu[:, 0:128]
    hid_e[0] = (gate * sigmoid(gate) * gu[:, 128:256]).astype(BF16)

    for d in far_first:
        rd = back_rel(d)
        if rd in e_near:
            send(hid_e.at[0], hid_e.at[rd], s_e.at[d], r_e.at[rd], zdev(d))

    def put(dst, y, at=()):
        for p in range(2):
            dst[(p, slice(None)) + at] = y[:, p * 128 : (p + 1) * 128].astype(BF16).reshape(HS, CAP, 128)

    def give_back(src, dst, ssem, rsem):
        def one(i, carry):
            s = c * HS + i

            @pl.when(s != me)
            def _():
                send(src.at[c, i], dst.at[me], ssem.at[i, 0], rsem, (s, tp))

            send(src.at[other, i], dst.at[me], ssem.at[i, 1], rsem, (s, 2 * z + other))
            return carry

        lax.fori_loop(0, HS, one, 0, unroll=True)

        @pl.when(own_half)
        def _():
            dst[me] = src[c, at_me]

    def own_down(d):
        cols = pl.ds(pl.multiple_of(zrel(d) * 256, 256), 256)
        return dnp[:, :, cols].reshape(128, 256)

    loads[k_w].wait()
    take(x_dn)
    for n, d in enumerate(e_far):
        put(yf_v, mm(hid_e[0], own_down(d)), (n,))
    if e_far:
        give_back(yf_v, backf_v, s_k, r_k.at[0])
    out = mm(hid_e[0], own_down(0))
    for rd in e_near:
        wait(wdn.at[rd, 1], r_w.at[rd, 1])
        wait(hid_e.at[rd], r_e.at[rd])
        out = out + mm(hid_e[rd], wdn[rd].reshape(128, 256))
    put(y_v, out)

    give_back(y_v, back_v, s_f, r_f.at[0])

    def combined(back):
        pair = mm(comb, back)
        return pair[0:S] + pair[S : 2 * S]

    if e_far:
        wait_blocks(backf_v, own_half, r_k.at[0])
        parts = combined(jnp.concatenate([backf_v[:, n].reshape(L, 128) for n in range(len(e_far))], axis=1))
    for n, d in sorted(enumerate(e_far), key=lambda p: -min(p[1], NZ - p[1])):
        moe_v[d] = parts[:, n * 128 : (n + 1) * 128].astype(BF16)
        rd = back_rel(d)
        send(moe_v.at[d], moe_in.at[rd], s_m.at[d], r_m.at[rd], zdev(d))
    for d in range(1, NZ):
        for j in range(2):
            wait(gain_a.at[0, 0], s_g.at[d, j])
            wait(tok_a.at[0, 0], s_a.at[d, j])
            wait(res_x, s_c.at[d, j])
        if min(d, NZ - d) <= ENEAR:
            wait(wdn.at[0, 0], s_w.at[d])
            wait(hid_e.at[0], s_e.at[d])
        else:
            wait(moe_v.at[d], s_m.at[d])
        wait(hid_b.at[0], s_b.at[d])
    for rd in e_near:
        wait(wdn.at[0, 0], f_w.at[rd])
    wait(gain_a.at[0, 0], s_g.at[0, 1])
    wait(tok_a.at[0, 0], s_a.at[0, 1])
    wait(res_x, s_c.at[0, 1])
    for k, dst in enumerate(shared):
        wait(dst, s_x.at[k])
    wait_blocks(ysel, own_half, s_d.at[0])
    for b, part in enumerate(batches):
        wait_blocks(yfar, own_half, s_d.at[1 + b], part)
    for rd in near:
        wait(xbuf.at[0], s_h.at[rd])
    wait(ns_x, s_o.at[0])
    wait(br_x, s_o.at[1])
    wait(lg_own, s_l.at[0])
    wait(ss_own, s_l.at[1])

    def left(i, carry):
        @pl.when(c * HS + i != me)
        def _():
            wait(y_v.at[0, 0], s_f.at[i, 0])
            if e_far:
                wait(yf_v.at[0, 0], s_k.at[i, 0])

        wait(y_v.at[0, 0], s_f.at[i, 1])
        if e_far:
            wait(yf_v.at[0, 0], s_k.at[i, 1])
        return carry

    lax.fori_loop(0, HS, left, 0)
    wait_blocks(back_v, own_half, r_f.at[0])
    moe = combined(back_v[...].reshape(L, 128))
    for rd in e_far:
        wait(moe_in.at[rd], r_m.at[rd])
        moe = moe + moe_in[rd].astype(F32)
    mixed_o[...] = (res_c[0].reshape(S, 128).astype(F32) + moe).astype(BF16)


def emit(a_v, b_v, c_v, ao_h, bo_h, co_h, sem):
    copies = [
        pltpu.make_async_copy(src, dst, sem.at[k])
        for k, (src, dst) in enumerate(((a_v, ao_h), (b_v, bo_h), (c_v, co_h)))
    ]
    for copy in copies:
        copy.start()
    for copy in copies:
        copy.wait()


def on_device(
    tokens, conv_state, recur_state, norm1_gain, branch_weight, gating_weight, conv_taps, conv_bias,
    recur_weight, recur_bias, input_weight, input_bias, decay_logit, out_weight, norm2_gain,
    group_router, expert_router, routes, gate_experts, up_experts, down_experts,
):
    EP = lax.axis_size("ep")
    TPN = lax.axis_size("tp")
    NZ = TPN // 2
    S = tokens.shape[0]
    CAP = 2 * routes.shape[1] * S // EP
    GS = expert_router.shape[1] // group_router.shape[1]
    L = EP * CAP
    args = (
        tokens,
        jnp.transpose(conv_state, (1, 0, 2)),
        recur_state,
        norm1_gain,
        norm2_gain,
        conv_bias,
        recur_bias,
        input_bias,
        decay_logit,
        conv_taps,
        branch_weight,
        gating_weight,
        recur_weight[0],
        input_weight[0],
        out_weight,
        group_router.T,
        expert_router.T,
        routes.T,
        gate_experts[0].T,
        up_experts[0].T,
        down_experts[0],
    )
    D = TPN * 128
    V = pltpu.VMEM
    dma = pltpu.SemaphoreType.DMA
    H = S // 2
    near_count = 3 if NZ > 4 else min(NZ - 1, 2)
    NF = max(NZ - 1 - near_count, 1)
    NFE = max(len([d for d in range(1, NZ) if min(d, NZ - d) > ENEAR]), 1)
    scratch = [
        V((S, 128), BF16),
        V((NZ, 2, H, 128), BF16),
        V((NZ, 2, 2, 128), F32),
        V((2, S, 128), BF16),
        V((2, 3, H, 128), BF16),
        V((2, H, 128), F32),
        V((128,), BF16), V((128,), BF16), V((128,), BF16),
        V((128,), F32), V((128,), F32), V((128,), F32),
        V((4, 128), BF16),
        V((2, 8, 128), F32),
        V((2, D, 128), BF16),
        V((2, D, 128), BF16),
        V((2, 128, 128), BF16),
        V((2, 128, 128), BF16),
        V((2, D, 128), BF16),
        V(group_router.T.shape, BF16),
        V(expert_router.T.shape, BF16),
        V((2, S), jnp.int32),
        V((4, 64, D), BF16),
        V((2, 64, D), BF16),
        V((NZ, 2, 64, 256), BF16),
        V((NZ, H, 256), BF16),
        V((NZ, 2, H, 128), BF16),
        V((H, 128), BF16),
        V((EP, 2, CAP, 128), BF16),
        V((EP, NF, CAP, 128), BF16),
        V((EP, 2, CAP, 128), BF16),
        V((NZ, EP, CAP, 128), BF16),
        V((EP, NF, CAP, 128), BF16),
        V((NZ, 2 * L, 128), BF16),
        V((S, 2 * L), F32),
        V((S, 2 * L), F32),
        V((S, 128), F32),
        V((S, 128), F32),
        V((L // 2, 256), F32),
        V((L // 2, 128), F32),
        V((NZ, L // 2, 128), BF16),
        V((2, EP // 2, CAP, 128), BF16),
        V((2, EP // 2, NFE, CAP, 128), BF16),
        V((EP, CAP, 128), BF16),
        V((EP, NFE, CAP, 128), BF16),
        V((NZ, S, 128), BF16),
        V((NZ, S, 128), BF16),
        V((S, 128), F32),
        V((H, 128), F32),
        V((S, 128), BF16),
        V((H, 128), BF16),
        V((L, S), BF16),
        V((L, H), BF16),
        V((2, S, L), F32),
        dma((24,)),
        dma((NZ, 2)), dma((NZ, 2)),
        dma((NZ, 2)), dma((NZ, 2)),
        dma((NZ,)), dma((NZ,)),
        dma((NZ,)), dma((NZ, 2)), dma((NZ,)),
        dma((11,)), dma((11,)),
        dma((NZ, 2)), dma((NZ, 2)),
        dma((NZ,)), dma((NZ,)),
        dma((NZ,)), dma((NZ,)),
        dma((2,)), dma((2,)),
        dma((2,)), dma((2,)),
        dma((NZ,)), dma((NZ,)),
        dma((EP // 2, 2)), dma((1,)),
        dma((EP // 2, 2)), dma((1,)),
        dma((NZ,)), dma((NZ,)),
    ]
    anyspace = pl.BlockSpec(memory_space=pl.ANY)
    mixed, new_state, new_conv = pl.pallas_call(
        functools.partial(kernel, EP, NZ, S, CAP, GS),
        out_shape=(
            V((S, 128), BF16),
            V((S, 128), F32),
            V((3, S, 128), BF16),
        ),
        in_specs=[anyspace] * len(args),
        out_specs=[pl.BlockSpec(memory_space=pltpu.VMEM)] * 3,
        scratch_shapes=scratch,
        compiler_params=pltpu.CompilerParams(
            collective_id=0, has_side_effects=True, vmem_limit_bytes=57000000
        ),
        name="layer",
    )(*args)
    shapes = ((S, 128), (S, 128), (3, S, 128))
    types = (BF16, F32, BF16)
    mixed, new_state, new_conv = pl.pallas_call(
        emit,
        out_shape=tuple(jax.ShapeDtypeStruct(a, b) for a, b in zip(shapes, types)),
        in_specs=[pl.BlockSpec(memory_space=pltpu.VMEM)] * 3,
        out_specs=[anyspace] * 3,
        scratch_shapes=[dma((3,))],
        compiler_params=pltpu.CompilerParams(vmem_limit_bytes=2 * 1024 * 1024),
        name="emit",
    )(mixed, new_state, new_conv)
    return mixed, new_state, jnp.transpose(new_conv, (1, 0, 2))


def solution(mesh):
    return jax.shard_map(
        on_device,
        mesh=mesh,
        in_specs=(
            P("ep", "tp"),
            P("ep", None, "tp"),
            P("ep", "tp"),
            P("tp"),
            P(None, "tp"),
            P(None, "tp"),
            P(None, "tp"),
            P("tp"),
            P("tp", None, None),
            P("tp"),
            P("tp", None, None),
            P("tp"),
            P("tp"),
            P(None, "tp"),
            P("tp"),
            P(),
            P(),
            P("ep", None),
            P("ep", None, "tp"),
            P("ep", None, "tp"),
            P("ep", "tp", None),
        ),
        out_specs=(P("ep", "tp"), P("ep", "tp"), P("ep", None, "tp")),
        check_vma=False,
    )
```

```python
import functools

import jax
import jax.numpy as jnp
from jax import lax
from jax.experimental import pallas as pl
from jax.experimental.pallas import tpu as pltpu
from jax.sharding import PartitionSpec as P

EPS = 1e-06
ENEAR = 2
BATCH_AT = 4
F32 = jnp.float32
BF16 = jnp.bfloat16
MESH = pl.DeviceIdType.MESH
NT = (((1,), (1,)), ((), ()))


def mm(a, b):
    return jnp.dot(a, b, preferred_element_type=F32)


def mm_nt(a, b):
    return lax.dot_general(a, b, NT, preferred_element_type=F32)


def expm1_neg(x):
    series = x * (1.0 + x * (0.5 + x * (1.0 / 6 + x * (1.0 / 24 + x * (1.0 / 120 + x / 720)))))
    return jnp.where(x > -0.2, -series, 1.0 - jnp.exp(x))


def log_sigmoid(x):
    u = jnp.exp(-jnp.abs(x))
    w = u / (2.0 + u)
    w2 = w * w
    poly = 1.0 / 15
    for k in (13, 11, 9, 7, 5, 3, 1):
        poly = poly * w2 + 1.0 / k
    return jnp.minimum(x, 0.0) - 2.0 * w * poly


def gelu(x):
    return 0.5 * x * (1.0 + jnp.tanh(0.7978845608028654 * (x + 0.044715 * x * x * x)))


def sigmoid(x):
    return 1.0 / (1.0 + jnp.exp(-x))


def kernel(
    EP, NZ, S, CAP, GS,
    tok_h, conv_h, state_h, n1_h, n2_h, cb_h, rb_h, ib_h, dl_h, taps_h, bw_h, gw_h, rw_h, iw_h, ow_h,
    grt_h, ert_h, rt_h, gt_h, ut_h, dn_h,
    mixed_o, nstate_o, nconv_o,
    tok_v, tok_a, gain_a, conv_v, conv_p, state_p, n1_v, n2_v, cb_v, rb_v, ib_v, dl_v, taps_v, par_v,
    bw_p, gw_p, rw_p, iw_p, ow_p, grt_v, ert_v, rt_v, wcat, dnp, wdn,
    hid_b, res_c, res_x, ysel, yfar, xown, xbuf, xfar, rexp, lg_own, lg_in, ss_own, ss_in, acc_v, ssx_v,
    hid_e, y_v, yf_v, back_v, backf_v, moe_v, moe_in, nstate_v, ns_x, branch_v, br_x, sel_v, selh_v, selt_v,
    sem_ld, s_a, r_a, s_g, r_g, s_b, r_b, s_w, r_w, f_w, s_x, r_x,
    s_c, r_c, s_d, r_d, s_h, r_h, s_l, r_l, s_o, r_o, s_e, r_e, s_f, r_f, s_k, r_k, s_m, r_m,
):
    me = lax.axis_index("ep")
    tp = lax.axis_index("tp")
    z = tp // 2
    c = tp % 2
    H = S // 2
    L = EP * CAP
    HS = EP // 2
    WIDTH = NZ * 256
    other = 1 - c
    partner = (me, 2 * z + other)
    home = me // HS
    own_half = home == c
    at_me = me - home * HS
    my_rows = pl.ds(pl.multiple_of(c * H, H), H)
    its_rows = pl.ds(pl.multiple_of(other * H, H), H)

    def zdev(d):
        return (me, 2 * ((z + d) % NZ) + c)

    def zcross(d):
        return (me, 2 * ((z + d) % NZ) + other)

    def zrel(rd):
        return (z + rd) % NZ

    def rows(j, rd):
        t = 2 * zrel(rd) + (c if j == 0 else other)
        return pl.multiple_of(t * 128, 128)

    def back_rel(d):
        return (NZ - d) % NZ

    far_first = sorted(range(1, NZ), key=lambda d: (-min(d, NZ - d), d))
    near_first = [0] + sorted(range(1, NZ), key=lambda d: (min(d, NZ - d), d))
    near = [rd for rd in near_first[1:] if min(rd, NZ - rd) <= 1]
    far = [rd for rd in near_first[1:] if min(rd, NZ - rd) > 1]
    if NZ > 4:
        by_parity = 2 + (z % 2) * (NZ - 4)
        near = [by_parity] + near
        far = [NZ - by_parity] + [rd for rd in far if min(rd, NZ - rd) > 2]
    step = max(BATCH_AT, 1)
    batches = [(lo, min(lo + step, len(far))) for lo in range(0, len(far), step)]

    e_near = [rd for rd in near_first[1:] if min(rd, NZ - rd) <= ENEAR]
    e_far = [rd for rd in near_first[1:] if min(rd, NZ - rd) > ENEAR]

    def row(ref):
        return ref[...].astype(F32).reshape(1, 128)

    def wait(ref, sem):
        pltpu.make_async_copy(ref, ref, sem).wait()

    def send(src, dst, ssem, rsem, dev):
        pltpu.make_async_remote_copy(
            src_ref=src, dst_ref=dst, send_sem=ssem, recv_sem=rsem, device_id=dev, device_id_type=MESH
        ).start()

    bar = pltpu.get_barrier_semaphore()

    def sig(dev):
        pl.semaphore_signal(bar, inc=1, device_id=dev, device_id_type=MESH)

    for d in far_first:
        sig(zdev(d))
        sig(zcross(d))

    def bar_ep(i, carry):
        e = (me + i) % EP
        sig((e, tp))
        sig((e, 2 * z + other))
        return carry

    lax.fori_loop(1, EP, bar_ep, 0, unroll=True)
    sig(partner)

    loads = []

    def load(src, dst):
        k = len(loads)
        cp = pltpu.make_async_copy(src, dst, sem_ld.at[k])
        cp.start()
        loads.append(cp)
        return k

    k_tok = load(tok_h, tok_v)
    k_own = load(tok_h.at[my_rows], tok_a.at[0, 0])
    k_small = [
        load(a, b)
        for a, b in (
            (n1_h, n1_v), (n2_h, n2_v), (cb_h, cb_v), (rb_h, rb_v), (ib_h, ib_v), (dl_h, dl_v), (taps_h, taps_v)
        )
    ]
    k_rt = load(rt_h, rt_v)

    k_gr = load(grt_h, grt_v)
    k_er = load(ert_h, ert_v)
    k_conv = load(conv_h.at[:, my_rows], conv_p.at[0])
    k_convo = load(conv_h.at[1:3], conv_v)
    k_state = load(state_h.at[my_rows], state_p.at[0])
    k_bw = load(bw_h, bw_p.at[0])
    k_gw = load(gw_h, gw_p.at[0])
    k_rw = load(rw_h, rw_p.at[0])
    k_iw = load(iw_h, iw_p.at[0])
    k_ow = load(ow_h, ow_p.at[0])
    k_w = load(dn_h, dnp.at[0])
    k_g = load(gt_h, wcat.at[0])
    k_u = load(ut_h, wcat.at[2])

    loads[k_tok].wait()
    for k in k_small:
        loads[k].wait()
    gain_a[0, 0] = jnp.concatenate([row(n1_v), row(n2_v)], axis=0)
    par_v[0, 0:4] = jnp.concatenate([row(cb_v), row(rb_v), row(ib_v), row(dl_v)], axis=0)
    par_v[0, 4:8] = taps_v[...].astype(F32)

    pl.semaphore_wait(bar, 2 * (NZ - 1) + 1 + 2 * (EP - 1))

    for d in far_first:
        rd = back_rel(d)
        send(gain_a.at[0, 0], gain_a.at[rd, 0], s_g.at[d, 0], r_g.at[rd, 0], zdev(d))
        send(gain_a.at[0, 0], gain_a.at[rd, 1], s_g.at[d, 1], r_g.at[rd, 1], zcross(d))
    for d in far_first:
        rd = back_rel(d)
        send(tok_v.at[my_rows], tok_a.at[rd, 0], s_a.at[d, 0], r_a.at[rd, 0], zdev(d))
        send(tok_v.at[its_rows], tok_a.at[rd, 1], s_a.at[d, 1], r_a.at[rd, 1], zcross(d))
    send(gain_a.at[0, 0], gain_a.at[0, 1], s_g.at[0, 1], r_g.at[0, 1], partner)
    send(tok_v.at[its_rows], tok_a.at[0, 1], s_a.at[0, 1], r_a.at[0, 1], partner)

    shared = []

    def share(src, dst):
        k = len(shared)
        send(src, dst, s_x.at[k], r_x.at[k], partner)
        shared.append(dst)
        return k

    x_bw = share(bw_h, bw_p.at[1])
    x_gw = share(gw_h, gw_p.at[1])
    x_par = share(par_v.at[0], par_v.at[1])
    x_conv = share(conv_h.at[:, its_rows], conv_p.at[1])
    x_rw = share(rw_h, rw_p.at[1])
    x_iw = share(iw_h, iw_p.at[1])
    x_state = share(state_h.at[its_rows], state_p.at[1])

    def take(*ks):
        for k in ks:
            wait(shared[k], r_x.at[k])

    def send_down(dists):
        for d in dists:
            cols = pl.ds(pl.multiple_of(((z + d) % NZ) * 256, 256), 256)
            rd = back_rel(d)
            send(dn_h.at[:, cols], wdn.at[rd, 0], s_w.at[d], r_w.at[rd, 0], zdev(d))


    loads[k_rt].wait()
    loads[k_gr].wait()
    loads[k_er].wait()
    slot_row = lax.broadcasted_iota(jnp.int32, (L, S), 0)
    r0 = rt_v[0:1, :]
    r1 = rt_v[1:2, :]
    hit = ((slot_row // CAP) == r0) | ((slot_row // CAP) == r1)
    hit_f = jnp.where(hit, 1.0, 0.0)
    hit_b = hit_f.astype(BF16)
    before = jnp.where(
        lax.broadcasted_iota(jnp.int32, (S, S), 0) < lax.broadcasted_iota(jnp.int32, (S, S), 1), 1.0, 0.0
    ).astype(BF16)
    rank = mm(hit_b, before)
    sel = jnp.where(rank == (slot_row % CAP).astype(F32), hit_f, 0.0).astype(BF16)
    sel_v[...] = sel
    pick = jnp.where(
        lax.broadcasted_iota(jnp.int32, (S, H), 0) == lax.broadcasted_iota(jnp.int32, (S, H), 1) + c * H, 1.0, 0.0
    ).astype(BF16)
    selh_v[...] = mm(sel, pick).astype(BF16)
    eye = jnp.where(
        lax.broadcasted_iota(jnp.int32, (S, S), 0) == lax.broadcasted_iota(jnp.int32, (S, S), 1), 1.0, 0.0
    ).astype(BF16)
    selt_v[0] = mm_nt(eye, sel)
    selt_v[1] = mm_nt(eye, hit_b)
    spread_e = jnp.where(
        lax.broadcasted_iota(jnp.int32, (L, EP), 0) // CAP == lax.broadcasted_iota(jnp.int32, (L, EP), 1), 1.0, 0.0
    ).astype(BF16)
    groups = grt_h.shape[0]
    spread_g = jnp.where(
        lax.broadcasted_iota(jnp.int32, (L, groups), 0) // (CAP * GS)
        == lax.broadcasted_iota(jnp.int32, (L, groups), 1),
        1.0,
        0.0,
    ).astype(BF16)
    for rd in range(NZ):
        cols = pl.ds(rows(0, rd), 128)
        rexp[rd, 0:L] = mm(spread_e, ert_v[:, cols]).astype(BF16)
        rexp[rd, L : 2 * L] = mm(spread_g, grt_v[:, cols]).astype(BF16)
    loads[k_conv].wait()
    loads[k_own].wait()
    take(x_par, x_conv)

    def par(i):
        return jnp.concatenate([par_v[0, i : i + 1, :], par_v[1, i : i + 1, :]], axis=1)

    conv_part = par(0) + sum(
        par(4 + j) * jnp.concatenate([conv_p[0, j], conv_p[1, j]], axis=1).astype(F32) for j in range(3)
    )
    base_decay = 8.0 * log_sigmoid(par(3))
    loads[k_bw].wait()
    loads[k_gw].wait()
    take(x_bw, x_gw)

    def both(w_p, rd):
        i0 = pl.ds(rows(0, rd), 128)
        i1 = pl.ds(rows(1, rd), 128)
        return jnp.concatenate(
            [
                jnp.concatenate([w_p[0, i0, :], w_p[1, i0, :]], axis=1),
                jnp.concatenate([w_p[0, i1, :], w_p[1, i1, :]], axis=1),
            ],
            axis=0,
        )

    sums = [jnp.zeros((H, 128), F32), jnp.zeros((H, 256), F32), jnp.zeros((H, 256), F32)]
    for rd in near_first:
        parts = []
        for j in range(2):
            if (rd, j) != (0, 0):
                wait(gain_a.at[rd, j], r_g.at[rd, j])
                wait(tok_a.at[rd, j], r_a.at[rd, j])
            x = tok_a[rd, j].astype(F32)
            sums[0] = sums[0] + x * x
            parts.append((x * gain_a[rd, j][0:1, :]).astype(BF16))
        if rd == near_first[-1]:
            x_ow = share(ow_h, ow_p.at[1])
        xg = jnp.concatenate(parts, axis=1)
        sums[1] = sums[1] + mm(xg, both(bw_p, rd))
        sums[2] = sums[2] + mm(xg, both(gw_p, rd))
    rstd = lax.rsqrt(jnp.sum(sums[0], axis=1, keepdims=True) / WIDTH + EPS)
    branch = (sums[1] * rstd).astype(BF16)
    gating = (sums[2] * rstd).astype(BF16).astype(F32)

    conv_out = conv_part + par(7) * branch.astype(F32)
    conv_low = conv_out.astype(BF16)
    loads[k_rw].wait()
    loads[k_iw].wait()
    loads[k_state].wait()
    take(x_rw, x_iw, x_state)

    def block_map(w_p):
        return jnp.concatenate([mm(conv_low[:, 0:128], w_p[0]), mm(conv_low[:, 128:256], w_p[1])], axis=1)

    recur_gate = sigmoid(block_map(rw_p) + par(1))
    input_gate = sigmoid(block_map(iw_p) + par(2))
    log_decay = recur_gate * base_decay
    state = jnp.concatenate([state_p[0], state_p[1]], axis=1)
    new_state = jnp.exp(log_decay) * state + jnp.sqrt(expm1_neg(2.0 * log_decay)) * (input_gate * conv_out)
    hid_b[0] = (new_state * gelu(gating)).astype(BF16)

    for d in far_first:
        rd = back_rel(d)
        send(hid_b.at[0], hid_b.at[rd], s_b.at[d], r_b.at[rd], zdev(d))
    nstate_v[my_rows, :] = new_state[:, 0:128]
    ns_x[...] = new_state[:, 128:256]
    branch_v[my_rows, :] = branch[:, 0:128]
    br_x[...] = branch[:, 128:256]
    send(ns_x, nstate_v.at[my_rows], s_o.at[0], r_o.at[0], partner)
    send(br_x, branch_v.at[my_rows], s_o.at[1], r_o.at[1], partner)
    loads[k_convo].wait()
    nconv_o[0:2] = conv_v[...]
    loads[k_ow].wait()
    take(x_ow)
    proj = None
    for rd in near_first:
        if rd != 0:
            wait(hid_b.at[rd], r_b.at[rd])
        part = mm(hid_b[rd], both(ow_p, rd))
        proj = part if proj is None else proj + part
    resid = (jnp.concatenate([tok_a[0, 0], tok_a[0, 1]], axis=1).astype(F32) + proj).astype(BF16)
    res_c[0, c] = resid[:, 0:128]
    res_x[...] = resid[:, 128:256]

    send(res_x, res_c.at[0, c], s_c.at[0, 1], r_c.at[0, 1], partner)
    for d in far_first:
        rd = back_rel(d)
        send(res_c.at[0, c], res_c.at[rd, c], s_c.at[d, 0], r_c.at[rd, 0], zdev(d))
        send(res_x, res_c.at[rd, c], s_c.at[d, 1], r_c.at[rd, 1], zcross(d))

    x_g = share(gt_h, wcat.at[1])
    x_u = share(ut_h, wcat.at[3])
    x_dn = share(dn_h, dnp.at[1])
    def dispatch(src, dst, ssem, rsem, part=None):
        slot = c * HS + at_me

        def piece(ref, e):
            return ref.at[e] if part is None else ref.at[e, part[0] : part[1]]

        def one(i, carry):
            e = (me + i) % EP
            send(piece(src, e), piece(dst, slot), ssem, rsem, (e, 2 * z + home))
            return carry

        lax.fori_loop(1, EP, one, 0, unroll=True)

        @pl.when(own_half)
        def _():
            piece(dst, slot)[...] = piece(src, me)[...]

        @pl.when(jnp.logical_not(own_half))
        def _():
            send(piece(src, me), piece(dst, slot), ssem, rsem, partner)

    def wait_blocks(ref, n_own, sem, part=None):
        @pl.when(n_own)
        def _():
            wait(ref.at[0 : EP - 1] if part is None else ref.at[0 : EP - 1, part[0] : part[1]], sem)

        @pl.when(jnp.logical_not(n_own))
        def _():
            wait(ref if part is None else ref.at[:, part[0] : part[1]], sem)

    for j in range(2):
        half = mm(selh_v[...], resid[:, j * 128 : (j + 1) * 128]).astype(BF16)
        ysel[:, c if j == 0 else other] = half.reshape(EP, CAP, 128)
    dispatch(ysel, xown, s_d.at[0], r_d.at[0])
    for b, (lo, hi) in enumerate(batches):
        for n in range(lo, hi):
            rd = far[n]
            wait(res_c.at[rd, c], r_c.at[rd, 0])
            wait(res_c.at[rd, other], r_c.at[rd, 1])
        chunks = jnp.concatenate([res_c[far[n]].reshape(S, 128) for n in range(lo, hi)], axis=1)
        rows_out = mm(sel_v[...], chunks).astype(BF16)
        for n in range(lo, hi):
            yfar[:, n] = rows_out[:, (n - lo) * 128 : (n - lo + 1) * 128].reshape(EP, CAP, 128)
        dispatch(yfar, xfar, s_d.at[1 + b], r_d.at[1 + b], (lo, hi))
    wait_blocks(xown, own_half, r_d.at[0])
    for p in range(2):
        xbuf[0, p * HS : (p + 1) * HS] = xown[0:HS, p] + xown[HS : 2 * HS, p]
    for rd in near:
        send(xbuf.at[0], xbuf.at[rd], s_h.at[rd], r_h.at[rd], zdev(back_rel(rd)))
    wait(res_c.at[0, other], r_c.at[0, 1])
    for rd in near:
        wait(res_c.at[rd, c], r_c.at[rd, 0])
        wait(res_c.at[rd, other], r_c.at[rd, 1])
    ss_row = jnp.zeros((S, 128), F32)
    for rd in near_first:
        xf = res_c[rd].reshape(S, 128).astype(F32)
        ss_row = ss_row + xf * xf
        xg = (xf * gain_a[rd, 0][1:2, :]).astype(BF16)
        part = mm_nt(xg, rexp[rd])
        if rd == 0:
            lg_own[...] = part
        else:
            lg_own[...] += part
    ss_own[...] = ss_row
    send(lg_own, lg_in, s_l.at[0], r_l.at[0], partner)
    send(ss_own, ss_in, s_l.at[1], r_l.at[1], partner)
    send_down([d for d in far_first if min(d, NZ - d) in (1, 2)])
    wait(ns_x, r_o.at[0])
    wait(br_x, r_o.at[1])
    nstate_o[...] = nstate_v[...]
    nconv_o[2] = branch_v[...]

    wait(lg_in, r_l.at[0])
    wait(ss_in, r_l.at[1])
    ss_tot = jnp.sum(ss_own[...] + ss_in[...], axis=1, keepdims=True)
    rstd2 = lax.rsqrt(ss_tot / WIDTH + EPS)
    logits = (lg_own[...] + lg_in[...]) * rstd2
    e_exp = jnp.where(selt_v[1] > 0.0, jnp.exp(logits[:, 0:L]), 0.0)
    g_exp = jnp.exp(logits[:, L : 2 * L])
    e_den = jnp.sum(e_exp * (1.0 / CAP), axis=1, keepdims=True)
    g_den = jnp.sum(g_exp * (1.0 / (CAP * GS)), axis=1, keepdims=True)
    combine = selt_v[0] * (g_exp / g_den) * (e_exp / e_den)
    comb_hi = combine.astype(BF16)
    comb_lo = (combine - comb_hi.astype(F32)).astype(BF16)
    comb = jnp.concatenate([comb_hi, comb_lo], axis=0)
    loads[k_g].wait()
    loads[k_u].wait()
    take(x_g, x_u)

    def expert(first, chunks):
        squares = None if first else ssx_v[...]
        parts, weights = [], []
        for rd, halves in chunks:
            for p in range(2):
                xf = halves[p].astype(F32)
                squares = xf * xf if squares is None else squares + xf * xf
                parts.append((xf * gain_a[rd, (p + c) % 2][1:2, :]).astype(BF16))
            cols = pl.ds(pl.multiple_of(zrel(rd) * 256, 256), 256)
            weights.append(wcat[:, :, cols].reshape(256, 256))
        ssx_v[...] = squares
        part = mm_nt(jnp.concatenate(parts, axis=1), jnp.concatenate(weights, axis=1))
        if first:
            acc_v[...] = part
        else:
            acc_v[...] += part

    def halves_of(ref):
        return [ref[p * HS : (p + 1) * HS].reshape(HS * CAP, 128) for p in range(2)]

    expert(True, [(0, halves_of(xbuf.at[0]))])
    for b, (lo, hi) in enumerate(batches):
        wait_blocks(xfar, own_half, r_d.at[1 + b], (lo, hi))
        expert(
            False,
            [
                (far[n], [xfar[p * HS : (p + 1) * HS, n].reshape(HS * CAP, 128) for p in range(2)])
                for n in range(lo, hi)
            ],
        )
    for rd in near:
        wait(xbuf.at[rd], r_h.at[rd])
    if near:
        expert(False, [(rd, halves_of(xbuf.at[rd])) for rd in near])
    ss_slot = jnp.sum(ssx_v[...], axis=1, keepdims=True)
    gu = acc_v[...] * lax.rsqrt(ss_slot / WIDTH + EPS)
    gate = gu[:, 0:128]
    hid_e[0] = (gate * sigmoid(gate) * gu[:, 128:256]).astype(BF16)

    for d in far_first:
        rd = back_rel(d)
        if rd in e_near:
            send(hid_e.at[0], hid_e.at[rd], s_e.at[d], r_e.at[rd], zdev(d))

    def put(dst, y, at=()):
        for p in range(2):
            dst[(p, slice(None)) + at] = y[:, p * 128 : (p + 1) * 128].astype(BF16).reshape(HS, CAP, 128)

    def give_back(src, dst, ssem, rsem):
        def one(i, carry):
            s = c * HS + i

            @pl.when(s != me)
            def _():
                send(src.at[c, i], dst.at[me], ssem.at[i, 0], rsem, (s, tp))

            send(src.at[other, i], dst.at[me], ssem.at[i, 1], rsem, (s, 2 * z + other))
            return carry

        lax.fori_loop(0, HS, one, 0, unroll=True)

        @pl.when(own_half)
        def _():
            dst[me] = src[c, at_me]

    def own_down(d):
        cols = pl.ds(pl.multiple_of(zrel(d) * 256, 256), 256)
        return dnp[:, :, cols].reshape(128, 256)

    loads[k_w].wait()
    take(x_dn)
    for n, d in enumerate(e_far):
        put(yf_v, mm(hid_e[0], own_down(d)), (n,))
    if e_far:
        give_back(yf_v, backf_v, s_k, r_k.at[0])
    for rd in e_near:
        wait(wdn.at[rd, 0], r_w.at[rd, 0])
        send(wdn.at[rd, 0], wdn.at[rd, 1], f_w.at[rd], r_w.at[rd, 1], partner)
    out = mm(hid_e[0], own_down(0))
    for rd in e_near:
        wait(wdn.at[rd, 1], r_w.at[rd, 1])
        wait(hid_e.at[rd], r_e.at[rd])
        out = out + mm(hid_e[rd], wdn[rd].reshape(128, 256))
    put(y_v, out)

    give_back(y_v, back_v, s_f, r_f.at[0])

    def combined(back):
        pair = mm(comb, back)
        return pair[0:S] + pair[S : 2 * S]

    if e_far:
        wait_blocks(backf_v, own_half, r_k.at[0])
        parts = combined(jnp.concatenate([backf_v[:, n].reshape(L, 128) for n in range(len(e_far))], axis=1))
    for n, d in sorted(enumerate(e_far), key=lambda p: -min(p[1], NZ - p[1])):
        moe_v[d] = parts[:, n * 128 : (n + 1) * 128].astype(BF16)
        rd = back_rel(d)
        send(moe_v.at[d], moe_in.at[rd], s_m.at[d], r_m.at[rd], zdev(d))
    for d in range(1, NZ):
        for j in range(2):
            wait(gain_a.at[0, 0], s_g.at[d, j])
            wait(tok_a.at[0, 0], s_a.at[d, j])
            wait(res_x, s_c.at[d, j])
        if min(d, NZ - d) <= ENEAR:
            wait(wdn.at[0, 0], s_w.at[d])
            wait(hid_e.at[0], s_e.at[d])
        else:
            wait(moe_v.at[d], s_m.at[d])
        wait(hid_b.at[0], s_b.at[d])
    for rd in e_near:
        wait(wdn.at[0, 0], f_w.at[rd])
    wait(gain_a.at[0, 0], s_g.at[0, 1])
    wait(tok_a.at[0, 0], s_a.at[0, 1])
    wait(res_x, s_c.at[0, 1])
    for k, dst in enumerate(shared):
        wait(dst, s_x.at[k])
    wait_blocks(ysel, own_half, s_d.at[0])
    for b, part in enumerate(batches):
        wait_blocks(yfar, own_half, s_d.at[1 + b], part)
    for rd in near:
        wait(xbuf.at[0], s_h.at[rd])
    wait(ns_x, s_o.at[0])
    wait(br_x, s_o.at[1])
    wait(lg_own, s_l.at[0])
    wait(ss_own, s_l.at[1])

    def left(i, carry):
        @pl.when(c * HS + i != me)
        def _():
            wait(y_v.at[0, 0], s_f.at[i, 0])
            if e_far:
                wait(yf_v.at[0, 0], s_k.at[i, 0])

        wait(y_v.at[0, 0], s_f.at[i, 1])
        if e_far:
            wait(yf_v.at[0, 0], s_k.at[i, 1])
        return carry

    lax.fori_loop(0, HS, left, 0)
    wait_blocks(back_v, own_half, r_f.at[0])
    moe = combined(back_v[...].reshape(L, 128))
    for rd in e_far:
        wait(moe_in.at[rd], r_m.at[rd])
        moe = moe + moe_in[rd].astype(F32)
    mixed_o[...] = (res_c[0].reshape(S, 128).astype(F32) + moe).astype(BF16)


def emit(a_v, b_v, c_v, ao_h, bo_h, co_h, sem):
    copies = [
        pltpu.make_async_copy(src, dst, sem.at[k])
        for k, (src, dst) in enumerate(((a_v, ao_h), (b_v, bo_h), (c_v, co_h)))
    ]
    for copy in copies:
        copy.start()
    for copy in copies:
        copy.wait()


def on_device(
    tokens, conv_state, recur_state, norm1_gain, branch_weight, gating_weight, conv_taps, conv_bias,
    recur_weight, recur_bias, input_weight, input_bias, decay_logit, out_weight, norm2_gain,
    group_router, expert_router, routes, gate_experts, up_experts, down_experts,
):
    EP = lax.axis_size("ep")
    TPN = lax.axis_size("tp")
    NZ = TPN // 2
    S = tokens.shape[0]
    CAP = 2 * routes.shape[1] * S // EP
    GS = expert_router.shape[1] // group_router.shape[1]
    L = EP * CAP
    args = (
        tokens,
        jnp.transpose(conv_state, (1, 0, 2)),
        recur_state,
        norm1_gain,
        norm2_gain,
        conv_bias,
        recur_bias,
        input_bias,
        decay_logit,
        conv_taps,
        branch_weight,
        gating_weight,
        recur_weight[0],
        input_weight[0],
        out_weight,
        group_router.T,
        expert_router.T,
        routes.T,
        gate_experts[0].T,
        up_experts[0].T,
        down_experts[0],
    )
    D = TPN * 128
    V = pltpu.VMEM
    dma = pltpu.SemaphoreType.DMA
    H = S // 2
    near_count = 3 if NZ > 4 else min(NZ - 1, 2)
    NF = max(NZ - 1 - near_count, 1)
    NFE = max(len([d for d in range(1, NZ) if min(d, NZ - d) > ENEAR]), 1)
    scratch = [
        V((S, 128), BF16),
        V((NZ, 2, H, 128), BF16),
        V((NZ, 2, 2, 128), F32),
        V((2, S, 128), BF16),
        V((2, 3, H, 128), BF16),
        V((2, H, 128), F32),
        V((128,), BF16), V((128,), BF16), V((128,), BF16),
        V((128,), F32), V((128,), F32), V((128,), F32),
        V((4, 128), BF16),
        V((2, 8, 128), F32),
        V((2, D, 128), BF16),
        V((2, D, 128), BF16),
        V((2, 128, 128), BF16),
        V((2, 128, 128), BF16),
        V((2, D, 128), BF16),
        V(group_router.T.shape, BF16),
        V(expert_router.T.shape, BF16),
        V((2, S), jnp.int32),
        V((4, 64, D), BF16),
        V((2, 64, D), BF16),
        V((NZ, 2, 64, 256), BF16),
        V((NZ, H, 256), BF16),
        V((NZ, 2, H, 128), BF16),
        V((H, 128), BF16),
        V((EP, 2, CAP, 128), BF16),
        V((EP, NF, CAP, 128), BF16),
        V((EP, 2, CAP, 128), BF16),
        V((NZ, EP, CAP, 128), BF16),
        V((EP, NF, CAP, 128), BF16),
        V((NZ, 2 * L, 128), BF16),
        V((S, 2 * L), F32),
        V((S, 2 * L), F32),
        V((S, 128), F32),
        V((S, 128), F32),
        V((L // 2, 256), F32),
        V((L // 2, 128), F32),
        V((NZ, L // 2, 128), BF16),
        V((2, EP // 2, CAP, 128), BF16),
        V((2, EP // 2, NFE, CAP, 128), BF16),
        V((EP, CAP, 128), BF16),
        V((EP, NFE, CAP, 128), BF16),
        V((NZ, S, 128), BF16),
        V((NZ, S, 128), BF16),
        V((S, 128), F32),
        V((H, 128), F32),
        V((S, 128), BF16),
        V((H, 128), BF16),
        V((L, S), BF16),
        V((L, H), BF16),
        V((2, S, L), F32),
        dma((24,)),
        dma((NZ, 2)), dma((NZ, 2)),
        dma((NZ, 2)), dma((NZ, 2)),
        dma((NZ,)), dma((NZ,)),
        dma((NZ,)), dma((NZ, 2)), dma((NZ,)),
        dma((11,)), dma((11,)),
        dma((NZ, 2)), dma((NZ, 2)),
        dma((NZ,)), dma((NZ,)),
        dma((NZ,)), dma((NZ,)),
        dma((2,)), dma((2,)),
        dma((2,)), dma((2,)),
        dma((NZ,)), dma((NZ,)),
        dma((EP // 2, 2)), dma((1,)),
        dma((EP // 2, 2)), dma((1,)),
        dma((NZ,)), dma((NZ,)),
    ]
    anyspace = pl.BlockSpec(memory_space=pl.ANY)
    mixed, new_state, new_conv = pl.pallas_call(
        functools.partial(kernel, EP, NZ, S, CAP, GS),
        out_shape=(
            V((S, 128), BF16),
            V((S, 128), F32),
            V((3, S, 128), BF16),
        ),
        in_specs=[anyspace] * len(args),
        out_specs=[pl.BlockSpec(memory_space=pltpu.VMEM)] * 3,
        scratch_shapes=scratch,
        compiler_params=pltpu.CompilerParams(
            collective_id=0, has_side_effects=True, vmem_limit_bytes=57000000
        ),
        name="layer",
    )(*args)
    shapes = ((S, 128), (S, 128), (3, S, 128))
    types = (BF16, F32, BF16)
    mixed, new_state, new_conv = pl.pallas_call(
        emit,
        out_shape=tuple(jax.ShapeDtypeStruct(a, b) for a, b in zip(shapes, types)),
        in_specs=[pl.BlockSpec(memory_space=pltpu.VMEM)] * 3,
        out_specs=[anyspace] * 3,
        scratch_shapes=[dma((3,))],
        compiler_params=pltpu.CompilerParams(vmem_limit_bytes=2 * 1024 * 1024),
        name="emit",
    )(mixed, new_state, new_conv)
    return mixed, new_state, jnp.transpose(new_conv, (1, 0, 2))


def solution(mesh):
    return jax.shard_map(
        on_device,
        mesh=mesh,
        in_specs=(
            P("ep", "tp"),
            P("ep", None, "tp"),
            P("ep", "tp"),
            P("tp"),
            P(None, "tp"),
            P(None, "tp"),
            P(None, "tp"),
            P("tp"),
            P("tp", None, None),
            P("tp"),
            P("tp", None, None),
            P("tp"),
            P("tp"),
            P(None, "tp"),
            P("tp"),
            P(),
            P(),
            P("ep", None),
            P("ep", None, "tp"),
            P("ep", None, "tp"),
            P("ep", "tp", None),
        ),
        out_specs=(P("ep", "tp"), P("ep", "tp"), P("ep", None, "tp")),
        check_vma=False,
    )
```
